32 devices in a mesh: grp: 2 (over y), sp: 4 (over z), tp: 4 (over x, core).
Axes of the slice: x: 2, y: 2, z: 4, core: 2. Of those that a mesh axis runs over, the one named last changes fastest.
Arguments:
- latents: bfloat16 [3072, 4096], P(('grp', 'sp', 'tp')), parts along dimension 0, may hold values from -3 to 3
- conditions: float32 [4, 4096], P('grp', 'sp'), parts along dimension 0, may hold values from -6 to 6
- context: bfloat16 [1024, 4096], P(('grp', 'sp')), parts along dimension 0, may hold values from -6 to 6
- w_shift: bfloat16 [4096, 4096], P('sp', 'tp'), may hold values from -0.09375 to 0.09375
- w_scale: bfloat16 [4096, 4096], P('sp', 'tp'), may hold values from -0.09375 to 0.09375
- w_gate: bfloat16 [4096, 4096], P('sp', 'tp'), may hold values from -0.09375 to 0.09375
- w_qdown: bfloat16 [4096, 1024], P(None, 'tp'), may hold values from -2 to 2
- w_kvdown: bfloat16 [4096, 512], P(None, 'tp'), may hold values from -2 to 2
- w_rope: bfloat16 [4096, 32], replicated, may hold values from -0.09375 to 0.09375
- q_gain: float32 [1024], replicated, may hold values from 1 to 24
- latent_norm_gain: float32 [512], replicated, may hold values from 0.1 to 1.9
- query_up_weight: bfloat16 [1024, 3072], P(None, 'tp'), may hold values from -0.1875 to 0.1875
- key_up_weight: bfloat16 [512, 2048], P(None, 'tp'), may hold values from -0.25 to 0.25
- value_up_weight: bfloat16 [512, 2048], P(None, 'tp'), may hold values from -0.25 to 0.25
- context_bias: float32 [32], P('tp'), may hold values from 0.5 to 2
- w_out: bfloat16 [2048, 4096], P(None, 'tp'), may hold values from -0.5 to 0.5
Outputs:
- mixed: bfloat16 [3072, 4096], P(('grp', 'sp', 'tp')), parts along dimension 0
The draws below stay inside these ranges and needn't reach their ends.
There are 2 independent parts, one for each index of `grp`. The reference program is written for one: setup_inputs(seed, part) draws one part's arguments, and reference() takes and returns one part's arrays. A program takes and returns all parts, laid end to end along the dimension named above; an argument that names none is the same for every part. Nothing has to cross between parts.
All inputs are finite; a program needn't handle non-finite values.
Results may differ from the reference program's by a relative error of at most 0.01345.
The reference program's roundings to bfloat16 on the way count: a program that leaves them out, or rounds other values in their place, can miss the bound.
Values may be sent and summed in bfloat16 or wider, within the bound.
No kernel may reach another device: no remote copies, remote signals or barrier semaphores. Data moves between devices by JAX's collectives and lax.ppermute only.
A program may use at most 64 MiB of HBM per device.

```python
import math
import jax
import jax.numpy as jnp
from jax import lax

MODEL_WIDTH = 4096
HEAD_TOTAL = 32
PLAIN_QK_DIM = 64
ROTARY_DIM = 32
VALUE_DIM = 64
QUERY_RANK = 1024
LATENT_KV_RANK = 512
GRID_W = 64
CTX = 512
TOKENS = 1536


def ascending_columns(key, row_count, col_count):
    entries = jax.random.normal(jax.random.fold_in(key, 11), (row_count, col_count), jnp.float32)
    jitter = jax.random.uniform(jax.random.fold_in(key, 12), (col_count,), jnp.float32, math.log(0.6), math.log(1.6))
    steepness = 10.0
    column_scale = jnp.exp(jitter + math.log(steepness) * jnp.arange(col_count, dtype=jnp.float32) / col_count)
    column_scale = column_scale / jnp.sqrt(jnp.mean(column_scale * column_scale))
    return jnp.clip(jnp.clip(entries, -4.0, 4.0) * column_scale * row_count ** (-0.5), -2.0, 2.0)


def draw_w_qdown(key, part):
    return ascending_columns(jax.random.fold_in(key, 3), MODEL_WIDTH, QUERY_RANK).astype(jnp.bfloat16)


def draw_w_kvdown(key, part):
    return ascending_columns(jax.random.fold_in(key, 5), MODEL_WIDTH, LATENT_KV_RANK).astype(jnp.bfloat16)


def draw_q_gain(key, part):
    return jax.random.uniform(jax.random.fold_in(key, 7), (QUERY_RANK,), jnp.float32, 1.5, 3.5)


def levels(stream_key, shape, shards, smallest, high):
    def one(position, shards_of):
        draws = jax.random.uniform(jax.random.fold_in(jax.random.fold_in(stream_key, 6), position), (shards_of,), jnp.float32, smallest / len(shards), high / len(shards))
        return jnp.repeat(jnp.exp(draws), shape[position] // shards_of).reshape((-1,) + (1,) * (len(shape) - position - 1))

    factor_of = one(*shards[0])
    for cut in shards[1:]:
        factor_of = factor_of * one(*cut)
    return factor_of


def noise(rng, extent, scale, most, cuts=(), held_as=jnp.bfloat16):
    loudness = levels(rng, extent, cuts, -0.22, 0.18) if cuts else 1.0
    result = jax.random.normal(rng, extent, jnp.float32) * scale * loudness
    return jnp.minimum(jnp.maximum(result, -most), most).astype(held_as)


def setup_inputs(seed: int = 0, part: int = 0) -> dict:
    streams_of = jax.random.split(jax.random.key(seed), 17)
    part_splits = jax.random.split(jax.random.fold_in(streams_of[16], part), 17)
    latents = noise(part_splits[0], (TOKENS, MODEL_WIDTH), 0.5, 3.0, ((0, 16),))
    conditions = noise(part_splits[1], (2, MODEL_WIDTH), 1.0, 6.0, ((1, 4),), jnp.float32)
    context = noise(part_splits[2], (CTX, MODEL_WIDTH), 1.0, 6.0, ((0, 4),))
    w_shift = noise(streams_of[3], (MODEL_WIDTH, MODEL_WIDTH), MODEL_WIDTH ** -0.5, 0.09375, ((0, 4), (1, 4)))
    w_scale = noise(streams_of[4], (MODEL_WIDTH, MODEL_WIDTH), MODEL_WIDTH ** -0.5, 0.09375, ((0, 4), (1, 4)))
    w_gate = noise(streams_of[5], (MODEL_WIDTH, MODEL_WIDTH), MODEL_WIDTH ** -0.5, 0.09375, ((0, 4), (1, 4)))
    w_qdown = draw_w_qdown(jax.random.fold_in(streams_of[16], 71), part)
    w_kvdown = draw_w_kvdown(jax.random.fold_in(streams_of[16], 71), part)
    w_rope = noise(streams_of[8], (MODEL_WIDTH, ROTARY_DIM), MODEL_WIDTH ** -0.5, 0.09375)
    q_gain = draw_q_gain(jax.random.fold_in(streams_of[16], 71), part)
    latent_norm_gain = jnp.clip(1.0 + 0.18 * jax.random.normal(streams_of[10], (LATENT_KV_RANK,), jnp.float32), 0.1, 1.9)
    query_up_weight = noise(streams_of[11], (QUERY_RANK, HEAD_TOTAL * (PLAIN_QK_DIM + ROTARY_DIM)), QUERY_RANK ** -0.5, 0.1875, ((1, 4),))
    key_up_weight = noise(streams_of[12], (LATENT_KV_RANK, HEAD_TOTAL * PLAIN_QK_DIM), LATENT_KV_RANK ** -0.5, 0.25, ((1, 4),))
    value_up_weight = noise(streams_of[13], (LATENT_KV_RANK, HEAD_TOTAL * VALUE_DIM), LATENT_KV_RANK ** -0.5, 0.25, ((1, 4),))
    context_bias = jnp.clip(0.5 + 1.5 * jax.random.uniform(streams_of[14], (HEAD_TOTAL,), jnp.float32) ** levels(streams_of[14], (HEAD_TOTAL,), ((0, 4),), -0.2, 0.2), 0.5, 2.0)
    w_out = noise(streams_of[15], (HEAD_TOTAL * VALUE_DIM, MODEL_WIDTH), (HEAD_TOTAL * VALUE_DIM // 16) ** -0.5, 0.5, ((1, 4),))
    return {"latents": latents, "conditions": conditions, "context": context, "w_shift": w_shift, "w_scale": w_scale, "w_gate": w_gate, "w_qdown": w_qdown, "w_kvdown": w_kvdown, "w_rope": w_rope, "q_gain": q_gain, "latent_norm_gain": latent_norm_gain, "query_up_weight": query_up_weight, "key_up_weight": key_up_weight, "value_up_weight": value_up_weight, "context_bias": context_bias, "w_out": w_out}


EPSILON = 1e-06

def layer_modulate(row_block, shift_by, scale_by):
    values = row_block.astype(jnp.float32)
    center = values - lax.optimization_barrier(jnp.mean(values, axis=-1, keepdims=True))
    spread = lax.optimization_barrier(jnp.mean(center * center, axis=-1, keepdims=True))
    normed = center * lax.rsqrt(spread + EPSILON)
    return (normed * (1.0 + scale_by) + shift_by).astype(jnp.bfloat16)

def rms_scale(raw_rows, gain_vec):
    values = raw_rows.astype(jnp.float32)
    factor = lax.rsqrt(lax.optimization_barrier(jnp.mean(values * values, axis=-1, keepdims=True)) + EPSILON)
    return (values * factor * gain_vec).astype(jnp.bfloat16)

def axial_turn(values, positions):
    freq_count = values.shape[-1] // 4
    inverse = 10000.0 ** (-jnp.arange(freq_count, dtype=jnp.float32) / freq_count)
    grid_row = (positions // GRID_W).astype(jnp.float32)
    grid_col = (positions % GRID_W).astype(jnp.float32)
    target = (positions.shape[0],) + (1,) * (values.ndim - 2) + (freq_count,)
    pieces = []
    for half_index, coordinate in enumerate((grid_row, grid_col)):
        angles = (coordinate[:, None] * inverse[None, :]).reshape(target)
        cosine = jnp.cos(angles)
        sine_of = jnp.sin(angles)
        segment = values[..., 2 * half_index * freq_count:2 * (half_index + 1) * freq_count]
        low_half = segment[..., :freq_count]
        high_half = segment[..., freq_count:]
        pieces.append(low_half * cosine - high_half * sine_of)
        pieces.append(low_half * sine_of + high_half * cosine)
    return jnp.concatenate(pieces, axis=-1)

def reference(latents, conditions, context, w_shift, w_scale, w_gate, w_qdown, w_kvdown, w_rope, q_gain, latent_norm_gain, query_up_weight, key_up_weight, value_up_weight, context_bias, w_out):
    cond_act = jax.nn.silu(conditions.astype(jnp.float32)).astype(jnp.bfloat16)
    shift_lat = jnp.dot(cond_act[0], w_shift, preferred_element_type=jnp.float32)
    scale_lat = jnp.dot(cond_act[0], w_scale, preferred_element_type=jnp.float32)
    gate_lat = jnp.dot(cond_act[0], w_gate, preferred_element_type=jnp.float32)
    shift_ctx = jnp.dot(cond_act[1], w_shift, preferred_element_type=jnp.float32)
    scale_ctx = jnp.dot(cond_act[1], w_scale, preferred_element_type=jnp.float32)
    h_lat = layer_modulate(latents, shift_lat, scale_lat)
    h_ctx = layer_modulate(context, shift_ctx, scale_ctx)
    cq_all = rms_scale(jnp.dot(h_lat, w_qdown, preferred_element_type=jnp.float32).astype(jnp.bfloat16), q_gain)
    ckv_lat = rms_scale(jnp.dot(h_lat, w_kvdown, preferred_element_type=jnp.float32).astype(jnp.bfloat16), latent_norm_gain)
    ckv_ctx = rms_scale(jnp.dot(h_ctx, w_kvdown, preferred_element_type=jnp.float32).astype(jnp.bfloat16), latent_norm_gain)
    positions = jnp.arange(TOKENS, dtype=jnp.int32)
    kr_lat = axial_turn(jnp.dot(h_lat, w_rope, preferred_element_type=jnp.float32), positions).astype(jnp.bfloat16)
    kr_ctx = jnp.dot(h_ctx, w_rope, preferred_element_type=jnp.float32).astype(jnp.bfloat16)
    q_all = jnp.dot(cq_all, query_up_weight, preferred_element_type=jnp.float32).reshape(TOKENS, HEAD_TOTAL, PLAIN_QK_DIM + ROTARY_DIM)
    queries = jnp.concatenate([q_all[..., :PLAIN_QK_DIM], axial_turn(q_all[..., PLAIN_QK_DIM:], positions)], axis=-1).astype(jnp.bfloat16)
    key_rows = jnp.concatenate([jnp.dot(ckv_lat, key_up_weight, preferred_element_type=jnp.float32).astype(jnp.bfloat16), jnp.dot(ckv_ctx, key_up_weight, preferred_element_type=jnp.float32).astype(jnp.bfloat16)], axis=0)
    value_rows = jnp.concatenate([jnp.dot(ckv_lat, value_up_weight, preferred_element_type=jnp.float32).astype(jnp.bfloat16), jnp.dot(ckv_ctx, value_up_weight, preferred_element_type=jnp.float32).astype(jnp.bfloat16)], axis=0)
    key_rows = key_rows.reshape(TOKENS + CTX, HEAD_TOTAL, PLAIN_QK_DIM)
    value_rows = value_rows.reshape(TOKENS + CTX, HEAD_TOTAL, VALUE_DIM)
    rope_keys = jnp.concatenate([kr_lat, kr_ctx], axis=0)
    is_ctx = (jnp.arange(TOKENS + CTX, dtype=jnp.int32) >= TOKENS).astype(jnp.float32)
    score_scale = (PLAIN_QK_DIM + ROTARY_DIM) ** (-0.5)

    def one_head(operands):
        head_q, head_k, head_v, head_bias = operands
        scores = jnp.dot(head_q[:, :PLAIN_QK_DIM], head_k.T, preferred_element_type=jnp.float32)
        scores = scores + jnp.dot(head_q[:, PLAIN_QK_DIM:], rope_keys.T, preferred_element_type=jnp.float32)
        scores = scores * score_scale + head_bias * is_ctx[None, :]
        largest = lax.optimization_barrier(jnp.max(scores, axis=-1, keepdims=True))
        exponent = jnp.exp(scores - largest)
        row_sum = lax.optimization_barrier(jnp.sum(exponent, axis=-1, keepdims=True))
        weights = exponent.astype(jnp.bfloat16)
        return (jnp.dot(weights, head_v, preferred_element_type=jnp.float32) / row_sum).astype(jnp.bfloat16)
    attended = lax.map(one_head, (queries.transpose(1, 0, 2), key_rows.transpose(1, 0, 2), value_rows.transpose(1, 0, 2), context_bias))
    attended = attended.transpose(1, 0, 2).reshape(TOKENS, HEAD_TOTAL * VALUE_DIM)
    projected = jnp.dot(attended, w_out, preferred_element_type=jnp.float32).astype(jnp.bfloat16)
    return (latents.astype(jnp.float32) + gate_lat * projected.astype(jnp.float32)).astype(jnp.bfloat16)
```

```python
import functools

import jax
import jax.numpy as jnp
from jax import lax
from jax.experimental import pallas as pl
from jax.experimental.pallas import tpu as pltpu
from jax.sharding import PartitionSpec as P

PLAIN_QK_DIM = 64
ROTARY_DIM = 32
VALUE_DIM = 64
GRID_W = 64
LANES = 128
LOG2E = 1.4426950408889634

EPSILON = 1e-06
NEGATIVE = -1e30


VMEM = pltpu.VMEM
SMEM = pltpu.SMEM


def in_vmem():
    return pl.BlockSpec(memory_space=VMEM)


def in_smem():
    return pl.BlockSpec(memory_space=SMEM)


def f32_dot(a, b):
    return jnp.dot(a, b, preferred_element_type=jnp.float32)


def swap(value, axis, bit):
    count = lax.axis_size(axis)
    return lax.ppermute(value, axis, [(i, i ^ bit) for i in range(count)])


def is_small(count):
    return count <= 4


def tp_bits(count):
    bits = []
    bit = 2
    while bit < count:
        bits.append(bit)
        bit *= 2
    if count > 1:
        bits.append(1)
    return bits


def spread(value, axis="tp"):
    if not is_small(lax.axis_size(axis)):
        return list(lax.all_gather(value, axis))
    got = {0: value}
    for bit in tp_bits(lax.axis_size(axis)):
        for member in list(got):
            got[member ^ bit] = swap(got[member], axis, bit)
    return [got[member] for member in range(len(got))]


def add_up(value, axis):
    count = lax.axis_size(axis)
    if not is_small(count):
        return lax.psum(value, axis)
    bit = 1
    while bit < count:
        value = value + swap(value, axis, bit)
        bit *= 2
    return value


def return_rows(value, ids, axis="tp"):
    count = lax.axis_size(axis)
    rows = value.shape[0] // count
    if not is_small(count):
        return list(lax.all_to_all(value.reshape(count, rows, -1), axis, 0, 0))
    pieces = []
    for member in range(count):
        piece = lax.dynamic_slice_in_dim(value, ids[member] * rows, rows, 0)
        pieces.append(swap(piece, axis, member) if member else piece)
    return pieces


def place(pieces, ids, axis):
    width = pieces[0].shape[axis]
    shape = list(pieces[0].shape)
    shape[axis] = width * len(pieces)
    whole = jnp.zeros(shape, pieces[0].dtype)
    for member, piece in enumerate(pieces):
        whole = lax.dynamic_update_slice_in_dim(whole, piece, ids[member] * width, axis)
    return whole


def turn_tables(positions, lanes):
    freq_count = ROTARY_DIM // 4
    inverse = 10000.0 ** (-jnp.arange(freq_count, dtype=jnp.float32) / freq_count)
    grid_row = (positions // GRID_W).astype(jnp.float32)
    grid_col = (positions % GRID_W).astype(jnp.float32)
    cosines, sines = [], []
    for coordinate in (grid_row, grid_col):
        angles = coordinate[:, None] * inverse[None, :]
        cosine, sine_of = jnp.cos(angles), jnp.sin(angles)
        cosines += [cosine, cosine]
        sines += [-sine_of, sine_of]
    cosine = jnp.concatenate(cosines, axis=1)
    sine_of = jnp.concatenate(sines, axis=1)
    repeat = lanes // ROTARY_DIM
    return jnp.tile(cosine, (1, repeat)), jnp.tile(sine_of, (1, repeat))


def turn(values, cosine, sine_of):
    freq_count = ROTARY_DIM // 4
    lanes = values.shape[1]
    lane = lax.broadcasted_iota(jnp.int32, values.shape, 1)
    first = (lane % (2 * freq_count)) < freq_count
    partner = jnp.where(
        first, pltpu.roll(values, lanes - freq_count, 1), pltpu.roll(values, freq_count, 1)
    )
    return values * cosine + partner * sine_of


def down_kernel(block_rows, tok_count, kv_cols, *refs):
    count = len(block_rows)
    offsets = refs[0]
    blocks = refs[1 : 1 + count]
    ctx_ref, mod_ref, wq_ref, wk_ref, cos_ref, sin_ref = refs[1 + count : 7 + count]
    cq_ref, kv_ref, kr_ref, h_ref = refs[7 + count :]
    step = 16

    def modulate(source, rows, base, shift_row, scale_row):
        shift_by = mod_ref[shift_row : shift_row + 1, :]
        scale_by = 1.0 + mod_ref[scale_row : scale_row + 1, :]
        for row in range(0, rows, step):
            values = source[row : row + step, :].astype(jnp.float32)
            center = values - jnp.mean(values, axis=-1, keepdims=True)
            spread_of = jnp.mean(center * center, axis=-1, keepdims=True)
            normed = center * lax.rsqrt(spread_of + EPSILON)
            h_ref[pl.ds(pl.multiple_of(base + row, step), step), :] = (
                normed * scale_by + shift_by
            ).astype(jnp.bfloat16)

    for number, (source, rows) in enumerate(zip(blocks, block_rows)):
        modulate(source, rows, offsets[number] * rows, 0, 2)
    modulate(ctx_ref, ctx_ref.shape[0], tok_count, 1, 3)
    cq_ref[...] = f32_dot(h_ref[:tok_count, :], wq_ref[...]).astype(jnp.bfloat16)
    mixed = f32_dot(h_ref[...], wk_ref[...])
    kv_ref[...] = mixed[:, LANES:].astype(jnp.bfloat16)
    turned = turn(mixed[:, :LANES], cos_ref[...], sin_ref[...])
    pick = (
        lax.broadcasted_iota(jnp.int32, (ROTARY_DIM, LANES), 0)
        == lax.broadcasted_iota(jnp.int32, (ROTARY_DIM, LANES), 1)
    ).astype(jnp.bfloat16)
    kr_ref[...] = lax.dot_general(
        pick,
        turned.astype(jnp.bfloat16),
        (((1,), (1,)), ((), ())),
        preferred_element_type=jnp.float32,
    ).astype(jnp.bfloat16)


def normed_into(scratch, ids, pieces, gain_ref):
    width = pieces[0].shape[1]
    total = width * len(pieces)
    squares = None
    for piece in pieces:
        values = piece[...].astype(jnp.float32)
        part = jnp.sum(values * values, axis=-1, keepdims=True)
        squares = part if squares is None else squares + part
    factor = lax.rsqrt(squares / total + EPSILON)
    for number, piece in enumerate(pieces):
        if len(pieces) == 1:
            where = slice(None)
        else:
            where = pl.ds(pl.multiple_of(ids[number] * width, LANES), width)
        gained = piece[...].astype(jnp.float32) * factor * gain_ref[:, where]
        scratch[:, where] = gained.astype(jnp.bfloat16)


def query_kernel(count, *refs):
    ids = refs[0]
    pieces = refs[1 : 1 + count]
    gain_ref, wn_ref, wr_ref, cos_ref, sin_ref, q_ref, scratch = refs[1 + count :]
    normed_into(scratch, ids, pieces, gain_ref)
    rows = scratch.shape[0]
    plain = f32_dot(scratch[...], wn_ref[...])
    rotary = f32_dot(scratch[...], wr_ref[...])
    group = q_ref.shape[2] - LANES
    per_group = group // ROTARY_DIM
    lane = lax.broadcasted_iota(jnp.int32, (rows, LANES), 1)
    glane = lax.broadcasted_iota(jnp.int32, (rows, group), 1)
    turned = {}
    for pair in range(q_ref.shape[0]):
        both = plain[:, pair * LANES : (pair + 1) * LANES].astype(jnp.bfloat16)
        for half in range(2):
            head = 2 * pair + half
            where = head // per_group
            if where not in turned:
                turned[where] = turn(
                    rotary[:, where * group : (where + 1) * group], cos_ref[...], sin_ref[...]
                ).astype(jnp.bfloat16)
            spot = slice(half * rows, (half + 1) * rows)
            q_ref[pair, spot, :LANES] = jnp.where(
                lane // PLAIN_QK_DIM == half, both, jnp.zeros_like(both)
            )
            q_ref[pair, spot, LANES:] = jnp.where(
                glane // ROTARY_DIM == head % per_group,
                turned[where],
                jnp.zeros_like(turned[where]),
            )


def expand_kernel(count, *refs):
    ids = refs[0]
    pieces = refs[1 : 1 + count]
    kr_ref, gain_ref, wk_ref, wv_ref, k_ref, v_ref, r_ref, scratch = refs[1 + count :]
    normed_into(scratch, ids, pieces, gain_ref)
    k_ref[...] = f32_dot(scratch[...], wk_ref[...]).astype(jnp.bfloat16)
    v_ref[...] = f32_dot(scratch[...], wv_ref[...]).astype(jnp.bfloat16)
    group = r_ref.shape[1]
    copies = (
        lax.broadcasted_iota(jnp.int32, (ROTARY_DIM, group), 0)
        == lax.broadcasted_iota(jnp.int32, (ROTARY_DIM, group), 1) % ROTARY_DIM
    ).astype(jnp.bfloat16)
    r_ref[...] = lax.dot_general(
        kr_ref[...], copies, (((0,), (0,)), ((), ())), preferred_element_type=jnp.float32
    ).astype(jnp.bfloat16)


def attend_kernel(count, tok_keys, *refs):
    q_ref, bias_ref = refs[:2]
    keys = refs[2 : 2 + count]
    values = refs[2 + count : 2 + 2 * count]
    ropes = refs[2 + 2 * count : 2 + 3 * count]
    out_ref = refs[2 + 3 * count]
    rows = out_ref.shape[0]
    score_scale = (PLAIN_QK_DIM + ROTARY_DIM) ** (-0.5) * LOG2E
    lane = lax.broadcasted_iota(jnp.int32, (rows, LANES), 1)
    for pair in range(q_ref.shape[0]):
        span = slice(pair * LANES, (pair + 1) * LANES)
        done = []
        for half in range(2):
            query = q_ref[pair, half * rows : (half + 1) * rows, :]
            bias = bias_ref[2 * pair + half] * LOG2E
            top = total = acc = None
            for number in range(count):
                key = jnp.concatenate([keys[number][:, span], ropes[number][...]], axis=1)
                scores = lax.dot_general(
                    query, key, (((1,), (1,)), ((), ())), preferred_element_type=jnp.float32
                )
                lat, ctx = scores[:, :tok_keys], scores[:, tok_keys:]
                peak = jnp.maximum(
                    jnp.max(lat, axis=-1, keepdims=True) * score_scale,
                    jnp.max(ctx, axis=-1, keepdims=True) * score_scale + bias,
                )
                new_top = peak if top is None else jnp.maximum(top, peak)
                e_lat = jnp.exp2(lat * score_scale - new_top)
                e_ctx = jnp.exp2(ctx * score_scale - (new_top - bias))
                part = jnp.sum(e_lat, axis=-1, keepdims=True) + jnp.sum(
                    e_ctx, axis=-1, keepdims=True
                )
                weights = jnp.concatenate([e_lat, e_ctx], axis=1).astype(jnp.bfloat16)
                gathered = f32_dot(weights, values[number][:, span])
                if top is None:
                    total, acc = part, gathered
                else:
                    rescale = jnp.exp2(top - new_top)
                    total = total * rescale + part
                    acc = acc * rescale + gathered
                top = new_top
            done.append(acc / total)
        out_ref[:, span] = jnp.where(lane < VALUE_DIM, done[0], done[1]).astype(jnp.bfloat16)


def out_kernel(count, *refs):
    ids = refs[0]
    pieces = refs[1 : 1 + count]
    w_ref, out_ref = refs[1 + count :]
    depth = pieces[0].shape[1]
    total = None
    for number, piece in enumerate(pieces):
        rows = pl.ds(pl.multiple_of(ids[number] * depth, LANES), depth)
        part = f32_dot(piece[...], w_ref[rows, :])
        total = part if total is None else total + part
    out_ref[...] = total.astype(jnp.bfloat16)


def final_kernel(count, *refs):
    ids = refs[0]
    pieces = refs[1 : 1 + count]
    lat_ref, gate_ref, out_ref = refs[1 + count :]
    width = pieces[0].shape[1]
    for number, piece in enumerate(pieces):
        span = pl.ds(pl.multiple_of(ids[number] * width, LANES), width)
        out_ref[:, span] = (
            lat_ref[:, span].astype(jnp.float32)
            + gate_ref[:, span] * piece[...].astype(jnp.float32)
        ).astype(jnp.bfloat16)


def call(kernel, outs, operands, smem=(0,), scratch=()):
    specs = [in_smem() if place_of in smem else in_vmem() for place_of in range(len(operands))]
    many = isinstance(outs, (list, tuple))
    return pl.pallas_call(
        kernel,
        out_shape=outs,
        in_specs=specs,
        out_specs=[in_vmem() for _ in outs] if many else in_vmem(),
        scratch_shapes=list(scratch),
        compiler_params=pltpu.CompilerParams(vmem_limit_bytes=60 * 1024 * 1024),
    )(*operands)


def on_device(
    latents,
    conditions,
    context,
    w_shift,
    w_scale,
    w_gate,
    w_qdown,
    w_kvdown,
    w_rope,
    q_gain,
    latent_norm_gain,
    query_up_weight,
    key_up_weight,
    value_up_weight,
    context_bias,
    w_out,
):
    tp_count = lax.axis_size("tp")
    sp_count = lax.axis_size("sp")
    tp_index = lax.axis_index("tp")
    sp_index = lax.axis_index("sp")
    own_rows, width = latents.shape
    tok_count = own_rows * tp_count
    ctx_rows = context.shape[0]
    seg_rows = tok_count + ctx_rows
    ids = jnp.arange(tp_count, dtype=jnp.int32)
    if is_small(tp_count):
        ids = jnp.bitwise_xor(tp_index, ids)
    bf16 = jnp.bfloat16

    lat_blocks = spread(latents)

    cond_act = jax.nn.silu(conditions).astype(bf16)
    partial_mod = jnp.concatenate(
        [f32_dot(cond_act, w_shift), f32_dot(cond_act, w_scale), f32_dot(cond_act[0:1], w_gate)],
        axis=0,
    )
    modulation = place(spread(add_up(partial_mod, "sp")), ids, 1)

    head_count = query_up_weight.shape[1] // (PLAIN_QK_DIM + ROTARY_DIM)
    group = min(LANES, head_count * ROTARY_DIM)
    pairs = head_count // 2
    by_head = query_up_weight.reshape(-1, head_count, PLAIN_QK_DIM + ROTARY_DIM)
    w_plain = by_head[:, :, :PLAIN_QK_DIM].reshape(-1, head_count * PLAIN_QK_DIM)
    w_rotary = by_head[:, :, PLAIN_QK_DIM:].reshape(-1, head_count * ROTARY_DIM)
    q_pos = sp_index * tok_count + jnp.arange(tok_count, dtype=jnp.int32)
    cosine, sine_of = turn_tables(q_pos, LANES)
    k_cosine = jnp.concatenate([cosine, jnp.ones((ctx_rows, LANES), jnp.float32)], axis=0)
    k_sine = jnp.concatenate([sine_of, jnp.zeros((ctx_rows, LANES), jnp.float32)], axis=0)
    kv_cols = w_kvdown.shape[1]
    q_cols = w_qdown.shape[1]
    w_kr = jnp.concatenate([jnp.tile(w_rope, (1, LANES // ROTARY_DIM)), w_kvdown], axis=1)

    if own_rows % 16:
        lat_blocks = [place(lat_blocks, ids, 0)]
        block_ids = jnp.zeros((1,), jnp.int32)
    else:
        block_ids = ids
    cq_cols, kv_cols_own, kr_own = call(
        functools.partial(down_kernel, [b.shape[0] for b in lat_blocks], tok_count, kv_cols),
        [
            jax.ShapeDtypeStruct((tok_count, q_cols), bf16),
            jax.ShapeDtypeStruct((seg_rows, kv_cols), bf16),
            jax.ShapeDtypeStruct((ROTARY_DIM, seg_rows), bf16),
        ],
        [block_ids, *lat_blocks, context, modulation, w_qdown, w_kr, k_cosine, k_sine],
        scratch=[VMEM((seg_rows, width), bf16)],
    )

    def columns(value):
        pieces = spread(value)
        if value.shape[1] % LANES:
            return [place(pieces, ids, 1)]
        return pieces

    if is_small(sp_count):
        kv_by_block = [kv_cols_own]
        kr_by_block = [kr_own]
        for member in range(1, sp_count):
            kv_by_block.append(swap(kv_cols_own, "sp", member))
            kr_by_block.append(swap(kr_own, "sp", member))
        kv_pieces = [columns(value) for value in kv_by_block]
    else:
        kr_by_block = list(lax.all_gather(kr_own, "sp"))
        every = lax.all_gather(lax.all_gather(kv_cols_own, "tp", axis=1, tiled=True), "sp")
        kv_pieces = [[value] for value in every]
    cq_pieces = columns(cq_cols)
    queries = call(
        functools.partial(query_kernel, len(cq_pieces)),
        jax.ShapeDtypeStruct((pairs, 2 * tok_count, LANES + group), bf16),
        [
            ids,
            *cq_pieces,
            q_gain[None, :],
            w_plain,
            w_rotary,
            cosine[:, :group],
            sine_of[:, :group],
        ],
        scratch=[VMEM((tok_count, q_gain.shape[0]), bf16)],
    )
    keys, values, ropes = [], [], []
    for pieces, rope in zip(kv_pieces, kr_by_block):
        key, value, rope = call(
            functools.partial(expand_kernel, len(pieces)),
            [
                jax.ShapeDtypeStruct((seg_rows, head_count * PLAIN_QK_DIM), bf16),
                jax.ShapeDtypeStruct((seg_rows, head_count * VALUE_DIM), bf16),
                jax.ShapeDtypeStruct((seg_rows, group), bf16),
            ],
            [ids, *pieces, rope, latent_norm_gain[None, :], key_up_weight, value_up_weight],
            scratch=[VMEM((seg_rows, latent_norm_gain.shape[0]), bf16)],
        )
        keys.append(key)
        values.append(value)
        ropes.append(rope)
    attended = call(
        functools.partial(attend_kernel, sp_count, tok_count),
        jax.ShapeDtypeStruct((tok_count, head_count * VALUE_DIM), bf16),
        [queries, context_bias, *keys, *values, *ropes],
        smem=(1,),
    )
    att_pieces = spread(attended)
    out_cols = w_out.shape[1]
    proj_cols = call(
        functools.partial(out_kernel, tp_count),
        jax.ShapeDtypeStruct((tok_count, out_cols), bf16),
        [ids, *att_pieces, w_out],
    )
    proj_pieces = return_rows(proj_cols, ids)
    return call(
        functools.partial(final_kernel, tp_count),
        jax.ShapeDtypeStruct((own_rows, width), bf16),
        [ids, *proj_pieces, latents, modulation[4:5]],
    )


def solution(mesh):
    in_specs = (
        P(("grp", "sp", "tp"), None),
        P("grp", "sp"),
        P(("grp", "sp"), None),
        P("sp", "tp"),
        P("sp", "tp"),
        P("sp", "tp"),
        P(None, "tp"),
        P(None, "tp"),
        P(),
        P(),
        P(),
        P(None, "tp"),
        P(None, "tp"),
        P(None, "tp"),
        P("tp"),
        P(None, "tp"),
    )
    out_specs = P(("grp", "sp", "tp"), None)
    return jax.shard_map(
        on_device, mesh=mesh, in_specs=in_specs, out_specs=out_specs, check_vma=False
    )
```

```python
import functools

import jax
import jax.numpy as jnp
from jax import lax
from jax.experimental import pallas as pl
from jax.experimental.pallas import tpu as pltpu
from jax.sharding import PartitionSpec as P

PLAIN_QK_DIM = 64
ROTARY_DIM = 32
VALUE_DIM = 64
GRID_W = 64
LANES = 128
LOG2E = 1.4426950408889634

EPSILON = 1e-06
NEGATIVE = -1e30


VMEM = pltpu.VMEM
SMEM = pltpu.SMEM


def in_vmem():
    return pl.BlockSpec(memory_space=VMEM)


def in_smem():
    return pl.BlockSpec(memory_space=SMEM)


def f32_dot(a, b):
    return jnp.dot(a, b, preferred_element_type=jnp.float32)


def swap(value, axis, bit):
    count = lax.axis_size(axis)
    return lax.ppermute(value, axis, [(i, i ^ bit) for i in range(count)])


def is_small(count):
    return count <= 4


def tp_bits(count):
    bits = []
    bit = 2
    while bit < count:
        bits.append(bit)
        bit *= 2
    if count > 1:
        bits.append(1)
    return bits


def spread(value, axis="tp"):
    if not is_small(lax.axis_size(axis)):
        return list(lax.all_gather(value, axis))
    got = {0: value}
    for bit in tp_bits(lax.axis_size(axis)):
        for member in list(got):
            got[member ^ bit] = swap(got[member], axis, bit)
    return [got[member] for member in range(len(got))]


def add_up(value, axis):
    count = lax.axis_size(axis)
    if not is_small(count):
        return lax.psum(value, axis)
    bit = 1
    while bit < count:
        value = value + swap(value, axis, bit)
        bit *= 2
    return value


def return_rows(value, ids, axis="tp"):
    count = lax.axis_size(axis)
    rows = value.shape[0] // count
    if not is_small(count):
        return list(lax.all_to_all(value.reshape(count, rows, -1), axis, 0, 0))
    pieces = []
    for member in range(count):
        piece = lax.dynamic_slice_in_dim(value, ids[member] * rows, rows, 0)
        pieces.append(swap(piece, axis, member) if member else piece)
    return pieces


def place(pieces, ids, axis):
    width = pieces[0].shape[axis]
    shape = list(pieces[0].shape)
    shape[axis] = width * len(pieces)
    whole = jnp.zeros(shape, pieces[0].dtype)
    for member, piece in enumerate(pieces):
        whole = lax.dynamic_update_slice_in_dim(whole, piece, ids[member] * width, axis)
    return whole


def turn_tables(positions, lanes):
    freq_count = ROTARY_DIM // 4
    inverse = 10000.0 ** (-jnp.arange(freq_count, dtype=jnp.float32) / freq_count)
    grid_row = (positions // GRID_W).astype(jnp.float32)
    grid_col = (positions % GRID_W).astype(jnp.float32)
    cosines, sines = [], []
    for coordinate in (grid_row, grid_col):
        angles = coordinate[:, None] * inverse[None, :]
        cosine, sine_of = jnp.cos(angles), jnp.sin(angles)
        cosines += [cosine, cosine]
        sines += [-sine_of, sine_of]
    cosine = jnp.concatenate(cosines, axis=1)
    sine_of = jnp.concatenate(sines, axis=1)
    repeat = lanes // ROTARY_DIM
    return jnp.tile(cosine, (1, repeat)), jnp.tile(sine_of, (1, repeat))


def turn(values, cosine, sine_of):
    freq_count = ROTARY_DIM // 4
    lanes = values.shape[1]
    lane = lax.broadcasted_iota(jnp.int32, values.shape, 1)
    first = (lane % (2 * freq_count)) < freq_count
    partner = jnp.where(
        first, pltpu.roll(values, lanes - freq_count, 1), pltpu.roll(values, freq_count, 1)
    )
    return values * cosine + partner * sine_of


def gather_rows(scratch, ids, pieces):
    width = pieces[0].shape[1]
    for number, piece in enumerate(pieces):
        scratch[:, pl.ds(pl.multiple_of(ids[number] * width, LANES), width)] = piece[...]


def down_kernel(block_rows, mod_count, tok_count, merged, *refs):
    count = len(block_rows)
    ids, offsets = refs[:2]
    blocks = refs[2 : 2 + count]
    pieces = refs[2 + count : 2 + count + mod_count]
    refs = refs[2 + count + mod_count :]
    ctx_ref, wq_ref, wk_ref, wr_ref, cos_ref, sin_ref = refs[:6]
    cq_ref, kv_ref, kr_ref, h_ref, mod_ref, wkr_ref, rope_ref = refs[6:]
    step = 16
    gather_rows(mod_ref, ids, pieces)
    rope_w = wr_ref[...]
    wkr_ref[:, :LANES] = jnp.concatenate([rope_w] * (LANES // ROTARY_DIM), axis=1)
    wkr_ref[:, LANES:] = wk_ref[...]

    def modulate(source, rows, base, shift_row, scale_row):
        shift_by = mod_ref[shift_row : shift_row + 1, :]
        scale_by = 1.0 + mod_ref[scale_row : scale_row + 1, :]
        for row in range(0, rows, step):
            values = source[row : row + step, :].astype(jnp.float32)
            center = values - jnp.mean(values, axis=-1, keepdims=True)
            spread_of = jnp.mean(center * center, axis=-1, keepdims=True)
            normed = center * lax.rsqrt(spread_of + EPSILON)
            h_ref[pl.ds(pl.multiple_of(base + row, step), step), :] = (
                normed * scale_by + shift_by
            ).astype(jnp.bfloat16)

    for number, (source, rows) in enumerate(zip(blocks, block_rows)):
        modulate(source, rows, offsets[number] * rows, 0, 2)
    modulate(ctx_ref, ctx_ref.shape[0], tok_count, 1, 3)
    cq_ref[...] = f32_dot(h_ref[:tok_count, :], wq_ref[...]).astype(jnp.bfloat16)
    both = f32_dot(h_ref[...], wkr_ref[...])
    seg = h_ref.shape[0]
    kv_ref[:seg, :] = both[:, LANES:].astype(jnp.bfloat16)
    turned = turn(both[:, :LANES], cos_ref[...], sin_ref[...]).astype(jnp.bfloat16)
    if merged:
        rope_ref[...] = turned.astype(jnp.float32)
        quarter = seg // mod_count
        sub = quarter // (LANES // ROTARY_DIM)
        lane = lax.broadcasted_iota(jnp.int32, (sub, LANES), 1)
        packed = None
        for part in range(LANES // ROTARY_DIM):
            start = pl.multiple_of(ids[0] * quarter + part * sub, 8)
            rows = rope_ref[pl.ds(start, sub), :]
            rows = jnp.where(lane // ROTARY_DIM == part, rows, 0.0)
            packed = rows if packed is None else packed + rows
        kv_ref[seg:, :] = packed.astype(jnp.bfloat16)
        kr_ref[...] = jnp.zeros_like(kr_ref)
    else:
        kr_ref[...] = turned


def normed_into(scratch, ids, pieces, gain_ref):
    width = pieces[0].shape[1]
    rows = scratch.shape[0]
    total = width * len(pieces)
    squares = None
    for piece in pieces:
        values = piece[:rows, :].astype(jnp.float32)
        part = jnp.sum(values * values, axis=-1, keepdims=True)
        squares = part if squares is None else squares + part
    factor = lax.rsqrt(squares / total + EPSILON)
    for number, piece in enumerate(pieces):
        if len(pieces) == 1:
            where = slice(None)
        else:
            where = pl.ds(pl.multiple_of(ids[number] * width, LANES), width)
        gained = piece[:rows, :].astype(jnp.float32) * factor * gain_ref[:, where]
        scratch[:, where] = gained.astype(jnp.bfloat16)


def query_kernel(count, *refs):
    ids = refs[0]
    pieces = refs[1 : 1 + count]
    gain_ref, w_ref, cos_ref, sin_ref, q_ref, scratch = refs[1 + count :]
    normed_into(scratch, ids, pieces, gain_ref)
    rows = scratch.shape[0]
    raw = f32_dot(scratch[...], w_ref[...])
    short = -raw.shape[1] % LANES
    if short:
        raw = jnp.concatenate([raw, jnp.zeros((rows, short), jnp.float32)], axis=1)
    group = q_ref.shape[2] - LANES
    per_group = group // ROTARY_DIM
    lane = lax.broadcasted_iota(jnp.int32, (rows, LANES), 1)
    span = PLAIN_QK_DIM + ROTARY_DIM

    def bring(start, size, target):
        first = start // LANES * LANES
        last = -(-(start + size) // LANES) * LANES
        tile = raw[:, first : first + LANES]
        moved = pltpu.roll(tile, (target - (start - first)) % LANES, 1)
        if last - first > LANES:
            other = pltpu.roll(
                raw[:, first + LANES : last], (target - (start - first)) % LANES, 1
            )
            moved = jnp.where(lane < target + first + LANES - start, moved, other)
        return moved

    head_count = 2 * q_ref.shape[0]
    turned = {}
    for where in range(head_count // per_group):
        rotary = None
        for slot in range(per_group):
            start = (where * per_group + slot) * span + PLAIN_QK_DIM
            piece = bring(start, ROTARY_DIM, slot * ROTARY_DIM)
            rotary = (
                piece if rotary is None else jnp.where(lane >= slot * ROTARY_DIM, piece, rotary)
            )
        turned[where] = turn(rotary, cos_ref[...], sin_ref[...])
    for head in range(head_count):
        half = head % 2
        spot = slice(half * rows, (half + 1) * rows)
        plain = bring(head * span, PLAIN_QK_DIM, half * PLAIN_QK_DIM)
        q_ref[head // 2, spot, :LANES] = jnp.where(
            lane // PLAIN_QK_DIM == half, plain, 0.0
        ).astype(jnp.bfloat16)
        slot = head % per_group
        q_ref[head // 2, spot, LANES:] = jnp.where(
            lane // ROTARY_DIM == slot, turned[head // per_group], 0.0
        ).astype(jnp.bfloat16)[:, :group]


def attend_kernel(counts, tok_keys, seg, merged, first, last, *refs):
    ids, q_ref, bias_ref, gain_ref, wk_ref, wv_ref = refs[:6]
    refs = refs[6:]
    blocks = []
    for count in counts:
        blocks.append(refs[: count + (0 if merged else 1)])
        refs = refs[len(blocks[-1]) :]
    if not first:
        state_in, refs = refs[:3], refs[3:]
    if last:
        out_ref, refs = refs[0], refs[1:]
    else:
        state_out, refs = refs[:3], refs[3:]
    scratch, k_ref, v_ref, r_ref = refs
    heads = 2 * q_ref.shape[0]
    rows = q_ref.shape[1] // 2
    group = q_ref.shape[2] - LANES
    for number, block in enumerate(blocks):
        pieces = block if merged else block[:-1]
        base = number * seg
        normed_into(scratch, ids, pieces, gain_ref)
        k_ref[base : base + seg, :] = f32_dot(scratch[...], wk_ref[...]).astype(jnp.bfloat16)
        v_ref[base : base + seg, :] = f32_dot(scratch[...], wv_ref[...]).astype(jnp.bfloat16)
        if merged:
            quarter = seg // len(pieces)
            sub = quarter // (LANES // ROTARY_DIM)
            rlane = lax.broadcasted_iota(jnp.int32, (sub, LANES), 1)
            for member, piece in enumerate(pieces):
                packed = piece[seg:, :].astype(jnp.float32)
                for part in range(LANES // ROTARY_DIM):
                    only = jnp.where(rlane // ROTARY_DIM == part, packed, 0.0)
                    copies = only
                    for turn_by in range(1, LANES // ROTARY_DIM):
                        copies = copies + pltpu.roll(only, turn_by * ROTARY_DIM, 1)
                    start = pl.multiple_of(base + ids[member] * quarter + part * sub, 16)
                    r_ref[pl.ds(start, sub), :] = copies.astype(jnp.bfloat16)
        else:
            r_ref[base : base + seg, :] = block[-1][:, :group]
    score_scale = (PLAIN_QK_DIM + ROTARY_DIM) ** (-0.5) * LOG2E
    lane = lax.broadcasted_iota(jnp.int32, (rows, LANES), 1)
    for pair in range(heads // 2):
        span = slice(pair * LANES, (pair + 1) * LANES)
        done = []
        for half in range(2):
            head = 2 * pair + half
            query = q_ref[pair, half * rows : (half + 1) * rows, :]
            bias = bias_ref[head] * LOG2E
            top = total = acc = None
            if not first:
                top, total, acc = (held[head] for held in state_in)
            for number in range(len(blocks)):
                base = number * seg
                key = jnp.concatenate(
                    [k_ref[base : base + seg, span], r_ref[base : base + seg, :]], axis=1
                )
                scores = lax.dot_general(
                    query, key, (((1,), (1,)), ((), ())), preferred_element_type=jnp.float32
                )
                lat, ctx = scores[:, :tok_keys], scores[:, tok_keys:]
                peak = jnp.maximum(
                    jnp.max(lat, axis=-1, keepdims=True) * score_scale,
                    jnp.max(ctx, axis=-1, keepdims=True) * score_scale + bias,
                )
                new_top = peak if top is None else jnp.maximum(top, peak)
                e_lat = jnp.exp2(lat * score_scale - new_top)
                e_ctx = jnp.exp2(ctx * score_scale - (new_top - bias))
                part = jnp.sum(e_lat, axis=-1, keepdims=True) + jnp.sum(
                    e_ctx, axis=-1, keepdims=True
                )
                weights = jnp.concatenate([e_lat, e_ctx], axis=1).astype(jnp.bfloat16)
                gathered = f32_dot(weights, v_ref[base : base + seg, span])
                if top is None:
                    total, acc = part, gathered
                else:
                    rescale = jnp.exp2(top - new_top)
                    total = total * rescale + part
                    acc = acc * rescale + gathered
                top = new_top
            if last:
                done.append(acc / total)
            else:
                for held, value in zip(state_out, (top, total, acc)):
                    held[head] = value
        if last:
            out_ref[:, span] = jnp.where(lane < VALUE_DIM, done[0], done[1]).astype(jnp.bfloat16)


def out_kernel(count, *refs):
    ids = refs[0]
    pieces = refs[1 : 1 + count]
    w_ref, out_ref = refs[1 + count :]
    depth = pieces[0].shape[1]
    total = None
    for number, piece in enumerate(pieces):
        rows = pl.ds(pl.multiple_of(ids[number] * depth, LANES), depth)
        part = f32_dot(piece[...], w_ref[rows, :])
        total = part if total is None else total + part
    out_ref[...] = total.astype(jnp.bfloat16)


def final_kernel(count, mod_count, *refs):
    ids = refs[0]
    pieces = refs[1 : 1 + count]
    gates = refs[1 + count : 1 + count + mod_count]
    lat_ref, out_ref = refs[1 + count + mod_count :]
    width = pieces[0].shape[1]
    for number, (piece, gate) in enumerate(zip(pieces, gates)):
        span = pl.ds(pl.multiple_of(ids[number] * width, LANES), width)
        out_ref[:, span] = (
            lat_ref[:, span].astype(jnp.float32)
            + gate[gate.shape[0] - 1 :, :] * piece[...].astype(jnp.float32)
        ).astype(jnp.bfloat16)


def call(kernel, outs, operands, smem=(0,), scratch=(), mib=16):
    specs = [in_smem() if place_of in smem else in_vmem() for place_of in range(len(operands))]
    many = isinstance(outs, (list, tuple))
    return pl.pallas_call(
        kernel,
        out_shape=outs,
        in_specs=specs,
        out_specs=[in_vmem() for _ in outs] if many else in_vmem(),
        scratch_shapes=list(scratch),
        compiler_params=pltpu.CompilerParams(vmem_limit_bytes=mib * 1024 * 1024),
    )(*operands)


def on_device(
    latents,
    conditions,
    context,
    w_shift,
    w_scale,
    w_gate,
    w_qdown,
    w_kvdown,
    w_rope,
    q_gain,
    latent_norm_gain,
    query_up_weight,
    key_up_weight,
    value_up_weight,
    context_bias,
    w_out,
):
    tp_count = lax.axis_size("tp")
    sp_count = lax.axis_size("sp")
    tp_index = lax.axis_index("tp")
    sp_index = lax.axis_index("sp")
    own_rows, width = latents.shape
    tok_count = own_rows * tp_count
    ctx_rows = context.shape[0]
    seg_rows = tok_count + ctx_rows
    ids = jnp.arange(tp_count, dtype=jnp.int32)
    if is_small(tp_count):
        ids = jnp.bitwise_xor(tp_index, ids)
    bf16 = jnp.bfloat16

    lat_blocks = spread(latents)

    cond_act = jax.nn.silu(conditions).astype(bf16)
    partial_mod = jnp.concatenate(
        [f32_dot(cond_act, w_shift), f32_dot(cond_act, w_scale), f32_dot(cond_act[0:1], w_gate)],
        axis=0,
    )
    mod_pieces = spread(add_up(partial_mod, "sp"))

    head_count = query_up_weight.shape[1] // (PLAIN_QK_DIM + ROTARY_DIM)
    group = min(LANES, head_count * ROTARY_DIM)
    pairs = head_count // 2
    q_pos = sp_index * tok_count + jnp.arange(tok_count, dtype=jnp.int32)
    cosine, sine_of = turn_tables(q_pos, LANES)
    k_cosine = jnp.concatenate([cosine, jnp.ones((ctx_rows, LANES), jnp.float32)], axis=0)
    k_sine = jnp.concatenate([sine_of, jnp.zeros((ctx_rows, LANES), jnp.float32)], axis=0)
    kv_cols = w_kvdown.shape[1]
    q_cols = w_qdown.shape[1]

    block_ids = ids
    if own_rows % 16:
        lat_blocks = [place(lat_blocks, ids, 0)]
        block_ids = jnp.zeros((1,), jnp.int32)
    merged = (
        kv_cols % LANES == 0
        and group == LANES
        and seg_rows % (16 * tp_count * LANES // ROTARY_DIM) == 0
        and is_small(tp_count)
    )
    extra = seg_rows // tp_count * ROTARY_DIM // LANES if merged else 0
    cq_cols, kv_own, kr_own = call(
        functools.partial(
            down_kernel, [b.shape[0] for b in lat_blocks], tp_count, tok_count, merged
        ),
        [
            jax.ShapeDtypeStruct((tok_count, q_cols), bf16),
            jax.ShapeDtypeStruct((seg_rows + extra, kv_cols), bf16),
            jax.ShapeDtypeStruct((16 if merged else seg_rows, LANES), bf16),
        ],
        [
            ids,
            block_ids,
            *lat_blocks,
            *mod_pieces,
            context,
            w_qdown,
            w_kvdown,
            w_rope,
            k_cosine,
            k_sine,
        ],
        smem=(0, 1),
        scratch=[
            VMEM((seg_rows, width), bf16),
            VMEM((5, width), jnp.float32),
            VMEM((width, LANES + kv_cols), bf16),
            VMEM((seg_rows, LANES), jnp.float32),
        ],
        mib=30,
    )

    def columns(value):
        pieces = spread(value)
        if value.shape[1] % LANES:
            return [place(pieces, ids, 1)]
        return pieces

    if is_small(sp_count):
        blocks = []
        for member in range(sp_count):
            block = columns(swap(kv_own, "sp", member) if member else kv_own)
            if not merged:
                block.append(swap(kr_own, "sp", member) if member else kr_own)
            blocks.append(block)
    else:
        kr_blocks = lax.all_gather(kr_own, "sp")
        whole_rows = lax.all_gather(kv_own, "tp", axis=1, tiled=True)
        kv_blocks = lax.all_gather(whole_rows, "sp")
        blocks = [[kv, kr] for kv, kr in zip(kv_blocks, kr_blocks)]
        merged = False
    cq_pieces = columns(cq_cols)
    queries = call(
        functools.partial(query_kernel, len(cq_pieces)),
        jax.ShapeDtypeStruct((pairs, 2 * tok_count, LANES + group), bf16),
        [ids, *cq_pieces, q_gain[None, :], query_up_weight, cosine, sine_of],
        scratch=[VMEM((tok_count, q_gain.shape[0]), bf16)],
    )
    held = [
        jax.ShapeDtypeStruct((head_count, tok_count, 1), jnp.float32),
        jax.ShapeDtypeStruct((head_count, tok_count, 1), jnp.float32),
        jax.ShapeDtypeStruct((head_count, tok_count, LANES), jnp.float32),
    ]
    state = []
    chunk = 2
    for begin in range(0, sp_count, chunk):
        part = blocks[begin : begin + chunk]
        last = begin + chunk >= sp_count
        state = call(
            functools.partial(
                attend_kernel,
                [len(block) - (0 if merged else 1) for block in part],
                tok_count,
                seg_rows,
                merged,
                begin == 0,
                last,
            ),
            jax.ShapeDtypeStruct((tok_count, head_count * VALUE_DIM), bf16) if last else held,
            [
                ids,
                queries,
                context_bias,
                latent_norm_gain[None, :],
                key_up_weight,
                value_up_weight,
                *[piece for block in part for piece in block],
                *state,
            ],
            smem=(0, 2),
            scratch=[
                VMEM((seg_rows, latent_norm_gain.shape[0]), bf16),
                VMEM((len(part) * seg_rows, head_count * PLAIN_QK_DIM), bf16),
                VMEM((len(part) * seg_rows, head_count * VALUE_DIM), bf16),
                VMEM((len(part) * seg_rows, group), bf16),
            ],
            mib=24,
        )
    att_pieces = spread(state)
    out_cols = w_out.shape[1]
    proj_cols = call(
        functools.partial(out_kernel, tp_count),
        jax.ShapeDtypeStruct((tok_count, out_cols), bf16),
        [ids, *att_pieces, w_out],
    )
    proj_pieces = return_rows(proj_cols, ids)
    return call(
        functools.partial(final_kernel, tp_count, tp_count),
        jax.ShapeDtypeStruct((own_rows, width), bf16),
        [ids, *proj_pieces, *mod_pieces, latents],
    )


def solution(mesh):
    in_specs = (
        P(("grp", "sp", "tp"), None),
        P("grp", "sp"),
        P(("grp", "sp"), None),
        P("sp", "tp"),
        P("sp", "tp"),
        P("sp", "tp"),
        P(None, "tp"),
        P(None, "tp"),
        P(),
        P(),
        P(),
        P(None, "tp"),
        P(None, "tp"),
        P(None, "tp"),
        P("tp"),
        P(None, "tp"),
    )
    out_specs = P(("grp", "sp", "tp"), None)
    return jax.shard_map(
        on_device, mesh=mesh, in_specs=in_specs, out_specs=out_specs, check_vma=False
    )
```

```python
import functools

import jax
import jax.numpy as jnp
from jax import lax
from jax.experimental import pallas as pl
from jax.experimental.pallas import tpu as pltpu
from jax.sharding import PartitionSpec as P


PLAIN_QK_DIM = 64
ROTARY_DIM = 32
VALUE_DIM = 64
GRID_W = 64
LANES = 128
LOG2E = 1.4426950408889634

EPSILON = 1e-06


VMEM = pltpu.VMEM
SMEM = pltpu.SMEM


def in_vmem():
    return pl.BlockSpec(memory_space=VMEM)


def in_smem():
    return pl.BlockSpec(memory_space=SMEM)


def f32_dot(a, b):
    return jnp.dot(a, b, preferred_element_type=jnp.float32)


def swap(value, axis, bit):
    count = lax.axis_size(axis)
    return lax.ppermute(value, axis, [(i, i ^ bit) for i in range(count)])


def is_small(count):
    return count <= 4


def tp_bits(count):
    bits = []
    bit = 2
    while bit < count:
        bits.append(bit)
        bit *= 2
    if count > 1:
        bits.append(1)
    return bits


def spread(value, axis="tp"):
    if not is_small(lax.axis_size(axis)):
        return list(lax.all_gather(value, axis))
    got = {0: value}
    for bit in tp_bits(lax.axis_size(axis)):
        for member in list(got):
            got[member ^ bit] = swap(got[member], axis, bit)
    return [got[member] for member in range(len(got))]


def add_up(value, axis):
    count = lax.axis_size(axis)
    if not is_small(count):
        return lax.psum(value, axis)
    bit = 1
    while bit < count:
        value = value + swap(value, axis, bit)
        bit *= 2
    return value


def place(pieces, ids, axis):
    width = pieces[0].shape[axis]
    shape = list(pieces[0].shape)
    shape[axis] = width * len(pieces)
    whole = jnp.zeros(shape, pieces[0].dtype)
    for member, piece in enumerate(pieces):
        whole = lax.dynamic_update_slice_in_dim(whole, piece, ids[member] * width, axis)
    return whole


def turn_tables(positions, lanes):
    freq_count = ROTARY_DIM // 4
    inverse = 10000.0 ** (-jnp.arange(freq_count, dtype=jnp.float32) / freq_count)
    grid_row = (positions // GRID_W).astype(jnp.float32)
    grid_col = (positions % GRID_W).astype(jnp.float32)
    cosines, sines = [], []
    for coordinate in (grid_row, grid_col):
        angles = coordinate[:, None] * inverse[None, :]
        cosine, sine_of = jnp.cos(angles), jnp.sin(angles)
        cosines += [cosine, cosine]
        sines += [-sine_of, sine_of]
    cosine = jnp.concatenate(cosines, axis=1)
    sine_of = jnp.concatenate(sines, axis=1)
    repeat = lanes // ROTARY_DIM
    return jnp.tile(cosine, (1, repeat)), jnp.tile(sine_of, (1, repeat))


def turn(values, cosine, sine_of):
    freq_count = ROTARY_DIM // 4
    lanes = values.shape[1]
    lane = lax.broadcasted_iota(jnp.int32, values.shape, 1)
    first = (lane % (2 * freq_count)) < freq_count
    partner = jnp.where(
        first, pltpu.roll(values, lanes - freq_count, 1), pltpu.roll(values, freq_count, 1)
    )
    return values * cosine + partner * sine_of


def gather_rows(scratch, ids, pieces):
    width = pieces[0].shape[1]
    for number, piece in enumerate(pieces):
        scratch[:, pl.ds(pl.multiple_of(ids[number] * width, LANES), width)] = piece[...]


def normalize(values):
    center = values - jnp.mean(values, axis=-1, keepdims=True)
    spread_of = jnp.mean(center * center, axis=-1, keepdims=True)
    return center * lax.rsqrt(spread_of + EPSILON)


def weights_kernel(wq_hbm, wk_ref, rope_ref, wq_ref, wkr_ref, sem):
    copy = pltpu.make_async_copy(wq_hbm, wq_ref, sem)
    copy.start()
    wkr_ref[:, LANES:] = wk_ref[...]
    copies = (
        lax.broadcasted_iota(jnp.int32, (ROTARY_DIM, LANES), 0)
        == lax.broadcasted_iota(jnp.int32, (ROTARY_DIM, LANES), 1) % ROTARY_DIM
    ).astype(jnp.bfloat16)
    wkr_ref[:, :LANES] = lax.dot_general(
        rope_ref[...], copies, (((0,), (0,)), ((), ())), preferred_element_type=jnp.float32
    ).astype(jnp.bfloat16)
    copy.wait()


def early_kernel(count, *refs):
    for source, out_ref in zip(refs[:count], refs[count:]):
        for row in range(0, source.shape[0], 16):
            values = source[row : row + 16, :].astype(jnp.float32)
            out_ref[row : row + 16, :] = normalize(values)


def fetch_kernel(wq_ref, wk_hbm, wv_ref, wo_hbm, wqt_ref, wk_ref, wvt_ref, wo_ref, sems):
    copies = [
        pltpu.make_async_copy(wk_hbm, wk_ref, sems.at[0]),
        pltpu.make_async_copy(wo_hbm, wo_ref, sems.at[1]),
    ]
    for copy in copies:
        copy.start()
    wqt_ref[...] = wq_ref[...].astype(jnp.float32).T.astype(jnp.bfloat16)
    wvt_ref[...] = wv_ref[...].astype(jnp.float32).T.astype(jnp.bfloat16)
    for copy in copies:
        copy.wait()


def down_kernel(early_rows, late_rows, mod_count, tok_count, merged, *refs):
    ids, offsets = refs[:2]
    refs = refs[2:]
    early, refs = refs[: len(early_rows)], refs[len(early_rows) :]
    late, refs = refs[: len(late_rows)], refs[len(late_rows) :]
    pieces, refs = refs[:mod_count], refs[mod_count:]
    ctx_ref, wq_ref, wkr_ref, cos_ref, sin_ref = refs[:5]
    cq_ref, kv_ref, kr_ref, ha_ref, hb_ref, mod_ref, both_ref = refs[5:]
    step = 16
    gather_rows(mod_ref, ids, pieces)

    def modulate(source, target, base, rows, is_ctx, is_normed):
        shift_by = mod_ref[is_ctx : is_ctx + 1, :]
        scale_by = 1.0 + mod_ref[2 + is_ctx : 3 + is_ctx, :]
        for row in range(0, rows, step):
            values = source[row : row + step, :]
            if not is_normed:
                values = normalize(values.astype(jnp.float32))
            target[base + row : base + row + step, :] = (values * scale_by + shift_by).astype(
                jnp.bfloat16
            )

    def multiply(source, rows_of, first, with_ctx):
        cq = f32_dot(source[...], wq_ref[...])
        both = f32_dot(source[...], wkr_ref[...])
        base = 0
        for number, rows in enumerate(rows_of):
            start = pl.multiple_of(offsets[first + number] * rows, 16)
            cq_ref[pl.ds(start, rows), :] = cq[base : base + rows].astype(jnp.bfloat16)
            both_ref[pl.ds(start, rows), :] = both[base : base + rows]
            base += rows
        if with_ctx:
            both_ref[tok_count:, :] = both[base:]

    base = 0
    for source, rows in zip(early, early_rows):
        modulate(source, ha_ref, base, rows, 0, True)
        base += rows
    modulate(ctx_ref, ha_ref, base, ctx_ref.shape[0], 1, True)
    multiply(ha_ref, early_rows, 0, True)
    base = 0
    for source, rows in zip(late, late_rows):
        modulate(source, hb_ref, base, rows, 0, False)
        base += rows
    multiply(hb_ref, late_rows, len(early_rows), False)
    seg = both_ref.shape[0]
    kv_ref[:seg, :] = both_ref[:, LANES:].astype(jnp.bfloat16)
    turned = turn(both_ref[:, :LANES], cos_ref[...], sin_ref[...]).astype(jnp.bfloat16)
    if merged:
        both_ref[:, :LANES] = turned.astype(jnp.float32)
        quarter = seg // mod_count
        sub = quarter // (LANES // ROTARY_DIM)
        lane = lax.broadcasted_iota(jnp.int32, (sub, LANES), 1)
        packed = None
        for part in range(LANES // ROTARY_DIM):
            start = pl.multiple_of(ids[0] * quarter + part * sub, 8)
            rows = both_ref[pl.ds(start, sub), :LANES]
            rows = jnp.where(lane // ROTARY_DIM == part, rows, 0.0)
            packed = rows if packed is None else packed + rows
        kv_ref[seg:, :] = packed.astype(jnp.bfloat16)
        kr_ref[...] = jnp.zeros_like(kr_ref)
    else:
        kr_ref[...] = turned


def normed_into(scratch, ids, pieces, gain_ref):
    width = pieces[0].shape[1]
    rows = scratch.shape[0]
    total = width * len(pieces)
    squares = None
    for piece in pieces:
        values = piece[:rows, :].astype(jnp.float32)
        part = jnp.sum(values * values, axis=-1, keepdims=True)
        squares = part if squares is None else squares + part
    factor = lax.rsqrt(squares / total + EPSILON)
    for number, piece in enumerate(pieces):
        if len(pieces) == 1:
            where = slice(None)
        else:
            where = pl.ds(pl.multiple_of(ids[number] * width, LANES), width)
        gained = piece[:rows, :].astype(jnp.float32) * factor * gain_ref[:, where]
        scratch[:, where] = gained.astype(jnp.bfloat16)


def query_kernel(count, *refs):
    ids = refs[0]
    pieces = refs[1 : 1 + count]
    gain_ref, w_ref, table_ref, q_ref, scratch = refs[1 + count :]
    normed_into(scratch, ids, pieces, gain_ref)
    rows = scratch.shape[0]
    raw = lax.dot_general(
        w_ref[...], scratch[...], (((1,), (1,)), ((), ())), preferred_element_type=jnp.float32
    )
    freq_count = ROTARY_DIM // 4
    tables = [table_ref[i * freq_count : (i + 1) * freq_count, :] for i in range(4)]
    span = PLAIN_QK_DIM + ROTARY_DIM
    q_ref[...] = jnp.zeros_like(q_ref)
    for head in range(2 * q_ref.shape[0]):
        half = head % 2
        lanes = slice(half * rows, (half + 1) * rows)
        start = head * span
        q_ref[head // 2, half * PLAIN_QK_DIM : (half + 1) * PLAIN_QK_DIM, lanes] = raw[
            start : start + PLAIN_QK_DIM
        ].astype(jnp.bfloat16)
        start += PLAIN_QK_DIM
        parts = [raw[start + i * freq_count : start + (i + 1) * freq_count] for i in range(4)]
        turned = []
        for axis in range(2):
            low, high = parts[2 * axis : 2 * axis + 2]
            cosine, sine_of = tables[2 * axis : 2 * axis + 2]
            turned += [low * cosine - high * sine_of, low * sine_of + high * cosine]
        q_ref[head // 2, LANES : LANES + ROTARY_DIM, lanes] = jnp.concatenate(
            turned, axis=0
        ).astype(jnp.bfloat16)


def fold_rows(values):
    return jnp.sum(values.reshape(-1, 8, values.shape[1]), axis=0)


def attend_kernel(counts, tok_keys, seg, merged, first, last, *refs):
    ids, bias_ref, q_ref, gain_ref, wk_ref, wv_ref = refs[:6]
    refs = refs[6:]
    blocks = []
    for count in counts:
        blocks.append(refs[: count + (0 if merged else 1)])
        refs = refs[len(blocks[-1]) :]
    if not first:
        state_in, refs = refs[:3], refs[3:]
    if last:
        out_ref, refs = refs[0], refs[1:]
    else:
        state_out, refs = refs[:3], refs[3:]
    scratch, k_ref, v_ref, r_ref = refs
    pairs, _, lanes = q_ref.shape
    rows = lanes // 2
    for number, block in enumerate(blocks):
        pieces = block if merged else block[:-1]
        base = number * seg
        normed_into(scratch, ids, pieces, gain_ref)
        k_ref[base : base + seg, :] = f32_dot(scratch[...], wk_ref[...]).astype(jnp.bfloat16)
        v_ref[number] = lax.dot_general(
            wv_ref[...], scratch[...], (((1,), (1,)), ((), ())), preferred_element_type=jnp.float32
        ).astype(jnp.bfloat16)
        if merged:
            quarter = seg // len(pieces)
            sub = quarter // (LANES // ROTARY_DIM)
            for member, piece in enumerate(pieces):
                packed = piece[seg:, :].astype(jnp.float32)
                for part in range(LANES // ROTARY_DIM):
                    moved = pltpu.roll(packed, (-part * ROTARY_DIM) % LANES, 1) if part else packed
                    start = pl.multiple_of(base + ids[member] * quarter + part * sub, 16)
                    r_ref[pl.ds(start, sub), :] = moved.astype(jnp.bfloat16)
        else:
            r_ref[base : base + seg, :] = block[-1][...]
    score_scale = (PLAIN_QK_DIM + ROTARY_DIM) ** (-0.5) * LOG2E
    lane = lax.broadcasted_iota(jnp.int32, (1, lanes), 1)
    for pair in range(pairs):
        span = slice(pair * LANES, (pair + 1) * LANES)
        bias = jnp.where(lane < rows, bias_ref[2 * pair], bias_ref[2 * pair + 1]) * LOG2E
        top = total = acc = None
        if not first:
            top = state_in[0][pair, :1, :]
            total, acc = state_in[1][pair], state_in[2][pair]
        for number in range(len(blocks)):
            base = number * seg
            key = jnp.concatenate(
                [k_ref[base : base + seg, span], r_ref[base : base + seg, :]], axis=1
            )
            scores = f32_dot(key, q_ref[pair])
            lat, ctx = scores[:tok_keys], scores[tok_keys:]
            peak = jnp.maximum(
                jnp.max(lat, axis=0, keepdims=True) * score_scale,
                jnp.max(ctx, axis=0, keepdims=True) * score_scale + bias,
            )
            new_top = peak if top is None else jnp.maximum(top, peak)
            e_lat = jnp.exp2(lat * score_scale - new_top)
            e_ctx = jnp.exp2(ctx * score_scale - (new_top - bias))
            part = fold_rows(e_lat) + fold_rows(e_ctx)
            weights = jnp.concatenate([e_lat, e_ctx], axis=0).astype(jnp.bfloat16)
            both = f32_dot(v_ref[number, span, :], weights)
            gathered = jnp.concatenate([both[:VALUE_DIM, :rows], both[VALUE_DIM:, rows:]], axis=0)
            if top is None:
                total, acc = part, gathered
            else:
                rescale = jnp.exp2(top - new_top)
                total = total * rescale + part
                acc = gathered + jnp.concatenate(
                    [acc[:VALUE_DIM] * rescale[:, :rows], acc[VALUE_DIM:] * rescale[:, rows:]],
                    axis=0,
                )
            top = new_top
        if last:
            total = jnp.sum(total, axis=0, keepdims=True)
            done = jnp.concatenate(
                [acc[:VALUE_DIM] / total[:, :rows], acc[VALUE_DIM:] / total[:, rows:]], axis=0
            )
            out_ref[:, span] = done.T.astype(jnp.bfloat16)
        else:
            state_out[0][pair] = jnp.broadcast_to(top, (8, lanes))
            state_out[1][pair] = total
            state_out[2][pair] = acc


def out_kernel(count, parts, *refs):
    ids = refs[0]
    pieces = refs[1 : 1 + count]
    w_ref = refs[1 + count]
    outs = refs[2 + count : 2 + count + parts]
    depth = pieces[0].shape[1]
    total = None
    for number, piece in enumerate(pieces):
        rows = pl.ds(pl.multiple_of(ids[number] * depth, LANES), depth)
        part = f32_dot(piece[...], w_ref[rows, :])
        total = part if total is None else total + part
    if parts == 1:
        outs[0][...] = total.astype(jnp.bfloat16)
        return
    scratch = refs[2 + count + parts]
    scratch[...] = total
    rows = outs[0].shape[0]
    for number, out_ref in enumerate(outs):
        start = pl.multiple_of(ids[number] * rows, 8)
        out_ref[...] = scratch[pl.ds(start, rows), :].astype(jnp.bfloat16)


def final_kernel(count, mod_count, *refs):
    ids = refs[0]
    pieces = refs[1 : 1 + count]
    gates = refs[1 + count : 1 + count + mod_count]
    lat_ref, out_ref = refs[1 + count + mod_count :]
    width = pieces[0].shape[1]
    for number, (piece, gate) in enumerate(zip(pieces, gates)):
        span = pl.ds(pl.multiple_of(ids[number] * width, LANES), width)
        out_ref[:, span] = (
            lat_ref[:, span].astype(jnp.float32)
            + gate[gate.shape[0] - 1 :, :] * piece[...].astype(jnp.float32)
        ).astype(jnp.bfloat16)


def call(kernel, outs, operands, smem=(0,), hbm=(), scratch=(), mib=16):
    specs = []
    for place_of in range(len(operands)):
        if place_of in hbm:
            specs.append(pl.BlockSpec(memory_space=pl.ANY))
        else:
            specs.append(in_smem() if place_of in smem else in_vmem())
    many = isinstance(outs, (list, tuple))
    return pl.pallas_call(
        kernel,
        out_shape=outs,
        in_specs=specs,
        out_specs=[in_vmem() for _ in outs] if many else in_vmem(),
        scratch_shapes=list(scratch),
        compiler_params=pltpu.CompilerParams(vmem_limit_bytes=mib * 1024 * 1024),
    )(*operands)


def on_device(
    latents,
    conditions,
    context,
    w_shift,
    w_scale,
    w_gate,
    w_qdown,
    w_kvdown,
    w_rope,
    q_gain,
    latent_norm_gain,
    query_up_weight,
    key_up_weight,
    value_up_weight,
    context_bias,
    w_out,
):
    tp_count = lax.axis_size("tp")
    sp_count = lax.axis_size("sp")
    tp_index = lax.axis_index("tp")
    sp_index = lax.axis_index("sp")
    own_rows, width = latents.shape
    tok_count = own_rows * tp_count
    ctx_rows = context.shape[0]
    seg_rows = tok_count + ctx_rows
    ids = jnp.arange(tp_count, dtype=jnp.int32)
    if is_small(tp_count):
        ids = jnp.bitwise_xor(tp_index, ids)
    bf16 = jnp.bfloat16

    small = is_small(tp_count)
    shape_of = jax.ShapeDtypeStruct

    lat_blocks = spread(latents)
    cond_act = jax.nn.silu(conditions).astype(bf16)
    partial_mod = jnp.concatenate(
        [f32_dot(cond_act, w_shift), f32_dot(cond_act, w_scale), f32_dot(cond_act[0:1], w_gate)],
        axis=0,
    )
    mod_pieces = spread(add_up(partial_mod, "sp"))

    head_count = query_up_weight.shape[1] // (PLAIN_QK_DIM + ROTARY_DIM)
    pairs = head_count // 2
    q_pos = sp_index * tok_count + jnp.arange(tok_count, dtype=jnp.int32)
    cosine, sine_of = turn_tables(q_pos, LANES)
    k_cosine = jnp.concatenate([cosine, jnp.ones((ctx_rows, LANES), jnp.float32)], axis=0)
    k_sine = jnp.concatenate([sine_of, jnp.zeros((ctx_rows, LANES), jnp.float32)], axis=0)
    freq = ROTARY_DIM // 4
    q_table = jnp.concatenate(
        [
            cosine[:, :freq],
            sine_of[:, freq : 2 * freq],
            cosine[:, 2 * freq : 3 * freq],
            sine_of[:, 3 * freq : 4 * freq],
        ],
        axis=1,
    ).T
    kv_cols = w_kvdown.shape[1]
    q_cols = w_qdown.shape[1]

    w_q, w_kr = call(
        weights_kernel,
        [shape_of(w_qdown.shape, bf16), shape_of((width, LANES + kv_cols), bf16)],
        [w_qdown, w_kvdown, w_rope.T],
        smem=(),
        hbm=(0,),
        scratch=[pltpu.SemaphoreType.DMA],
    )
    block_ids = ids
    if own_rows % 16 or not small:
        lat_blocks = [place(lat_blocks, ids, 0)]
        block_ids = jnp.zeros((1,), jnp.int32)
        order = [0]
    else:
        order = [0, 1] + list(range(2, tp_count)) if tp_count > 1 else [0]
    early_of = [lat_blocks[member] for member in order[:2]] if len(order) > 2 else []
    late_of = [lat_blocks[member] for member in order[len(early_of) :]]
    normed = call(
        functools.partial(early_kernel, len(early_of) + 1),
        [shape_of(value.shape, jnp.float32) for value in [*early_of, context]],
        [*early_of, context],
        smem=(),
        mib=12,
    )
    w_qt, w_k, w_vt, w_o = call(
        fetch_kernel,
        [
            shape_of(query_up_weight.shape[::-1], bf16),
            shape_of(key_up_weight.shape, bf16),
            shape_of(value_up_weight.shape[::-1], bf16),
            shape_of(w_out.shape, bf16),
        ],
        [query_up_weight, key_up_weight, value_up_weight, w_out],
        smem=(),
        hbm=(1, 3),
        scratch=[pltpu.SemaphoreType.DMA((2,))],
    )
    merged = (
        kv_cols % LANES == 0
        and seg_rows % (16 * tp_count * LANES // ROTARY_DIM) == 0
        and small
        and is_small(sp_count)
    )
    extra = seg_rows // tp_count * ROTARY_DIM // LANES if merged else 0
    late_rows = [value.shape[0] for value in late_of]
    early_rows = [value.shape[0] for value in early_of]
    cq_cols, kv_own, kr_own = call(
        functools.partial(down_kernel, early_rows, late_rows, tp_count, tok_count, merged),
        [
            shape_of((tok_count, q_cols), bf16),
            shape_of((seg_rows + extra, kv_cols), bf16),
            shape_of((16 if merged else seg_rows, LANES), bf16),
        ],
        [
            ids,
            block_ids,
            *normed[:-1],
            *late_of,
            *mod_pieces,
            normed[-1],
            w_q,
            w_kr,
            k_cosine,
            k_sine,
        ],
        smem=(0, 1),
        scratch=[
            VMEM((sum(early_rows) + ctx_rows, width), bf16),
            VMEM((sum(late_rows), width), bf16),
            VMEM((5, width), jnp.float32),
            VMEM((seg_rows, LANES + kv_cols), jnp.float32),
        ],
        mib=16,
    )

    def columns(value):
        pieces = spread(value)
        if value.shape[1] % LANES:
            return [place(pieces, ids, 1)]
        return pieces

    if is_small(sp_count):
        blocks = []
        for member in range(sp_count):
            moved = swap(kv_own, "sp", member) if member else kv_own
            block = columns(moved)
            if not merged:
                block.append(swap(kr_own, "sp", member) if member else kr_own)
            blocks.append(block)
    else:
        kr_blocks = lax.all_gather(kr_own, "sp")
        whole_rows = lax.all_gather(kv_own, "tp", axis=1, tiled=True)
        kv_blocks = lax.all_gather(whole_rows, "sp")
        blocks = [[kv, kr] for kv, kr in zip(kv_blocks, kr_blocks)]
    cq_pieces = columns(cq_cols)
    queries = call(
        functools.partial(query_kernel, len(cq_pieces)),
        shape_of((pairs, 2 * LANES, 2 * tok_count), bf16),
        [ids, *cq_pieces, q_gain[None, :], w_qt, q_table],
        scratch=[VMEM((tok_count, q_gain.shape[0]), bf16)],
    )
    held = [
        shape_of((pairs, 8, 2 * tok_count), jnp.float32),
        shape_of((pairs, 8, 2 * tok_count), jnp.float32),
        shape_of((pairs, LANES, tok_count), jnp.float32),
    ]
    state = []
    begin = 0
    while begin < sp_count:
        part = blocks[begin : begin + (1 if begin < 2 else 2)]
        first, last = begin == 0, begin + len(part) >= sp_count
        state = call(
            functools.partial(
                attend_kernel,
                [len(block) - (0 if merged else 1) for block in part],
                tok_count,
                seg_rows,
                merged,
                first,
                last,
            ),
            shape_of((tok_count, head_count * VALUE_DIM), bf16) if last else held,
            [
                ids,
                context_bias,
                queries,
                latent_norm_gain[None, :],
                w_k,
                w_vt,
                *[piece for block in part for piece in block],
                *state,
            ],
            smem=(0, 1),
            scratch=[
                VMEM((seg_rows, latent_norm_gain.shape[0]), bf16),
                VMEM((len(part) * seg_rows, head_count * PLAIN_QK_DIM), bf16),
                VMEM((len(part), head_count * VALUE_DIM, seg_rows), bf16),
                VMEM((len(part) * seg_rows, LANES), bf16),
            ],
            mib=16,
        )
        begin += len(part)
    att_pieces = spread(state)
    out_cols = w_out.shape[1]
    parts = tp_count if small and own_rows % 8 == 0 else 1
    proj = call(
        functools.partial(out_kernel, tp_count, parts),
        [shape_of((tok_count // parts, out_cols), bf16) for _ in range(parts)],
        [ids, *att_pieces, w_o],
        scratch=[VMEM((tok_count, out_cols), jnp.float32)] if parts > 1 else [],
    )
    if parts > 1:
        proj_pieces = [
            swap(value, "tp", member) if member else value
            for member, value in enumerate(proj)
        ]
    else:
        by_owner = proj[0].reshape(tp_count, own_rows, out_cols)
        proj_pieces = list(lax.all_to_all(by_owner, "tp", 0, 0))
        if small:
            proj_pieces = [
                lax.dynamic_index_in_dim(jnp.stack(proj_pieces), ids[member], 0, False)
                for member in range(tp_count)
            ]
    return call(
        functools.partial(final_kernel, tp_count, tp_count),
        shape_of((own_rows, width), bf16),
        [ids, *proj_pieces, *mod_pieces, latents],
    )


def solution(mesh):
    in_specs = (
        P(("grp", "sp", "tp"), None),
        P("grp", "sp"),
        P(("grp", "sp"), None),
        P("sp", "tp"),
        P("sp", "tp"),
        P("sp", "tp"),
        P(None, "tp"),
        P(None, "tp"),
        P(),
        P(),
        P(),
        P(None, "tp"),
        P(None, "tp"),
        P(None, "tp"),
        P("tp"),
        P(None, "tp"),
    )
    out_specs = P(("grp", "sp", "tp"), None)
    return jax.shard_map(
        on_device, mesh=mesh, in_specs=in_specs, out_specs=out_specs, check_vma=False
    )
```

```python
import functools

import jax
import jax.numpy as jnp
from jax import lax
from jax.experimental import pallas as pl
from jax.experimental.pallas import tpu as pltpu
from jax.sharding import PartitionSpec as P


PLAIN_QK_DIM = 64
ROTARY_DIM = 32
VALUE_DIM = 64
GRID_W = 64
LANES = 128
LOG2E = 1.4426950408889634

EPSILON = 1e-06


VMEM = pltpu.VMEM
SMEM = pltpu.SMEM


def in_vmem():
    return pl.BlockSpec(memory_space=VMEM)


def in_smem():
    return pl.BlockSpec(memory_space=SMEM)


def f32_dot(a, b):
    return jnp.dot(a, b, preferred_element_type=jnp.float32)


def swap(value, axis, bit):
    count = lax.axis_size(axis)
    return lax.ppermute(value, axis, [(i, i ^ bit) for i in range(count)])


def is_small(count):
    return count <= 4


def tp_bits(count):
    bits = []
    bit = 2
    while bit < count:
        bits.append(bit)
        bit *= 2
    if count > 1:
        bits.append(1)
    return bits


def spread(value, axis="tp"):
    if not is_small(lax.axis_size(axis)):
        return list(lax.all_gather(value, axis))
    got = {0: value}
    for bit in tp_bits(lax.axis_size(axis)):
        for member in list(got):
            got[member ^ bit] = swap(got[member], axis, bit)
    return [got[member] for member in range(len(got))]


def add_up(value, axis):
    count = lax.axis_size(axis)
    if not is_small(count):
        return lax.psum(value, axis)
    bit = 1
    while bit < count:
        value = value + swap(value, axis, bit)
        bit *= 2
    return value


def place(pieces, ids, axis):
    width = pieces[0].shape[axis]
    shape = list(pieces[0].shape)
    shape[axis] = width * len(pieces)
    whole = jnp.zeros(shape, pieces[0].dtype)
    for member, piece in enumerate(pieces):
        whole = lax.dynamic_update_slice_in_dim(whole, piece, ids[member] * width, axis)
    return whole


def angles(position, frequency, use_column):
    freq_count = ROTARY_DIM // 4
    inverse = jnp.zeros(frequency.shape, jnp.float32)
    for number in range(freq_count):
        inverse = jnp.where(
            frequency == number, jnp.float32(10000.0 ** (-number / freq_count)), inverse
        )
    coordinate = jnp.where(use_column, position % GRID_W, position // GRID_W)
    return coordinate.astype(jnp.float32) * inverse


def tables_kernel(tok_count, info, cos_ref, sin_ref, table_ref):
    freq_count = ROTARY_DIM // 4
    start = info[0] * tok_count
    shape = cos_ref.shape
    row = lax.broadcasted_iota(jnp.int32, shape, 0)
    lane = lax.broadcasted_iota(jnp.int32, shape, 1)
    angle = angles(start + row, lane % freq_count, (lane // (2 * freq_count)) % 2 == 1)
    is_lat = row < tok_count
    cos_ref[...] = jnp.where(is_lat, jnp.cos(angle), 1.0)
    sine_of = jnp.where((lane // freq_count) % 2 == 0, -jnp.sin(angle), jnp.sin(angle))
    sin_ref[...] = jnp.where(is_lat, sine_of, 0.0)
    shape = table_ref.shape
    row = lax.broadcasted_iota(jnp.int32, shape, 0)
    lane = lax.broadcasted_iota(jnp.int32, shape, 1)
    angle = angles(start + lane, row % freq_count, row // (2 * freq_count) == 1)
    table_ref[...] = jnp.where((row // freq_count) % 2 == 0, jnp.cos(angle), jnp.sin(angle))


def turn(values, cosine, sine_of):
    freq_count = ROTARY_DIM // 4
    lanes = values.shape[1]
    lane = lax.broadcasted_iota(jnp.int32, values.shape, 1)
    first = (lane % (2 * freq_count)) < freq_count
    partner = jnp.where(
        first, pltpu.roll(values, lanes - freq_count, 1), pltpu.roll(values, freq_count, 1)
    )
    return values * cosine + partner * sine_of


class Members:
    def __init__(self, info):
        self.info = info

    def __getitem__(self, member):
        return self.info[1 + member]


def member_ids(info, count):
    return Members(info) if is_small(count) else list(range(count))


def aligned(value, step):
    return value if isinstance(value, int) else pl.multiple_of(value, step)


def gather_rows(scratch, ids, pieces):
    width = pieces[0].shape[1]
    for number, piece in enumerate(pieces):
        scratch[:, pl.ds(aligned(ids[number] * width, LANES), width)] = piece[...]


def normalize(values):
    center = values - jnp.mean(values, axis=-1, keepdims=True)
    spread_of = jnp.mean(center * center, axis=-1, keepdims=True)
    return center * lax.rsqrt(spread_of + EPSILON)


def weights_kernel(wq_hbm, wk_ref, rope_ref, wq_ref, wkr_ref, sem):
    copy = pltpu.make_async_copy(wq_hbm, wq_ref, sem)
    copy.start()
    wkr_ref[:, LANES:] = wk_ref[...]
    copies = (
        lax.broadcasted_iota(jnp.int32, (ROTARY_DIM, LANES), 0)
        == lax.broadcasted_iota(jnp.int32, (ROTARY_DIM, LANES), 1) % ROTARY_DIM
    ).astype(jnp.bfloat16)
    wkr_ref[:, :LANES] = lax.dot_general(
        rope_ref[...], copies, (((0,), (0,)), ((), ())), preferred_element_type=jnp.float32
    ).astype(jnp.bfloat16)
    copy.wait()


def early_kernel(count, *refs):
    for source, out_ref in zip(refs[:count], refs[count:]):
        for row in range(0, source.shape[0], 16):
            values = source[row : row + 16, :].astype(jnp.float32)
            out_ref[row : row + 16, :] = normalize(values)


def fetch_kernel(wq_ref, wk_hbm, wv_ref, wo_hbm, wqt_ref, wk_ref, wvt_ref, wo_ref, sems):
    copies = [
        pltpu.make_async_copy(wk_hbm, wk_ref, sems.at[0]),
        pltpu.make_async_copy(wo_hbm, wo_ref, sems.at[1]),
    ]
    for copy in copies:
        copy.start()
    wqt_ref[...] = wq_ref[...].astype(jnp.float32).T.astype(jnp.bfloat16)
    wvt_ref[...] = wv_ref[...].astype(jnp.float32).T.astype(jnp.bfloat16)
    for copy in copies:
        copy.wait()


def down_kernel(early_rows, late_rows, mod_count, tok_count, merged, info, *refs):
    ids = member_ids(info, mod_count)
    offsets = [0] if len(early_rows) + len(late_rows) == 1 else ids
    early, refs = refs[: len(early_rows)], refs[len(early_rows) :]
    late, refs = refs[: len(late_rows)], refs[len(late_rows) :]
    pieces, refs = refs[:mod_count], refs[mod_count:]
    ctx_ref, wq_ref, wkr_ref, cos_ref, sin_ref = refs[:5]
    cq_ref, kv_ref, kr_ref, ha_ref, hb_ref, mod_ref, both_ref = refs[5:]
    step = 16
    gather_rows(mod_ref, ids, pieces)

    def modulate(source, target, base, rows, is_ctx, is_normed):
        shift_by = mod_ref[is_ctx : is_ctx + 1, :]
        scale_by = 1.0 + mod_ref[2 + is_ctx : 3 + is_ctx, :]
        for row in range(0, rows, step):
            values = source[row : row + step, :]
            if not is_normed:
                values = normalize(values.astype(jnp.float32))
            target[base + row : base + row + step, :] = (values * scale_by + shift_by).astype(
                jnp.bfloat16
            )

    def multiply(source, rows_of, first, with_ctx):
        cq = f32_dot(source[...], wq_ref[...])
        both = f32_dot(source[...], wkr_ref[...])
        base = 0
        for number, rows in enumerate(rows_of):
            start = aligned(offsets[first + number] * rows, 16)
            cq_ref[pl.ds(start, rows), :] = cq[base : base + rows].astype(jnp.bfloat16)
            both_ref[pl.ds(start, rows), :] = both[base : base + rows]
            base += rows
        if with_ctx:
            both_ref[tok_count:, :] = both[base:]

    base = 0
    for source, rows in zip(early, early_rows):
        modulate(source, ha_ref, base, rows, 0, True)
        base += rows
    modulate(ctx_ref, ha_ref, base, ctx_ref.shape[0], 1, True)
    multiply(ha_ref, early_rows, 0, True)
    base = 0
    for source, rows in zip(late, late_rows):
        modulate(source, hb_ref, base, rows, 0, False)
        base += rows
    multiply(hb_ref, late_rows, len(early_rows), False)
    seg = both_ref.shape[0]
    kv_ref[:seg, :] = both_ref[:, LANES:].astype(jnp.bfloat16)
    turned = turn(both_ref[:, :LANES], cos_ref[...], sin_ref[...]).astype(jnp.bfloat16)
    if merged:
        both_ref[:, :LANES] = turned.astype(jnp.float32)
        quarter = seg // mod_count
        sub = quarter // (LANES // ROTARY_DIM)
        lane = lax.broadcasted_iota(jnp.int32, (sub, LANES), 1)
        packed = None
        for part in range(LANES // ROTARY_DIM):
            start = aligned(ids[0] * quarter + part * sub, 8)
            rows = both_ref[pl.ds(start, sub), :LANES]
            rows = jnp.where(lane // ROTARY_DIM == part, rows, 0.0)
            packed = rows if packed is None else packed + rows
        kv_ref[seg:, :] = packed.astype(jnp.bfloat16)
        kr_ref[...] = jnp.zeros_like(kr_ref)
    else:
        kr_ref[...] = turned


def normed_into(scratch, ids, pieces, gain_ref):
    width = pieces[0].shape[1]
    rows = scratch.shape[0]
    total = width * len(pieces)
    squares = None
    for piece in pieces:
        values = piece[:rows, :].astype(jnp.float32)
        part = jnp.sum(values * values, axis=-1, keepdims=True)
        squares = part if squares is None else squares + part
    factor = lax.rsqrt(squares / total + EPSILON)
    for number, piece in enumerate(pieces):
        if len(pieces) == 1:
            where = slice(None)
        else:
            where = pl.ds(aligned(ids[number] * width, LANES), width)
        gained = piece[:rows, :].astype(jnp.float32) * factor * gain_ref[:, where]
        scratch[:, where] = gained.astype(jnp.bfloat16)


def query_kernel(count, info, *refs):
    ids = member_ids(info, count)
    pieces = refs[:count]
    gain_ref, w_ref, table_ref, q_ref, scratch = refs[count:]
    normed_into(scratch, ids, pieces, gain_ref)
    rows = scratch.shape[0]
    raw = lax.dot_general(
        w_ref[...], scratch[...], (((1,), (1,)), ((), ())), preferred_element_type=jnp.float32
    )
    freq_count = ROTARY_DIM // 4
    tables = [table_ref[i * freq_count : (i + 1) * freq_count, :] for i in range(4)]
    span = PLAIN_QK_DIM + ROTARY_DIM
    q_ref[...] = jnp.zeros_like(q_ref)
    for head in range(2 * q_ref.shape[0]):
        half = head % 2
        lanes = slice(half * rows, (half + 1) * rows)
        start = head * span
        q_ref[head // 2, half * PLAIN_QK_DIM : (half + 1) * PLAIN_QK_DIM, lanes] = raw[
            start : start + PLAIN_QK_DIM
        ].astype(jnp.bfloat16)
        start += PLAIN_QK_DIM
        parts = [raw[start + i * freq_count : start + (i + 1) * freq_count] for i in range(4)]
        turned = []
        for axis in range(2):
            low, high = parts[2 * axis : 2 * axis + 2]
            cosine, sine_of = tables[2 * axis : 2 * axis + 2]
            turned += [low * cosine - high * sine_of, low * sine_of + high * cosine]
        q_ref[head // 2, LANES : LANES + ROTARY_DIM, lanes] = jnp.concatenate(
            turned, axis=0
        ).astype(jnp.bfloat16)


def fold_rows(values):
    return jnp.sum(values.reshape(-1, 8, values.shape[1]), axis=0)


def attend_kernel(counts, tok_keys, seg, merged, first, last, info, *refs):
    ids = member_ids(info, counts[0])
    bias_ref, q_ref, gain_ref, wk_ref, wv_ref = refs[:5]
    refs = refs[5:]
    blocks = []
    for count in counts:
        blocks.append(refs[: count + (0 if merged else 1)])
        refs = refs[len(blocks[-1]) :]
    if not first:
        state_in, refs = refs[:3], refs[3:]
    if last:
        out_ref, refs = refs[0], refs[1:]
    else:
        state_out, refs = refs[:3], refs[3:]
    scratch, k_ref, v_ref, r_ref = refs
    pairs, _, lanes = q_ref.shape
    rows = lanes // 2
    for number, block in enumerate(blocks):
        pieces = block if merged else block[:-1]
        base = number * seg
        rows_ref = scratch.at[number]
        normed_into(rows_ref, ids, pieces, gain_ref)
        k_ref[base : base + seg, :] = f32_dot(rows_ref[...], wk_ref[...]).astype(jnp.bfloat16)
        v_ref[number] = lax.dot_general(
            wv_ref[...], rows_ref[...], (((1,), (1,)), ((), ())), preferred_element_type=jnp.float32
        ).astype(jnp.bfloat16)
        if merged:
            quarter = seg // len(pieces)
            sub = quarter // (LANES // ROTARY_DIM)
            for member, piece in enumerate(pieces):
                packed = piece[seg:, :].astype(jnp.float32)
                for part in range(LANES // ROTARY_DIM):
                    moved = pltpu.roll(packed, (-part * ROTARY_DIM) % LANES, 1) if part else packed
                    start = aligned(base + ids[member] * quarter + part * sub, 16)
                    r_ref[pl.ds(start, sub), :] = moved.astype(jnp.bfloat16)
        else:
            r_ref[base : base + seg, :] = block[-1][...]
    score_scale = (PLAIN_QK_DIM + ROTARY_DIM) ** (-0.5) * LOG2E
    lane = lax.broadcasted_iota(jnp.int32, (1, lanes), 1)
    for pair in range(pairs):
        span = slice(pair * LANES, (pair + 1) * LANES)
        bias = jnp.where(lane < rows, bias_ref[2 * pair], bias_ref[2 * pair + 1]) * LOG2E
        top = total = acc = None
        if not first:
            top = state_in[0][pair, :1, :]
            total, acc = state_in[1][pair], state_in[2][pair]
        for number in range(len(blocks)):
            base = number * seg
            key = jnp.concatenate(
                [k_ref[base : base + seg, span], r_ref[base : base + seg, :]], axis=1
            )
            scores = f32_dot(key, q_ref[pair])
            lat, ctx = scores[:tok_keys], scores[tok_keys:]
            peak = jnp.maximum(
                jnp.max(lat, axis=0, keepdims=True) * score_scale,
                jnp.max(ctx, axis=0, keepdims=True) * score_scale + bias,
            )
            new_top = peak if top is None else jnp.maximum(top, peak)
            e_lat = jnp.exp2(lat * score_scale - new_top)
            e_ctx = jnp.exp2(ctx * score_scale - (new_top - bias))
            part = fold_rows(e_lat) + fold_rows(e_ctx)
            weights = jnp.concatenate([e_lat, e_ctx], axis=0).astype(jnp.bfloat16)
            both = f32_dot(v_ref[number, span, :], weights)
            gathered = jnp.concatenate([both[:VALUE_DIM, :rows], both[VALUE_DIM:, rows:]], axis=0)
            if top is None:
                total, acc = part, gathered
            else:
                rescale = jnp.exp2(top - new_top)
                total = total * rescale + part
                acc = gathered + jnp.concatenate(
                    [acc[:VALUE_DIM] * rescale[:, :rows], acc[VALUE_DIM:] * rescale[:, rows:]],
                    axis=0,
                )
            top = new_top
        if last:
            total = jnp.sum(total, axis=0, keepdims=True)
            done = jnp.concatenate(
                [acc[:VALUE_DIM] / total[:, :rows], acc[VALUE_DIM:] / total[:, rows:]], axis=0
            )
            out_ref[:, span] = done.T.astype(jnp.bfloat16)
        else:
            state_out[0][pair] = jnp.broadcast_to(top, (8, lanes))
            state_out[1][pair] = total
            state_out[2][pair] = acc


def out_kernel(count, parts, info, *refs):
    ids = member_ids(info, count)
    pieces = refs[:count]
    w_ref = refs[count]
    outs = refs[1 + count : 1 + count + parts]
    depth = pieces[0].shape[1]
    total = None
    for number, piece in enumerate(pieces):
        rows = pl.ds(aligned(ids[number] * depth, LANES), depth)
        part = f32_dot(piece[...], w_ref[rows, :])
        total = part if total is None else total + part
    if parts == 1:
        outs[0][...] = total.astype(jnp.bfloat16)
        return
    scratch = refs[1 + count + parts]
    scratch[...] = total
    rows = outs[0].shape[0]
    for number, out_ref in enumerate(outs):
        start = aligned(ids[number] * rows, 8)
        out_ref[...] = scratch[pl.ds(start, rows), :].astype(jnp.bfloat16)


def final_kernel(count, mod_count, info, *refs):
    ids = member_ids(info, count)
    pieces = refs[:count]
    gates = refs[count : count + mod_count]
    lat_ref, out_ref = refs[count + mod_count :]
    width = pieces[0].shape[1]
    for number, (piece, gate) in enumerate(zip(pieces, gates)):
        span = pl.ds(aligned(ids[number] * width, LANES), width)
        out_ref[:, span] = (
            lat_ref[:, span].astype(jnp.float32)
            + gate[gate.shape[0] - 1 :, :] * piece[...].astype(jnp.float32)
        ).astype(jnp.bfloat16)


def call(kernel, outs, operands, smem=(), hbm=(), scratch=(), mib=16):
    specs = []
    for place_of in range(len(operands)):
        if place_of in hbm:
            specs.append(pl.BlockSpec(memory_space=pl.ANY))
        else:
            specs.append(in_smem() if place_of in smem else in_vmem())
    many = isinstance(outs, (list, tuple))
    return pl.pallas_call(
        kernel,
        out_shape=outs,
        in_specs=specs,
        out_specs=[in_vmem() for _ in outs] if many else in_vmem(),
        scratch_shapes=list(scratch),
        compiler_params=pltpu.CompilerParams(vmem_limit_bytes=mib * 1024 * 1024),
    )(*operands)


def on_device(
    latents,
    conditions,
    context,
    w_shift,
    w_scale,
    w_gate,
    w_qdown,
    w_kvdown,
    w_rope,
    q_gain,
    latent_norm_gain,
    query_up_weight,
    key_up_weight,
    value_up_weight,
    context_bias,
    w_out,
):
    tp_count = lax.axis_size("tp")
    sp_count = lax.axis_size("sp")
    own_rows, width = latents.shape
    tok_count = own_rows * tp_count
    ctx_rows = context.shape[0]
    seg_rows = tok_count + ctx_rows
    small = is_small(tp_count)
    members = jnp.arange(-1, tp_count, dtype=jnp.int32)
    info = jnp.where(
        members < 0, lax.axis_index("sp"), jnp.bitwise_xor(lax.axis_index("tp"), members)
    )
    info, conditions = lax.optimization_barrier((info, conditions))
    ids = member_ids(info, tp_count)
    bf16 = jnp.bfloat16

    shape_of = jax.ShapeDtypeStruct

    lat_blocks = spread(latents)
    cond_act = jax.nn.silu(conditions).astype(bf16)
    partial_mod = jnp.concatenate(
        [f32_dot(cond_act, w_shift), f32_dot(cond_act, w_scale), f32_dot(cond_act[0:1], w_gate)],
        axis=0,
    )
    mod_pieces = spread(add_up(partial_mod, "sp"))

    head_count = query_up_weight.shape[1] // (PLAIN_QK_DIM + ROTARY_DIM)
    pairs = head_count // 2
    k_cosine, k_sine, q_table = call(
        functools.partial(tables_kernel, tok_count),
        [
            shape_of((seg_rows, LANES), jnp.float32),
            shape_of((seg_rows, LANES), jnp.float32),
            shape_of((ROTARY_DIM, tok_count), jnp.float32),
        ],
        [info],
        smem=(0,),
    )
    kv_cols = w_kvdown.shape[1]
    q_cols = w_qdown.shape[1]

    w_q, w_kr = call(
        weights_kernel,
        [shape_of(w_qdown.shape, bf16), shape_of((width, LANES + kv_cols), bf16)],
        [w_qdown, w_kvdown, w_rope.T],
        hbm=(0,),
        scratch=[pltpu.SemaphoreType.DMA],
    )
    if own_rows % 16 or not small:
        lat_blocks = [place(lat_blocks, ids, 0)]
        order = [0]
    else:
        order = [0, 1] + list(range(2, tp_count)) if tp_count > 1 else [0]
    early_of = [lat_blocks[member] for member in order[:2]] if len(order) > 2 else []
    late_of = [lat_blocks[member] for member in order[len(early_of) :]]
    normed = call(
        functools.partial(early_kernel, len(early_of) + 1),
        [shape_of(value.shape, jnp.float32) for value in [*early_of, context]],
        [*early_of, context],
        mib=12,
    )
    w_qt, w_k, w_vt, w_o = call(
        fetch_kernel,
        [
            shape_of(query_up_weight.shape[::-1], bf16),
            shape_of(key_up_weight.shape, bf16),
            shape_of(value_up_weight.shape[::-1], bf16),
            shape_of(w_out.shape, bf16),
        ],
        [query_up_weight, key_up_weight, value_up_weight, w_out],
        hbm=(1, 3),
        scratch=[pltpu.SemaphoreType.DMA((2,))],
    )
    merged = (
        kv_cols % LANES == 0
        and seg_rows % (16 * tp_count * LANES // ROTARY_DIM) == 0
        and small
        and is_small(sp_count)
    )
    extra = seg_rows // tp_count * ROTARY_DIM // LANES if merged else 0
    late_rows = [value.shape[0] for value in late_of]
    early_rows = [value.shape[0] for value in early_of]
    cq_cols, kv_own, kr_own = call(
        functools.partial(down_kernel, early_rows, late_rows, tp_count, tok_count, merged),
        [
            shape_of((tok_count, q_cols), bf16),
            shape_of((seg_rows + extra, kv_cols), bf16),
            shape_of((16 if merged else seg_rows, LANES), bf16),
        ],
        [
            info,
            *normed[:-1],
            *late_of,
            *mod_pieces,
            normed[-1],
            w_q,
            w_kr,
            k_cosine,
            k_sine,
        ],
        smem=(0,),
        scratch=[
            VMEM((sum(early_rows) + ctx_rows, width), bf16),
            VMEM((sum(late_rows), width), bf16),
            VMEM((5, width), jnp.float32),
            VMEM((seg_rows, LANES + kv_cols), jnp.float32),
        ],
        mib=16,
    )

    def columns(value):
        pieces = spread(value)
        if value.shape[1] % LANES:
            return [place(pieces, ids, 1)]
        return pieces

    if is_small(sp_count):
        blocks = []
        for member in range(sp_count):
            moved = swap(kv_own, "sp", member) if member else kv_own
            block = columns(moved)
            if not merged:
                block.append(swap(kr_own, "sp", member) if member else kr_own)
            blocks.append(block)
    else:
        kr_blocks = lax.all_gather(kr_own, "sp")
        whole_rows = lax.all_gather(kv_own, "tp", axis=1, tiled=True)
        kv_blocks = lax.all_gather(whole_rows, "sp")
        blocks = [[kv, kr] for kv, kr in zip(kv_blocks, kr_blocks)]
    cq_pieces = columns(cq_cols)
    queries = call(
        functools.partial(query_kernel, len(cq_pieces)),
        shape_of((pairs, 2 * LANES, 2 * tok_count), bf16),
        [info, *cq_pieces, q_gain[None, :], w_qt, q_table],
        smem=(0,),
        scratch=[VMEM((tok_count, q_gain.shape[0]), bf16)],
    )
    held = [
        shape_of((pairs, 8, 2 * tok_count), jnp.float32),
        shape_of((pairs, 8, 2 * tok_count), jnp.float32),
        shape_of((pairs, LANES, tok_count), jnp.float32),
    ]
    state = []
    begin = 0
    while begin < sp_count:
        part = blocks[begin : begin + (1 if begin < 2 else 2)]
        first, last = begin == 0, begin + len(part) >= sp_count
        state = call(
            functools.partial(
                attend_kernel,
                [len(block) - (0 if merged else 1) for block in part],
                tok_count,
                seg_rows,
                merged,
                first,
                last,
            ),
            shape_of((tok_count, head_count * VALUE_DIM), bf16) if last else held,
            [
                info,
                context_bias,
                queries,
                latent_norm_gain[None, :],
                w_k,
                w_vt,
                *[piece for block in part for piece in block],
                *state,
            ],
            smem=(0, 1),
            scratch=[
                VMEM((len(part), seg_rows, latent_norm_gain.shape[0]), bf16),
                VMEM((len(part) * seg_rows, head_count * PLAIN_QK_DIM), bf16),
                VMEM((len(part), head_count * VALUE_DIM, seg_rows), bf16),
                VMEM((len(part) * seg_rows, LANES), bf16),
            ],
            mib=16,
        )
        begin += len(part)
    att_pieces = spread(state)
    out_cols = w_out.shape[1]
    parts = tp_count if small and own_rows % 8 == 0 else 1
    proj = call(
        functools.partial(out_kernel, tp_count, parts),
        [shape_of((tok_count // parts, out_cols), bf16) for _ in range(parts)],
        [info, *att_pieces, w_o],
        smem=(0,),
        scratch=[VMEM((tok_count, out_cols), jnp.float32)] if parts > 1 else [],
    )
    if parts > 1:
        proj_pieces = [
            swap(value, "tp", member) if member else value
            for member, value in enumerate(proj)
        ]
    else:
        by_owner = proj[0].reshape(tp_count, own_rows, out_cols)
        proj_pieces = list(lax.all_to_all(by_owner, "tp", 0, 0))
        if small:
            proj_pieces = [
                lax.dynamic_index_in_dim(jnp.stack(proj_pieces), ids[member], 0, False)
                for member in range(tp_count)
            ]
    return call(
        functools.partial(final_kernel, tp_count, tp_count),
        shape_of((own_rows, width), bf16),
        [info, *proj_pieces, *mod_pieces, latents],
        smem=(0,),
    )


def solution(mesh):
    in_specs = (
        P(("grp", "sp", "tp"), None),
        P("grp", "sp"),
        P(("grp", "sp"), None),
        P("sp", "tp"),
        P("sp", "tp"),
        P("sp", "tp"),
        P(None, "tp"),
        P(None, "tp"),
        P(),
        P(),
        P(),
        P(None, "tp"),
        P(None, "tp"),
        P(None, "tp"),
        P("tp"),
        P(None, "tp"),
    )
    out_specs = P(("grp", "sp", "tp"), None)
    step = jax.shard_map(
        on_device, mesh=mesh, in_specs=in_specs, out_specs=out_specs, check_vma=False
    )
    if not (is_small(mesh.shape["tp"]) and is_small(mesh.shape["sp"])):
        return step
    return step
```

```python
import functools

import jax
import jax.numpy as jnp
from jax import lax
from jax.experimental import pallas as pl
from jax.experimental.pallas import tpu as pltpu
from jax.sharding import PartitionSpec as P


PLAIN_QK_DIM = 64
ROTARY_DIM = 32
VALUE_DIM = 64
GRID_W = 64
LANES = 128
LOG2E = 1.4426950408889634

EPSILON = 1e-06


VMEM = pltpu.VMEM
SMEM = pltpu.SMEM


def in_vmem():
    return pl.BlockSpec(memory_space=VMEM)


def in_smem():
    return pl.BlockSpec(memory_space=SMEM)


def f32_dot(a, b):
    return jnp.dot(a, b, preferred_element_type=jnp.float32)


def swap(value, axis, bit):
    count = lax.axis_size(axis)
    return lax.ppermute(value, axis, [(i, i ^ bit) for i in range(count)])


def is_small(count):
    return count <= 4


def tp_bits(count):
    bits = []
    bit = 2
    while bit < count:
        bits.append(bit)
        bit *= 2
    if count > 1:
        bits.append(1)
    return bits


def spread(value, axis="tp"):
    if not is_small(lax.axis_size(axis)):
        return list(lax.all_gather(value, axis))
    got = {0: value}
    for bit in tp_bits(lax.axis_size(axis)):
        for member in list(got):
            got[member ^ bit] = swap(got[member], axis, bit)
    return [got[member] for member in range(len(got))]


def add_up(value, axis):
    count = lax.axis_size(axis)
    if not is_small(count):
        return lax.psum(value, axis)
    bit = 1
    while bit < count:
        value = value + swap(value, axis, bit)
        bit *= 2
    return value


def place(pieces, ids, axis):
    width = pieces[0].shape[axis]
    shape = list(pieces[0].shape)
    shape[axis] = width * len(pieces)
    whole = jnp.zeros(shape, pieces[0].dtype)
    for member, piece in enumerate(pieces):
        whole = lax.dynamic_update_slice_in_dim(whole, piece, ids[member] * width, axis)
    return whole


def angles(position, frequency, use_column):
    freq_count = ROTARY_DIM // 4
    inverse = jnp.zeros(frequency.shape, jnp.float32)
    for number in range(freq_count):
        inverse = jnp.where(
            frequency == number, jnp.float32(10000.0 ** (-number / freq_count)), inverse
        )
    coordinate = jnp.where(use_column, position % GRID_W, position // GRID_W)
    return coordinate.astype(jnp.float32) * inverse


def tables_kernel(tok_count, info, cos_ref, sin_ref, table_ref):
    freq_count = ROTARY_DIM // 4
    start = info[0] * tok_count
    shape = cos_ref.shape
    row = lax.broadcasted_iota(jnp.int32, shape, 0)
    lane = lax.broadcasted_iota(jnp.int32, shape, 1)
    angle = angles(start + row, lane % freq_count, (lane // (2 * freq_count)) % 2 == 1)
    is_lat = row < tok_count
    cos_ref[...] = jnp.where(is_lat, jnp.cos(angle), 1.0)
    sine_of = jnp.where((lane // freq_count) % 2 == 0, -jnp.sin(angle), jnp.sin(angle))
    sin_ref[...] = jnp.where(is_lat, sine_of, 0.0)
    shape = table_ref.shape
    row = lax.broadcasted_iota(jnp.int32, shape, 0)
    lane = lax.broadcasted_iota(jnp.int32, shape, 1)
    angle = angles(start + lane, row % freq_count, row // (2 * freq_count) == 1)
    table_ref[...] = jnp.where((row // freq_count) % 2 == 0, jnp.cos(angle), jnp.sin(angle))


def turn(values, cosine, sine_of):
    freq_count = ROTARY_DIM // 4
    lanes = values.shape[1]
    lane = lax.broadcasted_iota(jnp.int32, values.shape, 1)
    first = (lane % (2 * freq_count)) < freq_count
    partner = jnp.where(
        first, pltpu.roll(values, lanes - freq_count, 1), pltpu.roll(values, freq_count, 1)
    )
    return values * cosine + partner * sine_of


class Members:
    def __init__(self, info):
        self.info = info

    def __getitem__(self, member):
        return self.info[1 + member]


def member_ids(info, count):
    return Members(info) if is_small(count) else list(range(count))


def aligned(value, step):
    return value if isinstance(value, int) else pl.multiple_of(value, step)


def gather_rows(scratch, ids, pieces):
    width = pieces[0].shape[1]
    for number, piece in enumerate(pieces):
        scratch[:, pl.ds(aligned(ids[number] * width, LANES), width)] = piece[...]


def normalize(values):
    center = values - jnp.mean(values, axis=-1, keepdims=True)
    spread_of = jnp.mean(center * center, axis=-1, keepdims=True)
    return center * lax.rsqrt(spread_of + EPSILON)


def weights_kernel(wq_hbm, wk_ref, rope_ref, wq_ref, wkr_ref, sem):
    copy = pltpu.make_async_copy(wq_hbm, wq_ref, sem)
    copy.start()
    wkr_ref[:, LANES:] = wk_ref[...]
    copies = (
        lax.broadcasted_iota(jnp.int32, (ROTARY_DIM, LANES), 0)
        == lax.broadcasted_iota(jnp.int32, (ROTARY_DIM, LANES), 1) % ROTARY_DIM
    ).astype(jnp.bfloat16)
    wkr_ref[:, :LANES] = lax.dot_general(
        rope_ref[...], copies, (((0,), (0,)), ((), ())), preferred_element_type=jnp.float32
    ).astype(jnp.bfloat16)
    copy.wait()


def early_kernel(count, *refs):
    for source, out_ref in zip(refs[:count], refs[count:]):
        for row in range(0, source.shape[0], 16):
            values = source[row : row + 16, :].astype(jnp.float32)
            out_ref[row : row + 16, :] = normalize(values)


def fetch_kernel(wq_ref, wk_hbm, wv_ref, wo_hbm, wqt_ref, wk_ref, wvt_ref, wo_ref, sems):
    copies = [
        pltpu.make_async_copy(wk_hbm, wk_ref, sems.at[0]),
        pltpu.make_async_copy(wo_hbm, wo_ref, sems.at[1]),
    ]
    for copy in copies:
        copy.start()
    wqt_ref[...] = wq_ref[...].astype(jnp.float32).T.astype(jnp.bfloat16)
    wvt_ref[...] = wv_ref[...].astype(jnp.float32).T.astype(jnp.bfloat16)
    for copy in copies:
        copy.wait()


def down_kernel(early_rows, late_rows, mod_count, tok_count, merged, info, *refs):
    ids = member_ids(info, mod_count)
    offsets = [0] if len(early_rows) + len(late_rows) == 1 else ids
    early, refs = refs[: len(early_rows)], refs[len(early_rows) :]
    late, refs = refs[: len(late_rows)], refs[len(late_rows) :]
    pieces, refs = refs[:mod_count], refs[mod_count:]
    ctx_ref, wq_ref, wkr_ref, cos_ref, sin_ref = refs[:5]
    cq_ref, kv_ref, kr_ref, ha_ref, hb_ref, mod_ref, both_ref = refs[5:]
    step = 16
    gather_rows(mod_ref, ids, pieces)

    def modulate(source, target, base, rows, is_ctx, is_normed):
        shift_by = mod_ref[is_ctx : is_ctx + 1, :]
        scale_by = 1.0 + mod_ref[2 + is_ctx : 3 + is_ctx, :]
        for row in range(0, rows, step):
            values = source[row : row + step, :]
            if not is_normed:
                values = normalize(values.astype(jnp.float32))
            target[base + row : base + row + step, :] = (values * scale_by + shift_by).astype(
                jnp.bfloat16
            )

    def multiply(source, rows_of, first, with_ctx):
        cq = f32_dot(source[...], wq_ref[...])
        both = f32_dot(source[...], wkr_ref[...])
        base = 0
        for number, rows in enumerate(rows_of):
            start = aligned(offsets[first + number] * rows, 16)
            cq_ref[pl.ds(start, rows), :] = cq[base : base + rows].astype(jnp.bfloat16)
            both_ref[pl.ds(start, rows), :] = both[base : base + rows]
            base += rows
        if with_ctx:
            both_ref[tok_count:, :] = both[base:]

    base = 0
    for source, rows in zip(early, early_rows):
        modulate(source, ha_ref, base, rows, 0, True)
        base += rows
    modulate(ctx_ref, ha_ref, base, ctx_ref.shape[0], 1, True)
    multiply(ha_ref, early_rows, 0, True)
    base = 0
    for source, rows in zip(late, late_rows):
        modulate(source, hb_ref, base, rows, 0, False)
        base += rows
    multiply(hb_ref, late_rows, len(early_rows), False)
    seg = both_ref.shape[0]
    kv_ref[:seg, :] = both_ref[:, LANES:].astype(jnp.bfloat16)
    turned = turn(both_ref[:, :LANES], cos_ref[...], sin_ref[...]).astype(jnp.bfloat16)
    if merged:
        both_ref[:, :LANES] = turned.astype(jnp.float32)
        quarter = seg // mod_count
        sub = quarter // (LANES // ROTARY_DIM)
        lane = lax.broadcasted_iota(jnp.int32, (sub, LANES), 1)
        packed = None
        for part in range(LANES // ROTARY_DIM):
            start = aligned(ids[0] * quarter + part * sub, 8)
            rows = both_ref[pl.ds(start, sub), :LANES]
            rows = jnp.where(lane // ROTARY_DIM == part, rows, 0.0)
            packed = rows if packed is None else packed + rows
        kv_ref[seg:, :] = packed.astype(jnp.bfloat16)
        kr_ref[...] = jnp.zeros_like(kr_ref)
    else:
        kr_ref[...] = turned


def normed_into(scratch, ids, pieces, gain_ref):
    width = pieces[0].shape[1]
    rows = scratch.shape[0]
    total = width * len(pieces)
    squares = None
    for piece in pieces:
        values = piece[:rows, :].astype(jnp.float32)
        part = jnp.sum(values * values, axis=-1, keepdims=True)
        squares = part if squares is None else squares + part
    factor = lax.rsqrt(squares / total + EPSILON)
    for number, piece in enumerate(pieces):
        if len(pieces) == 1:
            where = slice(None)
        else:
            where = pl.ds(aligned(ids[number] * width, LANES), width)
        gained = piece[:rows, :].astype(jnp.float32) * factor * gain_ref[:, where]
        scratch[:, where] = gained.astype(jnp.bfloat16)


def query_kernel(count, info, *refs):
    ids = member_ids(info, count)
    pieces = refs[:count]
    gain_ref, w_ref, table_ref, q_ref, scratch = refs[count:]
    normed_into(scratch, ids, pieces, gain_ref)
    rows = scratch.shape[0]
    raw = lax.dot_general(
        w_ref[...], scratch[...], (((1,), (1,)), ((), ())), preferred_element_type=jnp.float32
    )
    freq_count = ROTARY_DIM // 4
    tables = [table_ref[i * freq_count : (i + 1) * freq_count, :] for i in range(4)]
    span = PLAIN_QK_DIM + ROTARY_DIM
    q_ref[...] = jnp.zeros_like(q_ref)
    for head in range(2 * q_ref.shape[0]):
        half = head % 2
        lanes = slice(half * rows, (half + 1) * rows)
        start = head * span
        q_ref[head // 2, half * PLAIN_QK_DIM : (half + 1) * PLAIN_QK_DIM, lanes] = raw[
            start : start + PLAIN_QK_DIM
        ].astype(jnp.bfloat16)
        start += PLAIN_QK_DIM
        parts = [raw[start + i * freq_count : start + (i + 1) * freq_count] for i in range(4)]
        turned = []
        for axis in range(2):
            low, high = parts[2 * axis : 2 * axis + 2]
            cosine, sine_of = tables[2 * axis : 2 * axis + 2]
            turned += [low * cosine - high * sine_of, low * sine_of + high * cosine]
        q_ref[head // 2, LANES : LANES + ROTARY_DIM, lanes] = jnp.concatenate(
            turned, axis=0
        ).astype(jnp.bfloat16)


def fold_rows(values):
    return jnp.sum(values.reshape(-1, 8, values.shape[1]), axis=0)


def attend_kernel(counts, tok_keys, seg, merged, first, last, info, *refs):
    ids = member_ids(info, counts[0])
    bias_ref, q_ref, gain_ref, wk_ref, wv_ref = refs[:5]
    refs = refs[5:]
    blocks = []
    for count in counts:
        blocks.append(refs[: count + (0 if merged else 1)])
        refs = refs[len(blocks[-1]) :]
    if not first:
        state_in, refs = refs[:3], refs[3:]
    if last:
        out_ref, refs = refs[0], refs[1:]
    else:
        state_out, refs = refs[:3], refs[3:]
    scratch, k_ref, v_ref, r_ref = refs
    pairs, _, lanes = q_ref.shape
    rows = lanes // 2
    for number, block in enumerate(blocks):
        pieces = block if merged else block[:-1]
        base = number * seg
        rows_ref = scratch.at[number]
        normed_into(rows_ref, ids, pieces, gain_ref)
        k_ref[base : base + seg, :] = f32_dot(rows_ref[...], wk_ref[...]).astype(jnp.bfloat16)
        v_ref[number] = lax.dot_general(
            wv_ref[...], rows_ref[...], (((1,), (1,)), ((), ())), preferred_element_type=jnp.float32
        ).astype(jnp.bfloat16)
        if merged:
            quarter = seg // len(pieces)
            sub = quarter // (LANES // ROTARY_DIM)
            for member, piece in enumerate(pieces):
                packed = piece[seg:, :].astype(jnp.float32)
                for part in range(LANES // ROTARY_DIM):
                    moved = pltpu.roll(packed, (-part * ROTARY_DIM) % LANES, 1) if part else packed
                    start = aligned(base + ids[member] * quarter + part * sub, 16)
                    r_ref[pl.ds(start, sub), :] = moved.astype(jnp.bfloat16)
        else:
            r_ref[base : base + seg, :] = block[-1][...]
    score_scale = (PLAIN_QK_DIM + ROTARY_DIM) ** (-0.5) * LOG2E
    lane = lax.broadcasted_iota(jnp.int32, (1, lanes), 1)

    def score(pair, number):
        base = number * seg
        span = slice(pair * LANES, (pair + 1) * LANES)
        key = jnp.concatenate([k_ref[base : base + seg, span], r_ref[base : base + seg, :]], axis=1)
        return f32_dot(key, q_ref[pair])

    steps = [(pair, number) for pair in range(pairs) for number in range(len(blocks))]
    ahead = score(*steps[0])
    for pair in range(pairs):
        span = slice(pair * LANES, (pair + 1) * LANES)
        bias = jnp.where(lane < rows, bias_ref[2 * pair], bias_ref[2 * pair + 1]) * LOG2E
        top = total = acc = None
        if not first:
            top = state_in[0][pair, :1, :]
            total, acc = state_in[1][pair], state_in[2][pair]
        for number in range(len(blocks)):
            scores = ahead
            after = pair * len(blocks) + number + 1
            if after < len(steps):
                ahead = score(*steps[after])
            lat, ctx = scores[:tok_keys], scores[tok_keys:]
            peak = jnp.maximum(
                jnp.max(lat, axis=0, keepdims=True) * score_scale,
                jnp.max(ctx, axis=0, keepdims=True) * score_scale + bias,
            )
            new_top = peak if top is None else jnp.maximum(top, peak)
            e_lat = jnp.exp2(lat * score_scale - new_top)
            e_ctx = jnp.exp2(ctx * score_scale - (new_top - bias))
            part = fold_rows(e_lat) + fold_rows(e_ctx)
            weights = jnp.concatenate([e_lat, e_ctx], axis=0).astype(jnp.bfloat16)
            both = f32_dot(v_ref[number, span, :], weights)
            gathered = jnp.concatenate([both[:VALUE_DIM, :rows], both[VALUE_DIM:, rows:]], axis=0)
            if top is None:
                total, acc = part, gathered
            else:
                rescale = jnp.exp2(top - new_top)
                total = total * rescale + part
                acc = gathered + jnp.concatenate(
                    [acc[:VALUE_DIM] * rescale[:, :rows], acc[VALUE_DIM:] * rescale[:, rows:]],
                    axis=0,
                )
            top = new_top
        if last:
            total = jnp.sum(total, axis=0, keepdims=True)
            done = jnp.concatenate(
                [acc[:VALUE_DIM] / total[:, :rows], acc[VALUE_DIM:] / total[:, rows:]], axis=0
            )
            out_ref[:, span] = done.T.astype(jnp.bfloat16)
        else:
            state_out[0][pair] = jnp.broadcast_to(top, (8, lanes))
            state_out[1][pair] = total
            state_out[2][pair] = acc


def out_kernel(count, parts, info, *refs):
    ids = member_ids(info, count)
    pieces = refs[:count]
    w_ref = refs[count]
    outs = refs[1 + count : 1 + count + parts]
    depth = pieces[0].shape[1]
    total = None
    for number, piece in enumerate(pieces):
        rows = pl.ds(aligned(ids[number] * depth, LANES), depth)
        part = f32_dot(piece[...], w_ref[rows, :])
        total = part if total is None else total + part
    if parts == 1:
        outs[0][...] = total.astype(jnp.bfloat16)
        return
    scratch = refs[1 + count + parts]
    scratch[...] = total
    rows = outs[0].shape[0]
    for number, out_ref in enumerate(outs):
        start = aligned(ids[number] * rows, 8)
        out_ref[...] = scratch[pl.ds(start, rows), :].astype(jnp.bfloat16)


def final_kernel(count, mod_count, info, *refs):
    ids = member_ids(info, count)
    pieces = refs[:count]
    gates = refs[count : count + mod_count]
    lat_ref, out_ref = refs[count + mod_count :]
    width = pieces[0].shape[1]
    for number, (piece, gate) in enumerate(zip(pieces, gates)):
        span = pl.ds(aligned(ids[number] * width, LANES), width)
        out_ref[:, span] = (
            lat_ref[:, span].astype(jnp.float32)
            + gate[gate.shape[0] - 1 :, :] * piece[...].astype(jnp.float32)
        ).astype(jnp.bfloat16)


def call(kernel, outs, operands, smem=(), hbm=(), scratch=(), mib=16):
    specs = []
    for place_of in range(len(operands)):
        if place_of in hbm:
            specs.append(pl.BlockSpec(memory_space=pl.ANY))
        else:
            specs.append(in_smem() if place_of in smem else in_vmem())
    many = isinstance(outs, (list, tuple))
    return pl.pallas_call(
        kernel,
        out_shape=outs,
        in_specs=specs,
        out_specs=[in_vmem() for _ in outs] if many else in_vmem(),
        scratch_shapes=list(scratch),
        compiler_params=pltpu.CompilerParams(vmem_limit_bytes=mib * 1024 * 1024),
    )(*operands)


def on_device(
    latents,
    conditions,
    context,
    w_shift,
    w_scale,
    w_gate,
    w_qdown,
    w_kvdown,
    w_rope,
    q_gain,
    latent_norm_gain,
    query_up_weight,
    key_up_weight,
    value_up_weight,
    context_bias,
    w_out,
):
    tp_count = lax.axis_size("tp")
    sp_count = lax.axis_size("sp")
    own_rows, width = latents.shape
    tok_count = own_rows * tp_count
    ctx_rows = context.shape[0]
    seg_rows = tok_count + ctx_rows
    small = is_small(tp_count)
    members = jnp.arange(-1, tp_count, dtype=jnp.int32)
    info = jnp.where(
        members < 0, lax.axis_index("sp"), jnp.bitwise_xor(lax.axis_index("tp"), members)
    )
    info, conditions = lax.optimization_barrier((info, conditions))
    ids = member_ids(info, tp_count)
    bf16 = jnp.bfloat16

    shape_of = jax.ShapeDtypeStruct

    lat_blocks = spread(latents)
    cond_act = jax.nn.silu(conditions).astype(bf16)
    partial_mod = jnp.concatenate(
        [f32_dot(cond_act, w_shift), f32_dot(cond_act, w_scale), f32_dot(cond_act[0:1], w_gate)],
        axis=0,
    )
    mod_pieces = spread(add_up(partial_mod, "sp"))

    head_count = query_up_weight.shape[1] // (PLAIN_QK_DIM + ROTARY_DIM)
    pairs = head_count // 2
    k_cosine, k_sine, q_table = call(
        functools.partial(tables_kernel, tok_count),
        [
            shape_of((seg_rows, LANES), jnp.float32),
            shape_of((seg_rows, LANES), jnp.float32),
            shape_of((ROTARY_DIM, tok_count), jnp.float32),
        ],
        [info],
        smem=(0,),
    )
    kv_cols = w_kvdown.shape[1]
    q_cols = w_qdown.shape[1]

    w_q, w_kr = call(
        weights_kernel,
        [shape_of(w_qdown.shape, bf16), shape_of((width, LANES + kv_cols), bf16)],
        [w_qdown, w_kvdown, w_rope.T],
        hbm=(0,),
        scratch=[pltpu.SemaphoreType.DMA],
    )
    if own_rows % 16 or not small:
        lat_blocks = [place(lat_blocks, ids, 0)]
        order = [0]
    else:
        order = [0, 1] + list(range(2, tp_count)) if tp_count > 1 else [0]
    early_of = [lat_blocks[member] for member in order[:2]] if len(order) > 2 else []
    late_of = [lat_blocks[member] for member in order[len(early_of) :]]
    normed = call(
        functools.partial(early_kernel, len(early_of) + 1),
        [shape_of(value.shape, jnp.float32) for value in [*early_of, context]],
        [*early_of, context],
        mib=12,
    )
    w_qt, w_k, w_vt, w_o = call(
        fetch_kernel,
        [
            shape_of(query_up_weight.shape[::-1], bf16),
            shape_of(key_up_weight.shape, bf16),
            shape_of(value_up_weight.shape[::-1], bf16),
            shape_of(w_out.shape, bf16),
        ],
        [query_up_weight, key_up_weight, value_up_weight, w_out],
        hbm=(1, 3),
        scratch=[pltpu.SemaphoreType.DMA((2,))],
    )
    merged = (
        kv_cols % LANES == 0
        and seg_rows % (16 * tp_count * LANES // ROTARY_DIM) == 0
        and small
        and is_small(sp_count)
    )
    extra = seg_rows // tp_count * ROTARY_DIM // LANES if merged else 0
    late_rows = [value.shape[0] for value in late_of]
    early_rows = [value.shape[0] for value in early_of]
    cq_cols, kv_own, kr_own = call(
        functools.partial(down_kernel, early_rows, late_rows, tp_count, tok_count, merged),
        [
            shape_of((tok_count, q_cols), bf16),
            shape_of((seg_rows + extra, kv_cols), bf16),
            shape_of((16 if merged else seg_rows, LANES), bf16),
        ],
        [
            info,
            *normed[:-1],
            *late_of,
            *mod_pieces,
            normed[-1],
            w_q,
            w_kr,
            k_cosine,
            k_sine,
        ],
        smem=(0,),
        scratch=[
            VMEM((sum(early_rows) + ctx_rows, width), bf16),
            VMEM((sum(late_rows), width), bf16),
            VMEM((5, width), jnp.float32),
            VMEM((seg_rows, LANES + kv_cols), jnp.float32),
        ],
        mib=16,
    )

    def columns(value):
        pieces = spread(value)
        if value.shape[1] % LANES:
            return [place(pieces, ids, 1)]
        return pieces

    if is_small(sp_count):
        blocks = []
        for member in range(sp_count):
            moved = swap(kv_own, "sp", member) if member else kv_own
            block = columns(moved)
            if not merged:
                block.append(swap(kr_own, "sp", member) if member else kr_own)
            blocks.append(block)
    else:
        kr_blocks = lax.all_gather(kr_own, "sp")
        whole_rows = lax.all_gather(kv_own, "tp", axis=1, tiled=True)
        kv_blocks = lax.all_gather(whole_rows, "sp")
        blocks = [[kv, kr] for kv, kr in zip(kv_blocks, kr_blocks)]
    cq_pieces = columns(cq_cols)
    queries = call(
        functools.partial(query_kernel, len(cq_pieces)),
        shape_of((pairs, 2 * LANES, 2 * tok_count), bf16),
        [info, *cq_pieces, q_gain[None, :], w_qt, q_table],
        smem=(0,),
        scratch=[VMEM((tok_count, q_gain.shape[0]), bf16)],
    )
    held = [
        shape_of((pairs, 8, 2 * tok_count), jnp.float32),
        shape_of((pairs, 8, 2 * tok_count), jnp.float32),
        shape_of((pairs, LANES, tok_count), jnp.float32),
    ]
    state = []
    begin = 0
    while begin < sp_count:
        part = blocks[begin : begin + (1 if begin < 2 else 2)]
        first, last = begin == 0, begin + len(part) >= sp_count
        state = call(
            functools.partial(
                attend_kernel,
                [len(block) - (0 if merged else 1) for block in part],
                tok_count,
                seg_rows,
                merged,
                first,
                last,
            ),
            shape_of((tok_count, head_count * VALUE_DIM), bf16) if last else held,
            [
                info,
                context_bias,
                queries,
                latent_norm_gain[None, :],
                w_k,
                w_vt,
                *[piece for block in part for piece in block],
                *state,
            ],
            smem=(0, 1),
            scratch=[
                VMEM((len(part), seg_rows, latent_norm_gain.shape[0]), bf16),
                VMEM((len(part) * seg_rows, head_count * PLAIN_QK_DIM), bf16),
                VMEM((len(part), head_count * VALUE_DIM, seg_rows), bf16),
                VMEM((len(part) * seg_rows, LANES), bf16),
            ],
            mib=16,
        )
        begin += len(part)
    att_pieces = spread(state)
    out_cols = w_out.shape[1]
    parts = tp_count if small and own_rows % 8 == 0 else 1
    proj = call(
        functools.partial(out_kernel, tp_count, parts),
        [shape_of((tok_count // parts, out_cols), bf16) for _ in range(parts)],
        [info, *att_pieces, w_o],
        smem=(0,),
        scratch=[VMEM((tok_count, out_cols), jnp.float32)] if parts > 1 else [],
    )
    if parts > 1:
        proj_pieces = [
            swap(value, "tp", member) if member else value
            for member, value in enumerate(proj)
        ]
    else:
        by_owner = proj[0].reshape(tp_count, own_rows, out_cols)
        proj_pieces = list(lax.all_to_all(by_owner, "tp", 0, 0))
        if small:
            proj_pieces = [
                lax.dynamic_index_in_dim(jnp.stack(proj_pieces), ids[member], 0, False)
                for member in range(tp_count)
            ]
    return call(
        functools.partial(final_kernel, tp_count, tp_count),
        shape_of((own_rows, width), bf16),
        [info, *proj_pieces, *mod_pieces, latents],
        smem=(0,),
    )


def solution(mesh):
    in_specs = (
        P(("grp", "sp", "tp"), None),
        P("grp", "sp"),
        P(("grp", "sp"), None),
        P("sp", "tp"),
        P("sp", "tp"),
        P("sp", "tp"),
        P(None, "tp"),
        P(None, "tp"),
        P(),
        P(),
        P(),
        P(None, "tp"),
        P(None, "tp"),
        P(None, "tp"),
        P("tp"),
        P(None, "tp"),
    )
    out_specs = P(("grp", "sp", "tp"), None)
    step = jax.shard_map(
        on_device, mesh=mesh, in_specs=in_specs, out_specs=out_specs, check_vma=False
    )
    if not (is_small(mesh.shape["tp"]) and is_small(mesh.shape["sp"])):
        return step
    return step
```

```python
import functools

import jax
import jax.numpy as jnp
from jax import lax
from jax.experimental import pallas as pl
from jax.experimental.pallas import tpu as pltpu
from jax.sharding import PartitionSpec as P


PLAIN_QK_DIM = 64
ROTARY_DIM = 32
VALUE_DIM = 64
GRID_W = 64
LANES = 128
LOG2E = 1.4426950408889634

EPSILON = 1e-06


VMEM = pltpu.VMEM
SMEM = pltpu.SMEM


def in_vmem():
    return pl.BlockSpec(memory_space=VMEM)


def in_smem():
    return pl.BlockSpec(memory_space=SMEM)


def f32_dot(a, b):
    return jnp.dot(a, b, preferred_element_type=jnp.float32)


def swap(value, axis, bit):
    count = lax.axis_size(axis)
    return lax.ppermute(value, axis, [(i, i ^ bit) for i in range(count)])


def is_small(count):
    return count <= 4


def tp_bits(count):
    bits = []
    bit = 2
    while bit < count:
        bits.append(bit)
        bit *= 2
    if count > 1:
        bits.append(1)
    return bits


def spread(value, axis="tp"):
    if not is_small(lax.axis_size(axis)):
        return list(lax.all_gather(value, axis))
    got = {0: value}
    for bit in tp_bits(lax.axis_size(axis)):
        for member in list(got):
            got[member ^ bit] = swap(got[member], axis, bit)
    return [got[member] for member in range(len(got))]


def add_up(value, axis):
    count = lax.axis_size(axis)
    if not is_small(count):
        return lax.psum(value, axis)
    bit = 1
    while bit < count:
        value = value + swap(value, axis, bit)
        bit *= 2
    return value


def place(pieces, ids, axis):
    width = pieces[0].shape[axis]
    shape = list(pieces[0].shape)
    shape[axis] = width * len(pieces)
    whole = jnp.zeros(shape, pieces[0].dtype)
    for member, piece in enumerate(pieces):
        whole = lax.dynamic_update_slice_in_dim(whole, piece, ids[member] * width, axis)
    return whole


def angles(position, frequency, use_column):
    freq_count = ROTARY_DIM // 4
    inverse = jnp.zeros(frequency.shape, jnp.float32)
    for number in range(freq_count):
        inverse = jnp.where(
            frequency == number, jnp.float32(10000.0 ** (-number / freq_count)), inverse
        )
    coordinate = jnp.where(use_column, position % GRID_W, position // GRID_W)
    return coordinate.astype(jnp.float32) * inverse


def tables_kernel(tok_count, info, cos_ref, sin_ref, table_ref):
    freq_count = ROTARY_DIM // 4
    start = info[0] * tok_count
    shape = cos_ref.shape
    row = lax.broadcasted_iota(jnp.int32, shape, 0)
    lane = lax.broadcasted_iota(jnp.int32, shape, 1)
    angle = angles(start + row, lane % freq_count, (lane // (2 * freq_count)) % 2 == 1)
    is_lat = row < tok_count
    cos_ref[...] = jnp.where(is_lat, jnp.cos(angle), 1.0)
    sine_of = jnp.where((lane // freq_count) % 2 == 0, -jnp.sin(angle), jnp.sin(angle))
    sin_ref[...] = jnp.where(is_lat, sine_of, 0.0)
    shape = table_ref.shape
    row = lax.broadcasted_iota(jnp.int32, shape, 0)
    lane = lax.broadcasted_iota(jnp.int32, shape, 1)
    angle = angles(start + lane, row % freq_count, row // (2 * freq_count) == 1)
    table_ref[...] = jnp.where((row // freq_count) % 2 == 0, jnp.cos(angle), jnp.sin(angle))


def turn(values, cosine, sine_of):
    freq_count = ROTARY_DIM // 4
    lanes = values.shape[1]
    lane = lax.broadcasted_iota(jnp.int32, values.shape, 1)
    first = (lane % (2 * freq_count)) < freq_count
    partner = jnp.where(
        first, pltpu.roll(values, lanes - freq_count, 1), pltpu.roll(values, freq_count, 1)
    )
    return values * cosine + partner * sine_of


class Members:
    def __init__(self, info):
        self.info = info

    def __getitem__(self, member):
        return self.info[1 + member]


def member_ids(info, count):
    return Members(info) if is_small(count) else list(range(count))


def aligned(value, step):
    return value if isinstance(value, int) else pl.multiple_of(value, step)


def gather_rows(scratch, ids, pieces):
    width = pieces[0].shape[1]
    for number, piece in enumerate(pieces):
        scratch[:, pl.ds(aligned(ids[number] * width, LANES), width)] = piece[...]


def normalize(values):
    center = values - jnp.mean(values, axis=-1, keepdims=True)
    spread_of = jnp.mean(center * center, axis=-1, keepdims=True)
    return center * lax.rsqrt(spread_of + EPSILON)


def weights_kernel(wq_hbm, wk_ref, rope_ref, wq_ref, wkr_ref, sem):
    copy = pltpu.make_async_copy(wq_hbm, wq_ref, sem)
    copy.start()
    wkr_ref[:, LANES:] = wk_ref[...]
    copies = (
        lax.broadcasted_iota(jnp.int32, (ROTARY_DIM, LANES), 0)
        == lax.broadcasted_iota(jnp.int32, (ROTARY_DIM, LANES), 1) % ROTARY_DIM
    ).astype(jnp.bfloat16)
    wkr_ref[:, :LANES] = lax.dot_general(
        rope_ref[...], copies, (((0,), (0,)), ((), ())), preferred_element_type=jnp.float32
    ).astype(jnp.bfloat16)
    copy.wait()


def early_kernel(count, *refs):
    for source, out_ref in zip(refs[:count], refs[count:]):
        for row in range(0, source.shape[0], 16):
            values = source[row : row + 16, :].astype(jnp.float32)
            out_ref[row : row + 16, :] = normalize(values)


def fetch_kernel(wq_ref, wk_hbm, wv_ref, wo_hbm, wqt_ref, wk_ref, wvt_ref, wo_ref, sems):
    copies = [
        pltpu.make_async_copy(wk_hbm, wk_ref, sems.at[0]),
        pltpu.make_async_copy(wo_hbm, wo_ref, sems.at[1]),
    ]
    for copy in copies:
        copy.start()
    wqt_ref[...] = wq_ref[...].astype(jnp.float32).T.astype(jnp.bfloat16)
    wvt_ref[...] = wv_ref[...].astype(jnp.float32).T.astype(jnp.bfloat16)
    for copy in copies:
        copy.wait()


def down_kernel(early_rows, late_rows, mod_count, tok_count, merged, info, *refs):
    ids = member_ids(info, mod_count)
    offsets = [0] if len(early_rows) + len(late_rows) == 1 else ids
    early, refs = refs[: len(early_rows)], refs[len(early_rows) :]
    late, refs = refs[: len(late_rows)], refs[len(late_rows) :]
    pieces, refs = refs[:mod_count], refs[mod_count:]
    ctx_ref, wq_ref, wkr_ref, cos_ref, sin_ref = refs[:5]
    cq_ref, kv_ref, kr_ref, ha_ref, hb_ref, mod_ref, both_ref = refs[5:]
    step = 16
    gather_rows(mod_ref, ids, pieces)

    def modulate(source, target, base, rows, is_ctx, is_normed):
        shift_by = mod_ref[is_ctx : is_ctx + 1, :]
        scale_by = 1.0 + mod_ref[2 + is_ctx : 3 + is_ctx, :]
        for row in range(0, rows, step):
            values = source[row : row + step, :]
            if not is_normed:
                values = normalize(values.astype(jnp.float32))
            target[base + row : base + row + step, :] = (values * scale_by + shift_by).astype(
                jnp.bfloat16
            )

    def multiply(source, rows_of, first, with_ctx):
        cq = f32_dot(source[...], wq_ref[...])
        both = f32_dot(source[...], wkr_ref[...])
        base = 0
        for number, rows in enumerate(rows_of):
            start = aligned(offsets[first + number] * rows, 16)
            cq_ref[pl.ds(start, rows), :] = cq[base : base + rows].astype(jnp.bfloat16)
            both_ref[pl.ds(start, rows), :] = both[base : base + rows]
            base += rows
        if with_ctx:
            both_ref[tok_count:, :] = both[base:]

    base = 0
    for source, rows in zip(early, early_rows):
        modulate(source, ha_ref, base, rows, 0, True)
        base += rows
    modulate(ctx_ref, ha_ref, base, ctx_ref.shape[0], 1, True)
    multiply(ha_ref, early_rows, 0, True)
    base = 0
    for source, rows in zip(late, late_rows):
        modulate(source, hb_ref, base, rows, 0, False)
        base += rows
    multiply(hb_ref, late_rows, len(early_rows), False)
    seg = both_ref.shape[0]
    kv_ref[:seg, :] = both_ref[:, LANES:].astype(jnp.bfloat16)
    turned = turn(both_ref[:, :LANES], cos_ref[...], sin_ref[...]).astype(jnp.bfloat16)
    if merged:
        both_ref[:, :LANES] = turned.astype(jnp.float32)
        quarter = seg // mod_count
        sub = quarter // (LANES // ROTARY_DIM)
        lane = lax.broadcasted_iota(jnp.int32, (sub, LANES), 1)
        packed = None
        for part in range(LANES // ROTARY_DIM):
            start = aligned(ids[0] * quarter + part * sub, 8)
            rows = both_ref[pl.ds(start, sub), :LANES]
            rows = jnp.where(lane // ROTARY_DIM == part, rows, 0.0)
            packed = rows if packed is None else packed + rows
        kv_ref[seg:, :] = packed.astype(jnp.bfloat16)
        kr_ref[...] = jnp.zeros_like(kr_ref)
    else:
        kr_ref[...] = turned


def normed_into(scratch, ids, pieces, gain_ref):
    width = pieces[0].shape[1]
    rows = scratch.shape[0]
    total = width * len(pieces)
    squares = None
    for piece in pieces:
        values = piece[:rows, :].astype(jnp.float32)
        part = jnp.sum(values * values, axis=-1, keepdims=True)
        squares = part if squares is None else squares + part
    factor = lax.rsqrt(squares / total + EPSILON)
    for number, piece in enumerate(pieces):
        if len(pieces) == 1:
            where = slice(None)
        else:
            where = pl.ds(aligned(ids[number] * width, LANES), width)
        gained = piece[:rows, :].astype(jnp.float32) * factor * gain_ref[:, where]
        scratch[:, where] = gained.astype(jnp.bfloat16)


def query_kernel(count, info, *refs):
    ids = member_ids(info, count)
    pieces = refs[:count]
    gain_ref, w_ref, table_ref, q_ref, scratch = refs[count:]
    normed_into(scratch, ids, pieces, gain_ref)
    rows = scratch.shape[0]
    raw = lax.dot_general(
        w_ref[...], scratch[...], (((1,), (1,)), ((), ())), preferred_element_type=jnp.float32
    )
    freq_count = ROTARY_DIM // 4
    tables = [table_ref[i * freq_count : (i + 1) * freq_count, :] for i in range(4)]
    span = PLAIN_QK_DIM + ROTARY_DIM
    q_ref[...] = jnp.zeros_like(q_ref)
    for head in range(2 * q_ref.shape[0]):
        half = head % 2
        lanes = slice(half * rows, (half + 1) * rows)
        start = head * span
        q_ref[head // 2, half * PLAIN_QK_DIM : (half + 1) * PLAIN_QK_DIM, lanes] = raw[
            start : start + PLAIN_QK_DIM
        ].astype(jnp.bfloat16)
        start += PLAIN_QK_DIM
        parts = [raw[start + i * freq_count : start + (i + 1) * freq_count] for i in range(4)]
        turned = []
        for axis in range(2):
            low, high = parts[2 * axis : 2 * axis + 2]
            cosine, sine_of = tables[2 * axis : 2 * axis + 2]
            turned += [low * cosine - high * sine_of, low * sine_of + high * cosine]
        q_ref[head // 2, LANES : LANES + ROTARY_DIM, lanes] = jnp.concatenate(
            turned, axis=0
        ).astype(jnp.bfloat16)


def fold_rows(values):
    return jnp.sum(values.reshape(-1, 8, values.shape[1]), axis=0)


def attend_kernel(counts, tok_keys, seg, merged, first, last, chosen, info, *refs):
    ids = member_ids(info, counts[0])
    bias_ref, q_ref, gain_ref, wk_ref, wv_ref = refs[:5]
    refs = refs[5:]
    blocks = []
    for count in counts:
        blocks.append(refs[: count + (0 if merged else 1)])
        refs = refs[len(blocks[-1]) :]
    if not first:
        state_in, refs = refs[:3], refs[3:]
    if last:
        out_ref, refs = refs[0], refs[1:]
    else:
        state_out, refs = refs[:3], refs[3:]
    scratch, k_ref, v_ref, r_ref = refs
    lanes = q_ref.shape[2]
    rows = lanes // 2
    heads_of = slice(chosen[0] * LANES, (chosen[-1] + 1) * LANES)
    for number, block in enumerate(blocks):
        pieces = block if merged else block[:-1]
        base = number * seg
        rows_ref = scratch.at[number]
        normed_into(rows_ref, ids, pieces, gain_ref)
        k_ref[base : base + seg, :] = f32_dot(rows_ref[...], wk_ref[:, heads_of]).astype(jnp.bfloat16)
        v_ref[number] = lax.dot_general(
            wv_ref[heads_of, :], rows_ref[...], (((1,), (1,)), ((), ())), preferred_element_type=jnp.float32
        ).astype(jnp.bfloat16)
        if merged:
            quarter = seg // len(pieces)
            sub = quarter // (LANES // ROTARY_DIM)
            for member, piece in enumerate(pieces):
                packed = piece[seg:, :].astype(jnp.float32)
                for part in range(LANES // ROTARY_DIM):
                    moved = pltpu.roll(packed, (-part * ROTARY_DIM) % LANES, 1) if part else packed
                    start = aligned(base + ids[member] * quarter + part * sub, 16)
                    r_ref[pl.ds(start, sub), :] = moved.astype(jnp.bfloat16)
        else:
            r_ref[base : base + seg, :] = block[-1][...]
    score_scale = (PLAIN_QK_DIM + ROTARY_DIM) ** (-0.5) * LOG2E
    lane = lax.broadcasted_iota(jnp.int32, (1, lanes), 1)

    def score(pair, number):
        base = number * seg
        local = pair - chosen[0]
        span = slice(local * LANES, (local + 1) * LANES)
        key = jnp.concatenate([k_ref[base : base + seg, span], r_ref[base : base + seg, :]], axis=1)
        return f32_dot(key, q_ref[pair])

    steps = [(pair, number) for pair in chosen for number in range(len(blocks))]
    ahead = score(*steps[0])
    for local, pair in enumerate(chosen):
        span = slice(local * LANES, (local + 1) * LANES)
        bias = jnp.where(lane < rows, bias_ref[2 * pair], bias_ref[2 * pair + 1]) * LOG2E
        top = total = acc = None
        if not first:
            top = state_in[0][pair, :1, :]
            total, acc = state_in[1][pair], state_in[2][pair]
        for number in range(len(blocks)):
            scores = ahead
            after = local * len(blocks) + number + 1
            if after < len(steps):
                ahead = score(*steps[after])
            lat, ctx = scores[:tok_keys], scores[tok_keys:]
            peak = jnp.maximum(
                jnp.max(lat, axis=0, keepdims=True) * score_scale,
                jnp.max(ctx, axis=0, keepdims=True) * score_scale + bias,
            )
            new_top = peak if top is None else jnp.maximum(top, peak)
            e_lat = jnp.exp2(lat * score_scale - new_top)
            e_ctx = jnp.exp2(ctx * score_scale - (new_top - bias))
            part = fold_rows(e_lat) + fold_rows(e_ctx)
            weights = jnp.concatenate([e_lat, e_ctx], axis=0).astype(jnp.bfloat16)
            both = f32_dot(v_ref[number, span, :], weights)
            gathered = jnp.concatenate([both[:VALUE_DIM, :rows], both[VALUE_DIM:, rows:]], axis=0)
            if top is None:
                total, acc = part, gathered
            else:
                rescale = jnp.exp2(top - new_top)
                total = total * rescale + part
                acc = gathered + jnp.concatenate(
                    [acc[:VALUE_DIM] * rescale[:, :rows], acc[VALUE_DIM:] * rescale[:, rows:]],
                    axis=0,
                )
            top = new_top
        if last:
            total = jnp.sum(total, axis=0, keepdims=True)
            done = jnp.concatenate(
                [acc[:VALUE_DIM] / total[:, :rows], acc[VALUE_DIM:] / total[:, rows:]], axis=0
            )
            out_ref[:, span] = done.T.astype(jnp.bfloat16)
        else:
            state_out[0][pair] = jnp.broadcast_to(top, (8, lanes))
            state_out[1][pair] = total
            state_out[2][pair] = acc


def out_kernel(count, splits, parts, info, *refs):
    ids = member_ids(info, count)
    pieces = refs[: count * splits]
    w_ref = refs[count * splits]
    refs = refs[1 + count * splits :]
    outs = refs[:parts]
    depth = pieces[0].shape[1]
    total = None
    for number, piece in enumerate(pieces):
        split, member = divmod(number, count)
        start = aligned((ids[member] * splits + split) * depth, LANES)
        part = f32_dot(piece[...], w_ref[pl.ds(start, depth), :])
        total = part if total is None else total + part
    if parts == 1:
        outs[0][...] = total.astype(jnp.bfloat16)
        return
    scratch = refs[parts]
    scratch[...] = total
    rows = outs[0].shape[0]
    for number, out_ref in enumerate(outs):
        start = aligned(ids[number] * rows, 8)
        out_ref[...] = scratch[pl.ds(start, rows), :].astype(jnp.bfloat16)


def final_kernel(count, mod_count, info, *refs):
    ids = member_ids(info, count)
    pieces = refs[:count]
    gates = refs[count : count + mod_count]
    lat_ref, out_ref = refs[count + mod_count :]
    width = pieces[0].shape[1]
    for number, (piece, gate) in enumerate(zip(pieces, gates)):
        span = pl.ds(aligned(ids[number] * width, LANES), width)
        out_ref[:, span] = (
            lat_ref[:, span].astype(jnp.float32)
            + gate[gate.shape[0] - 1 :, :] * piece[...].astype(jnp.float32)
        ).astype(jnp.bfloat16)


def call(kernel, outs, operands, smem=(), hbm=(), scratch=(), mib=16):
    specs = []
    for place_of in range(len(operands)):
        if place_of in hbm:
            specs.append(pl.BlockSpec(memory_space=pl.ANY))
        else:
            specs.append(in_smem() if place_of in smem else in_vmem())
    many = isinstance(outs, (list, tuple))
    return pl.pallas_call(
        kernel,
        out_shape=outs,
        in_specs=specs,
        out_specs=[in_vmem() for _ in outs] if many else in_vmem(),
        scratch_shapes=list(scratch),
        compiler_params=pltpu.CompilerParams(vmem_limit_bytes=mib * 1024 * 1024),
    )(*operands)


def on_device(
    latents,
    conditions,
    context,
    w_shift,
    w_scale,
    w_gate,
    w_qdown,
    w_kvdown,
    w_rope,
    q_gain,
    latent_norm_gain,
    query_up_weight,
    key_up_weight,
    value_up_weight,
    context_bias,
    w_out,
):
    tp_count = lax.axis_size("tp")
    sp_count = lax.axis_size("sp")
    own_rows, width = latents.shape
    tok_count = own_rows * tp_count
    ctx_rows = context.shape[0]
    seg_rows = tok_count + ctx_rows
    small = is_small(tp_count)
    members = jnp.arange(-1, tp_count, dtype=jnp.int32)
    info = jnp.where(
        members < 0, lax.axis_index("sp"), jnp.bitwise_xor(lax.axis_index("tp"), members)
    )
    info, conditions = lax.optimization_barrier((info, conditions))
    ids = member_ids(info, tp_count)
    bf16 = jnp.bfloat16

    shape_of = jax.ShapeDtypeStruct

    lat_blocks = spread(latents)
    cond_act = jax.nn.silu(conditions).astype(bf16)
    partial_mod = jnp.concatenate(
        [f32_dot(cond_act, w_shift), f32_dot(cond_act, w_scale), f32_dot(cond_act[0:1], w_gate)],
        axis=0,
    )
    mod_pieces = spread(add_up(partial_mod, "sp"))

    head_count = query_up_weight.shape[1] // (PLAIN_QK_DIM + ROTARY_DIM)
    pairs = head_count // 2
    k_cosine, k_sine, q_table = call(
        functools.partial(tables_kernel, tok_count),
        [
            shape_of((seg_rows, LANES), jnp.float32),
            shape_of((seg_rows, LANES), jnp.float32),
            shape_of((ROTARY_DIM, tok_count), jnp.float32),
        ],
        [info],
        smem=(0,),
    )
    kv_cols = w_kvdown.shape[1]
    q_cols = w_qdown.shape[1]

    w_q, w_kr = call(
        weights_kernel,
        [shape_of(w_qdown.shape, bf16), shape_of((width, LANES + kv_cols), bf16)],
        [w_qdown, w_kvdown, w_rope.T],
        hbm=(0,),
        scratch=[pltpu.SemaphoreType.DMA],
    )
    if own_rows % 16 or not small:
        lat_blocks = [place(lat_blocks, ids, 0)]
        order = [0]
    else:
        order = [0, 1] + list(range(2, tp_count)) if tp_count > 1 else [0]
    early_of = [lat_blocks[member] for member in order[:2]] if len(order) > 2 else []
    late_of = [lat_blocks[member] for member in order[len(early_of) :]]
    normed = call(
        functools.partial(early_kernel, len(early_of) + 1),
        [shape_of(value.shape, jnp.float32) for value in [*early_of, context]],
        [*early_of, context],
        mib=12,
    )
    w_qt, w_k, w_vt, w_o = call(
        fetch_kernel,
        [
            shape_of(query_up_weight.shape[::-1], bf16),
            shape_of(key_up_weight.shape, bf16),
            shape_of(value_up_weight.shape[::-1], bf16),
            shape_of(w_out.shape, bf16),
        ],
        [query_up_weight, key_up_weight, value_up_weight, w_out],
        hbm=(1, 3),
        scratch=[pltpu.SemaphoreType.DMA((2,))],
    )
    merged = (
        kv_cols % LANES == 0
        and seg_rows % (16 * tp_count * LANES // ROTARY_DIM) == 0
        and small
        and is_small(sp_count)
    )
    extra = seg_rows // tp_count * ROTARY_DIM // LANES if merged else 0
    late_rows = [value.shape[0] for value in late_of]
    early_rows = [value.shape[0] for value in early_of]
    cq_cols, kv_own, kr_own = call(
        functools.partial(down_kernel, early_rows, late_rows, tp_count, tok_count, merged),
        [
            shape_of((tok_count, q_cols), bf16),
            shape_of((seg_rows + extra, kv_cols), bf16),
            shape_of((16 if merged else seg_rows, LANES), bf16),
        ],
        [
            info,
            *normed[:-1],
            *late_of,
            *mod_pieces,
            normed[-1],
            w_q,
            w_kr,
            k_cosine,
            k_sine,
        ],
        smem=(0,),
        scratch=[
            VMEM((sum(early_rows) + ctx_rows, width), bf16),
            VMEM((sum(late_rows), width), bf16),
            VMEM((5, width), jnp.float32),
            VMEM((seg_rows, LANES + kv_cols), jnp.float32),
        ],
        mib=16,
    )

    def columns(value):
        pieces = spread(value)
        if value.shape[1] % LANES:
            return [place(pieces, ids, 1)]
        return pieces

    if is_small(sp_count):
        blocks = []
        for member in range(sp_count):
            moved = swap(kv_own, "sp", member) if member else kv_own
            block = columns(moved)
            if not merged:
                block.append(swap(kr_own, "sp", member) if member else kr_own)
            blocks.append(block)
    else:
        kr_blocks = lax.all_gather(kr_own, "sp")
        whole_rows = lax.all_gather(kv_own, "tp", axis=1, tiled=True)
        kv_blocks = lax.all_gather(whole_rows, "sp")
        blocks = [[kv, kr] for kv, kr in zip(kv_blocks, kr_blocks)]
    cq_pieces = columns(cq_cols)
    queries = call(
        functools.partial(query_kernel, len(cq_pieces)),
        shape_of((pairs, 2 * LANES, 2 * tok_count), bf16),
        [info, *cq_pieces, q_gain[None, :], w_qt, q_table],
        smem=(0,),
        scratch=[VMEM((tok_count, q_gain.shape[0]), bf16)],
    )
    held = [
        shape_of((pairs, 8, 2 * tok_count), jnp.float32),
        shape_of((pairs, 8, 2 * tok_count), jnp.float32),
        shape_of((pairs, LANES, tok_count), jnp.float32),
    ]

    def attend(part, first, last, chosen, state):
        heads = len(chosen) * LANES
        return call(
            functools.partial(
                attend_kernel,
                [len(block) - (0 if merged else 1) for block in part],
                tok_count,
                seg_rows,
                merged,
                first,
                last,
                chosen,
            ),
            shape_of((tok_count, heads), bf16) if last else held,
            [
                info,
                context_bias,
                queries,
                latent_norm_gain[None, :],
                w_k,
                w_vt,
                *[piece for block in part for piece in block],
                *state,
            ],
            smem=(0, 1),
            scratch=[
                VMEM((len(part), seg_rows, latent_norm_gain.shape[0]), bf16),
                VMEM((len(part) * seg_rows, heads), bf16),
                VMEM((len(part), heads, seg_rows), bf16),
                VMEM((len(part) * seg_rows, LANES), bf16),
            ],
            mib=16,
        )

    every = list(range(pairs))
    state = []
    begin = 0
    att_pieces = []
    while begin < sp_count:
        part = blocks[begin : begin + (1 if begin < 2 else 2)]
        first, last = begin == 0, begin + len(part) >= sp_count
        if not last:
            state = attend(part, first, False, every, state)
        begin += len(part)
    splits = [every[: pairs // 2], every[pairs // 2 :]] if pairs > 1 else [every]
    for chosen in splits:
        done = attend(part, first, True, chosen, state)
        att_pieces.append(spread(done))
    out_cols = w_out.shape[1]
    parts = tp_count if small and own_rows % 8 == 0 else 1
    proj = call(
        functools.partial(out_kernel, tp_count, len(att_pieces), parts),
        [shape_of((tok_count // parts, out_cols), bf16) for _ in range(parts)],
        [info, *[piece for group in att_pieces for piece in group], w_o],
        smem=(0,),
        scratch=[VMEM((tok_count, out_cols), jnp.float32)] if parts > 1 else [],
    )
    if parts > 1:
        proj_pieces = [
            swap(value, "tp", member) if member else value
            for member, value in enumerate(proj)
        ]
    else:
        by_owner = proj[0].reshape(tp_count, own_rows, out_cols)
        proj_pieces = list(lax.all_to_all(by_owner, "tp", 0, 0))
        if small:
            proj_pieces = [
                lax.dynamic_index_in_dim(jnp.stack(proj_pieces), ids[member], 0, False)
                for member in range(tp_count)
            ]
    return call(
        functools.partial(final_kernel, tp_count, tp_count),
        shape_of((own_rows, width), bf16),
        [info, *proj_pieces, *mod_pieces, latents],
        smem=(0,),
    )


def solution(mesh):
    in_specs = (
        P(("grp", "sp", "tp"), None),
        P("grp", "sp"),
        P(("grp", "sp"), None),
        P("sp", "tp"),
        P("sp", "tp"),
        P("sp", "tp"),
        P(None, "tp"),
        P(None, "tp"),
        P(),
        P(),
        P(),
        P(None, "tp"),
        P(None, "tp"),
        P(None, "tp"),
        P("tp"),
        P(None, "tp"),
    )
    out_specs = P(("grp", "sp", "tp"), None)
    step = jax.shard_map(
        on_device, mesh=mesh, in_specs=in_specs, out_specs=out_specs, check_vma=False
    )
    if not (is_small(mesh.shape["tp"]) and is_small(mesh.shape["sp"])):
        return step
    return step
```

```python
import functools

import jax
import jax.numpy as jnp
from jax import lax
from jax.experimental import pallas as pl
from jax.experimental.pallas import tpu as pltpu
from jax.sharding import PartitionSpec as P


PLAIN_QK_DIM = 64
ROTARY_DIM = 32
VALUE_DIM = 64
GRID_W = 64
LANES = 128
LOG2E = 1.4426950408889634

EPSILON = 1e-06


VMEM = pltpu.VMEM
SMEM = pltpu.SMEM


def in_vmem():
    return pl.BlockSpec(memory_space=VMEM)


def in_smem():
    return pl.BlockSpec(memory_space=SMEM)


def f32_dot(a, b):
    return jnp.dot(a, b, preferred_element_type=jnp.float32)


def swap(value, axis, bit):
    count = lax.axis_size(axis)
    return lax.ppermute(value, axis, [(i, i ^ bit) for i in range(count)])


def is_small(count):
    return count <= 4


def tp_bits(count):
    bits = []
    bit = 2
    while bit < count:
        bits.append(bit)
        bit *= 2
    if count > 1:
        bits.append(1)
    return bits


def spread(value, axis="tp"):
    if not is_small(lax.axis_size(axis)):
        return list(lax.all_gather(value, axis))
    got = {0: value}
    for bit in tp_bits(lax.axis_size(axis)):
        for member in list(got):
            got[member ^ bit] = swap(got[member], axis, bit)
    return [got[member] for member in range(len(got))]


def add_up(value, axis):
    count = lax.axis_size(axis)
    if not is_small(count):
        return lax.psum(value, axis)
    bit = 1
    while bit < count:
        value = value + swap(value, axis, bit)
        bit *= 2
    return value


def place(pieces, ids, axis):
    width = pieces[0].shape[axis]
    shape = list(pieces[0].shape)
    shape[axis] = width * len(pieces)
    whole = jnp.zeros(shape, pieces[0].dtype)
    for member, piece in enumerate(pieces):
        whole = lax.dynamic_update_slice_in_dim(whole, piece, ids[member] * width, axis)
    return whole


def angles(position, frequency, use_column):
    freq_count = ROTARY_DIM // 4
    inverse = jnp.zeros(frequency.shape, jnp.float32)
    for number in range(freq_count):
        inverse = jnp.where(
            frequency == number, jnp.float32(10000.0 ** (-number / freq_count)), inverse
        )
    coordinate = jnp.where(use_column, position % GRID_W, position // GRID_W)
    return coordinate.astype(jnp.float32) * inverse


def tables_kernel(tok_count, info, cos_ref, sin_ref, table_ref):
    freq_count = ROTARY_DIM // 4
    start = info[0] * tok_count
    shape = cos_ref.shape
    row = lax.broadcasted_iota(jnp.int32, shape, 0)
    lane = lax.broadcasted_iota(jnp.int32, shape, 1)
    angle = angles(start + row, lane % freq_count, (lane // (2 * freq_count)) % 2 == 1)
    is_lat = row < tok_count
    cos_ref[...] = jnp.where(is_lat, jnp.cos(angle), 1.0)
    sine_of = jnp.where((lane // freq_count) % 2 == 0, -jnp.sin(angle), jnp.sin(angle))
    sin_ref[...] = jnp.where(is_lat, sine_of, 0.0)
    shape = table_ref.shape
    row = lax.broadcasted_iota(jnp.int32, shape, 0)
    lane = lax.broadcasted_iota(jnp.int32, shape, 1)
    angle = angles(start + lane, row % freq_count, row // (2 * freq_count) == 1)
    table_ref[...] = jnp.where((row // freq_count) % 2 == 0, jnp.cos(angle), jnp.sin(angle))


def turn(values, cosine, sine_of):
    freq_count = ROTARY_DIM // 4
    lanes = values.shape[1]
    lane = lax.broadcasted_iota(jnp.int32, values.shape, 1)
    first = (lane % (2 * freq_count)) < freq_count
    partner = jnp.where(
        first, pltpu.roll(values, lanes - freq_count, 1), pltpu.roll(values, freq_count, 1)
    )
    return values * cosine + partner * sine_of


class Members:
    def __init__(self, info):
        self.info = info

    def __getitem__(self, member):
        return self.info[1 + member]


def member_ids(info, count):
    return Members(info) if is_small(count) else list(range(count))


def aligned(value, step):
    return value if isinstance(value, int) else pl.multiple_of(value, step)


def gather_rows(scratch, ids, pieces):
    width = pieces[0].shape[1]
    for number, piece in enumerate(pieces):
        scratch[:, pl.ds(aligned(ids[number] * width, LANES), width)] = piece[...]


def normalize(values):
    center = values - jnp.mean(values, axis=-1, keepdims=True)
    spread_of = jnp.mean(center * center, axis=-1, keepdims=True)
    return center * lax.rsqrt(spread_of + EPSILON)


def weights_kernel(wq_hbm, wk_ref, rope_ref, wq_ref, wkr_ref, sem):
    copy = pltpu.make_async_copy(wq_hbm, wq_ref, sem)
    copy.start()
    wkr_ref[:, LANES:] = wk_ref[...]
    copies = (
        lax.broadcasted_iota(jnp.int32, (ROTARY_DIM, LANES), 0)
        == lax.broadcasted_iota(jnp.int32, (ROTARY_DIM, LANES), 1) % ROTARY_DIM
    ).astype(jnp.bfloat16)
    wkr_ref[:, :LANES] = lax.dot_general(
        rope_ref[...], copies, (((0,), (0,)), ((), ())), preferred_element_type=jnp.float32
    ).astype(jnp.bfloat16)
    copy.wait()


def early_kernel(count, *refs):
    for source, out_ref in zip(refs[:count], refs[count:]):
        for row in range(0, source.shape[0], 16):
            values = source[row : row + 16, :].astype(jnp.float32)
            out_ref[row : row + 16, :] = normalize(values)


def fetch_kernel(wq_ref, wk_hbm, wv_ref, wo_hbm, wqt_ref, wk_ref, wvt_ref, wo_ref, sems):
    copies = [
        pltpu.make_async_copy(wk_hbm, wk_ref, sems.at[0]),
        pltpu.make_async_copy(wo_hbm, wo_ref, sems.at[1]),
    ]
    for copy in copies:
        copy.start()
    wqt_ref[...] = wq_ref[...].astype(jnp.float32).T.astype(jnp.bfloat16)
    wvt_ref[...] = wv_ref[...].astype(jnp.float32).T.astype(jnp.bfloat16)
    for copy in copies:
        copy.wait()


def down_kernel(early_rows, late_rows, mod_count, tok_count, merged, info, *refs):
    ids = member_ids(info, mod_count)
    offsets = [0] if len(early_rows) + len(late_rows) == 1 else ids
    early, refs = refs[: len(early_rows)], refs[len(early_rows) :]
    late, refs = refs[: len(late_rows)], refs[len(late_rows) :]
    pieces, refs = refs[:mod_count], refs[mod_count:]
    ctx_ref, wq_ref, wkr_ref, cos_ref, sin_ref = refs[:5]
    cq_ref, kv_ref, kr_ref, ha_ref, hb_ref, mod_ref, both_ref = refs[5:]
    step = 16
    gather_rows(mod_ref, ids, pieces)

    def modulate(source, target, base, rows, is_ctx, is_normed):
        shift_by = mod_ref[is_ctx : is_ctx + 1, :]
        scale_by = 1.0 + mod_ref[2 + is_ctx : 3 + is_ctx, :]
        for row in range(0, rows, step):
            values = source[row : row + step, :]
            if not is_normed:
                values = normalize(values.astype(jnp.float32))
            target[base + row : base + row + step, :] = (values * scale_by + shift_by).astype(
                jnp.bfloat16
            )

    def multiply(source, rows_of, first, with_ctx):
        cq = f32_dot(source[...], wq_ref[...])
        both = f32_dot(source[...], wkr_ref[...])
        base = 0
        for number, rows in enumerate(rows_of):
            start = aligned(offsets[first + number] * rows, 16)
            cq_ref[pl.ds(start, rows), :] = cq[base : base + rows].astype(jnp.bfloat16)
            both_ref[pl.ds(start, rows), :] = both[base : base + rows]
            base += rows
        if with_ctx:
            both_ref[tok_count:, :] = both[base:]

    base = 0
    for source, rows in zip(early, early_rows):
        modulate(source, ha_ref, base, rows, 0, True)
        base += rows
    modulate(ctx_ref, ha_ref, base, ctx_ref.shape[0], 1, True)
    multiply(ha_ref, early_rows, 0, True)
    base = 0
    for source, rows in zip(late, late_rows):
        modulate(source, hb_ref, base, rows, 0, False)
        base += rows
    multiply(hb_ref, late_rows, len(early_rows), False)
    seg = both_ref.shape[0]
    kv_ref[:seg, :] = both_ref[:, LANES:].astype(jnp.bfloat16)
    turned = turn(both_ref[:, :LANES], cos_ref[...], sin_ref[...]).astype(jnp.bfloat16)
    if merged:
        both_ref[:, :LANES] = turned.astype(jnp.float32)
        quarter = seg // mod_count
        sub = quarter // (LANES // ROTARY_DIM)
        lane = lax.broadcasted_iota(jnp.int32, (sub, LANES), 1)
        packed = None
        for part in range(LANES // ROTARY_DIM):
            start = aligned(ids[0] * quarter + part * sub, 8)
            rows = both_ref[pl.ds(start, sub), :LANES]
            rows = jnp.where(lane // ROTARY_DIM == part, rows, 0.0)
            packed = rows if packed is None else packed + rows
        kv_ref[seg:, :] = packed.astype(jnp.bfloat16)
        kr_ref[...] = jnp.zeros_like(kr_ref)
    else:
        kr_ref[...] = turned


def normed_into(scratch, ids, pieces, gain_ref):
    width = pieces[0].shape[1]
    rows = scratch.shape[0]
    total = width * len(pieces)
    squares = None
    for piece in pieces:
        values = piece[:rows, :].astype(jnp.float32)
        part = jnp.sum(values * values, axis=-1, keepdims=True)
        squares = part if squares is None else squares + part
    factor = lax.rsqrt(squares / total + EPSILON)
    for number, piece in enumerate(pieces):
        if len(pieces) == 1:
            where = slice(None)
        else:
            where = pl.ds(aligned(ids[number] * width, LANES), width)
        gained = piece[:rows, :].astype(jnp.float32) * factor * gain_ref[:, where]
        scratch[:, where] = gained.astype(jnp.bfloat16)


def query_kernel(count, info, *refs):
    ids = member_ids(info, count)
    pieces = refs[:count]
    gain_ref, w_ref, table_ref, q_ref, scratch = refs[count:]
    normed_into(scratch, ids, pieces, gain_ref)
    rows = scratch.shape[0]
    raw = lax.dot_general(
        w_ref[...], scratch[...], (((1,), (1,)), ((), ())), preferred_element_type=jnp.float32
    )
    freq_count = ROTARY_DIM // 4
    tables = [table_ref[i * freq_count : (i + 1) * freq_count, :] for i in range(4)]
    span = PLAIN_QK_DIM + ROTARY_DIM
    q_ref[...] = jnp.zeros_like(q_ref)
    for head in range(2 * q_ref.shape[0]):
        half = head % 2
        lanes = slice(half * rows, (half + 1) * rows)
        start = head * span
        q_ref[head // 2, half * PLAIN_QK_DIM : (half + 1) * PLAIN_QK_DIM, lanes] = raw[
            start : start + PLAIN_QK_DIM
        ].astype(jnp.bfloat16)
        start += PLAIN_QK_DIM
        parts = [raw[start + i * freq_count : start + (i + 1) * freq_count] for i in range(4)]
        turned = []
        for axis in range(2):
            low, high = parts[2 * axis : 2 * axis + 2]
            cosine, sine_of = tables[2 * axis : 2 * axis + 2]
            turned += [low * cosine - high * sine_of, low * sine_of + high * cosine]
        q_ref[head // 2, LANES : LANES + ROTARY_DIM, lanes] = jnp.concatenate(
            turned, axis=0
        ).astype(jnp.bfloat16)


def fold_rows(values):
    return jnp.sum(values.reshape(-1, 8, values.shape[1]), axis=0)


def attend_kernel(counts, tok_keys, seg, merged, first, last, chosen, info, *refs):
    ids = member_ids(info, counts[0])
    bias_ref, q_ref, gain_ref, wk_ref, wv_ref = refs[:5]
    refs = refs[5:]
    blocks = []
    for count in counts:
        blocks.append(refs[: count + (0 if merged else 1)])
        refs = refs[len(blocks[-1]) :]
    if not first:
        state_in, refs = refs[:3], refs[3:]
    if last:
        out_ref, refs = refs[0], refs[1:]
    else:
        state_out, refs = refs[:3], refs[3:]
    scratch, k_ref, v_ref, r_ref = refs
    lanes = q_ref.shape[2]
    rows = lanes // 2
    heads_of = slice(chosen[0] * LANES, (chosen[-1] + 1) * LANES)
    for number, block in enumerate(blocks):
        pieces = block if merged else block[:-1]
        base = number * seg
        rows_ref = scratch.at[number]
        normed_into(rows_ref, ids, pieces, gain_ref)
        k_ref[base : base + seg, :] = f32_dot(rows_ref[...], wk_ref[:, heads_of]).astype(jnp.bfloat16)
        v_ref[number] = lax.dot_general(
            wv_ref[heads_of, :], rows_ref[...], (((1,), (1,)), ((), ())), preferred_element_type=jnp.float32
        ).astype(jnp.bfloat16)
        if merged:
            quarter = seg // len(pieces)
            sub = quarter // (LANES // ROTARY_DIM)
            for member, piece in enumerate(pieces):
                packed = piece[seg:, :].astype(jnp.float32)
                for part in range(LANES // ROTARY_DIM):
                    moved = pltpu.roll(packed, (-part * ROTARY_DIM) % LANES, 1) if part else packed
                    start = aligned(base + ids[member] * quarter + part * sub, 16)
                    r_ref[pl.ds(start, sub), :] = moved.astype(jnp.bfloat16)
        else:
            r_ref[base : base + seg, :] = block[-1][...]
    score_scale = (PLAIN_QK_DIM + ROTARY_DIM) ** (-0.5) * LOG2E
    lane = lax.broadcasted_iota(jnp.int32, (1, lanes), 1)

    def score(pair, number):
        base = number * seg
        local = pair - chosen[0]
        span = slice(local * LANES, (local + 1) * LANES)
        key = jnp.concatenate([k_ref[base : base + seg, span], r_ref[base : base + seg, :]], axis=1)
        return f32_dot(key, q_ref[pair])

    steps = [(pair, number) for pair in chosen for number in range(len(blocks))]
    ahead = score(*steps[0])
    for local, pair in enumerate(chosen):
        span = slice(local * LANES, (local + 1) * LANES)
        bias = jnp.where(lane < rows, bias_ref[2 * pair], bias_ref[2 * pair + 1]) * LOG2E
        top = total = acc = None
        if not first:
            top = state_in[0][pair, :1, :]
            total, acc = state_in[1][pair], state_in[2][pair]
        for number in range(len(blocks)):
            scores = ahead
            after = local * len(blocks) + number + 1
            if after < len(steps):
                ahead = score(*steps[after])
            lat, ctx = scores[:tok_keys], scores[tok_keys:]
            peak = jnp.maximum(
                jnp.max(lat, axis=0, keepdims=True) * score_scale,
                jnp.max(ctx, axis=0, keepdims=True) * score_scale + bias,
            )
            new_top = peak if top is None else jnp.maximum(top, peak)
            e_lat = jnp.exp2(lat * score_scale - new_top)
            e_ctx = jnp.exp2(ctx * score_scale - (new_top - bias))
            part = fold_rows(e_lat) + fold_rows(e_ctx)
            weights = jnp.concatenate([e_lat, e_ctx], axis=0).astype(jnp.bfloat16)
            both = f32_dot(v_ref[number, span, :], weights)
            gathered = jnp.concatenate([both[:VALUE_DIM, :rows], both[VALUE_DIM:, rows:]], axis=0)
            if top is None:
                total, acc = part, gathered
            else:
                rescale = jnp.exp2(top - new_top)
                total = total * rescale + part
                acc = gathered + jnp.concatenate(
                    [acc[:VALUE_DIM] * rescale[:, :rows], acc[VALUE_DIM:] * rescale[:, rows:]],
                    axis=0,
                )
            top = new_top
        if last:
            total = jnp.sum(total, axis=0, keepdims=True)
            done = jnp.concatenate(
                [acc[:VALUE_DIM] / total[:, :rows], acc[VALUE_DIM:] / total[:, rows:]], axis=0
            )
            out_ref[:, span] = done.T.astype(jnp.bfloat16)
        else:
            state_out[0][pair] = jnp.broadcast_to(top, (8, lanes))
            state_out[1][pair] = total
            state_out[2][pair] = acc


def out_kernel(count, splits, parts, wanted, info, *refs):
    ids = member_ids(info, count)
    pieces = refs[: count * splits]
    w_ref = refs[count * splits]
    outs = refs[1 + count * splits :]
    depth = pieces[0].shape[1]
    rows = outs[0].shape[0]
    for place_of in range(0, len(wanted), 2):
        group = wanted[place_of : place_of + 2]
        total = None
        for number, piece in enumerate(pieces):
            split, member = divmod(number, count)
            start = aligned((ids[member] * splits + split) * depth, LANES)
            if parts == 1:
                left = piece[...]
            else:
                left = jnp.concatenate(
                    [piece[pl.ds(aligned(ids[owner] * rows, 16), rows), :] for owner in group],
                    axis=0,
                )
            part = f32_dot(left, w_ref[pl.ds(start, depth), :])
            total = part if total is None else total + part
        for number in range(len(group)):
            outs[place_of + number][...] = total[number * rows : (number + 1) * rows].astype(
                jnp.bfloat16
            )


def final_kernel(count, mod_count, info, *refs):
    ids = member_ids(info, count)
    pieces = refs[:count]
    gates = refs[count : count + mod_count]
    lat_ref, out_ref = refs[count + mod_count :]
    width = pieces[0].shape[1]
    for number, (piece, gate) in enumerate(zip(pieces, gates)):
        span = pl.ds(aligned(ids[number] * width, LANES), width)
        out_ref[:, span] = (
            lat_ref[:, span].astype(jnp.float32)
            + gate[gate.shape[0] - 1 :, :] * piece[...].astype(jnp.float32)
        ).astype(jnp.bfloat16)


def call(kernel, outs, operands, smem=(), hbm=(), scratch=(), mib=16):
    specs = []
    for place_of in range(len(operands)):
        if place_of in hbm:
            specs.append(pl.BlockSpec(memory_space=pl.ANY))
        else:
            specs.append(in_smem() if place_of in smem else in_vmem())
    many = isinstance(outs, (list, tuple))
    return pl.pallas_call(
        kernel,
        out_shape=outs,
        in_specs=specs,
        out_specs=[in_vmem() for _ in outs] if many else in_vmem(),
        scratch_shapes=list(scratch),
        compiler_params=pltpu.CompilerParams(vmem_limit_bytes=mib * 1024 * 1024),
    )(*operands)


def on_device(
    latents,
    conditions,
    context,
    w_shift,
    w_scale,
    w_gate,
    w_qdown,
    w_kvdown,
    w_rope,
    q_gain,
    latent_norm_gain,
    query_up_weight,
    key_up_weight,
    value_up_weight,
    context_bias,
    w_out,
):
    tp_count = lax.axis_size("tp")
    sp_count = lax.axis_size("sp")
    own_rows, width = latents.shape
    tok_count = own_rows * tp_count
    ctx_rows = context.shape[0]
    seg_rows = tok_count + ctx_rows
    small = is_small(tp_count)
    members = jnp.arange(-1, tp_count, dtype=jnp.int32)
    info = jnp.where(
        members < 0, lax.axis_index("sp"), jnp.bitwise_xor(lax.axis_index("tp"), members)
    )
    info, conditions = lax.optimization_barrier((info, conditions))
    ids = member_ids(info, tp_count)
    bf16 = jnp.bfloat16

    shape_of = jax.ShapeDtypeStruct

    lat_blocks = spread(latents)
    cond_act = jax.nn.silu(conditions).astype(bf16)
    partial_mod = jnp.concatenate(
        [f32_dot(cond_act, w_shift), f32_dot(cond_act, w_scale), f32_dot(cond_act[0:1], w_gate)],
        axis=0,
    )
    mod_pieces = spread(add_up(partial_mod, "sp"))

    head_count = query_up_weight.shape[1] // (PLAIN_QK_DIM + ROTARY_DIM)
    pairs = head_count // 2
    k_cosine, k_sine, q_table = call(
        functools.partial(tables_kernel, tok_count),
        [
            shape_of((seg_rows, LANES), jnp.float32),
            shape_of((seg_rows, LANES), jnp.float32),
            shape_of((ROTARY_DIM, tok_count), jnp.float32),
        ],
        [info],
        smem=(0,),
    )
    kv_cols = w_kvdown.shape[1]
    q_cols = w_qdown.shape[1]

    w_q, w_kr = call(
        weights_kernel,
        [shape_of(w_qdown.shape, bf16), shape_of((width, LANES + kv_cols), bf16)],
        [w_qdown, w_kvdown, w_rope.T],
        hbm=(0,),
        scratch=[pltpu.SemaphoreType.DMA],
    )
    if own_rows % 16 or not small:
        lat_blocks = [place(lat_blocks, ids, 0)]
        order = [0]
    else:
        order = [0, 1] + list(range(2, tp_count)) if tp_count > 1 else [0]
    early_of = [lat_blocks[member] for member in order[:2]] if len(order) > 2 else []
    late_of = [lat_blocks[member] for member in order[len(early_of) :]]
    normed = call(
        functools.partial(early_kernel, len(early_of) + 1),
        [shape_of(value.shape, jnp.float32) for value in [*early_of, context]],
        [*early_of, context],
        mib=12,
    )
    w_qt, w_k, w_vt, w_o = call(
        fetch_kernel,
        [
            shape_of(query_up_weight.shape[::-1], bf16),
            shape_of(key_up_weight.shape, bf16),
            shape_of(value_up_weight.shape[::-1], bf16),
            shape_of(w_out.shape, bf16),
        ],
        [query_up_weight, key_up_weight, value_up_weight, w_out],
        hbm=(1, 3),
        scratch=[pltpu.SemaphoreType.DMA((2,))],
    )
    merged = (
        kv_cols % LANES == 0
        and seg_rows % (16 * tp_count * LANES // ROTARY_DIM) == 0
        and small
        and is_small(sp_count)
    )
    extra = seg_rows // tp_count * ROTARY_DIM // LANES if merged else 0
    late_rows = [value.shape[0] for value in late_of]
    early_rows = [value.shape[0] for value in early_of]
    cq_cols, kv_own, kr_own = call(
        functools.partial(down_kernel, early_rows, late_rows, tp_count, tok_count, merged),
        [
            shape_of((tok_count, q_cols), bf16),
            shape_of((seg_rows + extra, kv_cols), bf16),
            shape_of((16 if merged else seg_rows, LANES), bf16),
        ],
        [
            info,
            *normed[:-1],
            *late_of,
            *mod_pieces,
            normed[-1],
            w_q,
            w_kr,
            k_cosine,
            k_sine,
        ],
        smem=(0,),
        scratch=[
            VMEM((sum(early_rows) + ctx_rows, width), bf16),
            VMEM((sum(late_rows), width), bf16),
            VMEM((5, width), jnp.float32),
            VMEM((seg_rows, LANES + kv_cols), jnp.float32),
        ],
        mib=16,
    )

    def columns(value):
        pieces = spread(value)
        if value.shape[1] % LANES:
            return [place(pieces, ids, 1)]
        return pieces

    if is_small(sp_count):
        blocks = []
        for member in range(sp_count):
            moved = swap(kv_own, "sp", member) if member else kv_own
            block = columns(moved)
            if not merged:
                block.append(swap(kr_own, "sp", member) if member else kr_own)
            blocks.append(block)
    else:
        kr_blocks = lax.all_gather(kr_own, "sp")
        whole_rows = lax.all_gather(kv_own, "tp", axis=1, tiled=True)
        kv_blocks = lax.all_gather(whole_rows, "sp")
        blocks = [[kv, kr] for kv, kr in zip(kv_blocks, kr_blocks)]
    cq_pieces = columns(cq_cols)
    queries = call(
        functools.partial(query_kernel, len(cq_pieces)),
        shape_of((pairs, 2 * LANES, 2 * tok_count), bf16),
        [info, *cq_pieces, q_gain[None, :], w_qt, q_table],
        smem=(0,),
        scratch=[VMEM((tok_count, q_gain.shape[0]), bf16)],
    )
    held = [
        shape_of((pairs, 8, 2 * tok_count), jnp.float32),
        shape_of((pairs, 8, 2 * tok_count), jnp.float32),
        shape_of((pairs, LANES, tok_count), jnp.float32),
    ]

    def attend(part, first, last, chosen, state):
        heads = len(chosen) * LANES
        return call(
            functools.partial(
                attend_kernel,
                [len(block) - (0 if merged else 1) for block in part],
                tok_count,
                seg_rows,
                merged,
                first,
                last,
                chosen,
            ),
            shape_of((tok_count, heads), bf16) if last else held,
            [
                info,
                context_bias,
                queries,
                latent_norm_gain[None, :],
                w_k,
                w_vt,
                *[piece for block in part for piece in block],
                *state,
            ],
            smem=(0, 1),
            scratch=[
                VMEM((len(part), seg_rows, latent_norm_gain.shape[0]), bf16),
                VMEM((len(part) * seg_rows, heads), bf16),
                VMEM((len(part), heads, seg_rows), bf16),
                VMEM((len(part) * seg_rows, LANES), bf16),
            ],
            mib=16,
        )

    every = list(range(pairs))
    state = []
    begin = 0
    att_pieces = []
    while begin < sp_count:
        part = blocks[begin : begin + (1 if begin < 2 else 2)]
        first, last = begin == 0, begin + len(part) >= sp_count
        if not last:
            state = attend(part, first, False, every, state)
        begin += len(part)
    splits = [every[: pairs // 2], every[pairs // 2 :]] if pairs > 1 else [every]
    for chosen in splits:
        done = attend(part, first, True, chosen, state)
        att_pieces.append(spread(done))
    out_cols = w_out.shape[1]
    parts = tp_count if small and own_rows % 16 == 0 else 1
    if parts > 2:
        turns = [list(range(2, parts)), [0, 1]]
    else:
        turns = [list(range(parts))]
    proj = {}
    for wanted in turns:
        emitted = call(
            functools.partial(out_kernel, tp_count, len(att_pieces), parts, wanted),
            [shape_of((tok_count // parts, out_cols), bf16) for _ in wanted],
            [info, *[piece for group in att_pieces for piece in group], w_o],
            smem=(0,),
        )
        proj.update(zip(wanted, emitted))
    if parts > 1:
        proj_pieces = [
            swap(value, "tp", member) if member else value
            for member, value in sorted(proj.items())
        ]
    else:
        by_owner = proj[0].reshape(tp_count, own_rows, out_cols)
        proj_pieces = list(lax.all_to_all(by_owner, "tp", 0, 0))
        if small:
            proj_pieces = [
                lax.dynamic_index_in_dim(jnp.stack(proj_pieces), ids[member], 0, False)
                for member in range(tp_count)
            ]
    return call(
        functools.partial(final_kernel, tp_count, tp_count),
        shape_of((own_rows, width), bf16),
        [info, *proj_pieces, *mod_pieces, latents],
        smem=(0,),
    )


def solution(mesh):
    in_specs = (
        P(("grp", "sp", "tp"), None),
        P("grp", "sp"),
        P(("grp", "sp"), None),
        P("sp", "tp"),
        P("sp", "tp"),
        P("sp", "tp"),
        P(None, "tp"),
        P(None, "tp"),
        P(),
        P(),
        P(),
        P(None, "tp"),
        P(None, "tp"),
        P(None, "tp"),
        P("tp"),
        P(None, "tp"),
    )
    out_specs = P(("grp", "sp", "tp"), None)
    step = jax.shard_map(
        on_device, mesh=mesh, in_specs=in_specs, out_specs=out_specs, check_vma=False
    )
    if not (is_small(mesh.shape["tp"]) and is_small(mesh.shape["sp"])):
        return step
    return step
```

```python
import functools

import jax
import jax.numpy as jnp
from jax import lax
from jax.experimental import pallas as pl
from jax.experimental.pallas import tpu as pltpu
from jax.sharding import PartitionSpec as P


PLAIN_QK_DIM = 64
ROTARY_DIM = 32
VALUE_DIM = 64
GRID_W = 64
LANES = 128
LOG2E = 1.4426950408889634

EPSILON = 1e-06


VMEM = pltpu.VMEM
SMEM = pltpu.SMEM


def in_vmem():
    return pl.BlockSpec(memory_space=VMEM)


def in_smem():
    return pl.BlockSpec(memory_space=SMEM)


def f32_dot(a, b):
    return jnp.dot(a, b, preferred_element_type=jnp.float32)


def swap(value, axis, bit):
    count = lax.axis_size(axis)
    return lax.ppermute(value, axis, [(i, i ^ bit) for i in range(count)])


def is_small(count):
    return count <= 4


def tp_bits(count):
    bits = []
    bit = 2
    while bit < count:
        bits.append(bit)
        bit *= 2
    if count > 1:
        bits.append(1)
    return bits


def spread(value, axis="tp"):
    if not is_small(lax.axis_size(axis)):
        return list(lax.all_gather(value, axis))
    got = {0: value}
    for bit in tp_bits(lax.axis_size(axis)):
        for member in list(got):
            got[member ^ bit] = swap(got[member], axis, bit)
    return [got[member] for member in range(len(got))]


def add_up(value, axis):
    count = lax.axis_size(axis)
    if not is_small(count):
        return lax.psum(value, axis)
    bit = 1
    while bit < count:
        value = value + swap(value, axis, bit)
        bit *= 2
    return value


def place(pieces, ids, axis):
    width = pieces[0].shape[axis]
    shape = list(pieces[0].shape)
    shape[axis] = width * len(pieces)
    whole = jnp.zeros(shape, pieces[0].dtype)
    for member, piece in enumerate(pieces):
        whole = lax.dynamic_update_slice_in_dim(whole, piece, ids[member] * width, axis)
    return whole


def angles(position, frequency, use_column):
    freq_count = ROTARY_DIM // 4
    inverse = jnp.zeros(frequency.shape, jnp.float32)
    for number in range(freq_count):
        inverse = jnp.where(
            frequency == number, jnp.float32(10000.0 ** (-number / freq_count)), inverse
        )
    coordinate = jnp.where(use_column, position % GRID_W, position // GRID_W)
    return coordinate.astype(jnp.float32) * inverse


def tables_kernel(tok_count, info, cos_ref, sin_ref, table_ref):
    freq_count = ROTARY_DIM // 4
    start = info[0] * tok_count
    shape = cos_ref.shape
    row = lax.broadcasted_iota(jnp.int32, shape, 0)
    lane = lax.broadcasted_iota(jnp.int32, shape, 1)
    angle = angles(start + row, lane % freq_count, (lane // (2 * freq_count)) % 2 == 1)
    is_lat = row < tok_count
    cos_ref[...] = jnp.where(is_lat, jnp.cos(angle), 1.0)
    sine_of = jnp.where((lane // freq_count) % 2 == 0, -jnp.sin(angle), jnp.sin(angle))
    sin_ref[...] = jnp.where(is_lat, sine_of, 0.0)
    shape = table_ref.shape
    row = lax.broadcasted_iota(jnp.int32, shape, 0)
    lane = lax.broadcasted_iota(jnp.int32, shape, 1)
    angle = angles(start + lane, row % freq_count, row // (2 * freq_count) == 1)
    table_ref[...] = jnp.where((row // freq_count) % 2 == 0, jnp.cos(angle), jnp.sin(angle))


def turn(values, cosine, sine_of):
    freq_count = ROTARY_DIM // 4
    lanes = values.shape[1]
    lane = lax.broadcasted_iota(jnp.int32, values.shape, 1)
    first = (lane % (2 * freq_count)) < freq_count
    partner = jnp.where(
        first, pltpu.roll(values, lanes - freq_count, 1), pltpu.roll(values, freq_count, 1)
    )
    return values * cosine + partner * sine_of


class Members:
    def __init__(self, info):
        self.info = info

    def __getitem__(self, member):
        return self.info[1 + member]


def member_ids(info, count):
    return Members(info) if is_small(count) else list(range(count))


def aligned(value, step):
    return value if isinstance(value, int) else pl.multiple_of(value, step)


def gather_rows(scratch, ids, pieces):
    width = pieces[0].shape[1]
    for number, piece in enumerate(pieces):
        scratch[:, pl.ds(aligned(ids[number] * width, LANES), width)] = piece[...]


def normalize(values):
    center = values - jnp.mean(values, axis=-1, keepdims=True)
    spread_of = jnp.mean(center * center, axis=-1, keepdims=True)
    return center * lax.rsqrt(spread_of + EPSILON)


def weights_kernel(wq_hbm, wk_ref, rope_ref, wq_ref, wkr_ref, sem):
    copy = pltpu.make_async_copy(wq_hbm, wq_ref, sem)
    copy.start()
    wkr_ref[:, LANES:] = wk_ref[...]
    copies = (
        lax.broadcasted_iota(jnp.int32, (ROTARY_DIM, LANES), 0)
        == lax.broadcasted_iota(jnp.int32, (ROTARY_DIM, LANES), 1) % ROTARY_DIM
    ).astype(jnp.bfloat16)
    wkr_ref[:, :LANES] = lax.dot_general(
        rope_ref[...], copies, (((0,), (0,)), ((), ())), preferred_element_type=jnp.float32
    ).astype(jnp.bfloat16)
    copy.wait()


def early_kernel(count, *refs):
    for source, out_ref in zip(refs[:count], refs[count:]):
        for row in range(0, source.shape[0], 16):
            values = source[row : row + 16, :].astype(jnp.float32)
            out_ref[row : row + 16, :] = normalize(values)


def fetch_kernel(wq_ref, wk_hbm, wv_ref, wo_hbm, wqt_ref, wk_ref, wvt_ref, wo_ref, sems):
    copies = [
        pltpu.make_async_copy(wk_hbm, wk_ref, sems.at[0]),
        pltpu.make_async_copy(wo_hbm, wo_ref, sems.at[1]),
    ]
    for copy in copies:
        copy.start()
    wqt_ref[...] = wq_ref[...].astype(jnp.float32).T.astype(jnp.bfloat16)
    wvt_ref[...] = wv_ref[...].astype(jnp.float32).T.astype(jnp.bfloat16)
    for copy in copies:
        copy.wait()


def down_kernel(early_rows, late_rows, mod_count, tok_count, merged, info, *refs):
    ids = member_ids(info, mod_count)
    offsets = [0] if len(early_rows) + len(late_rows) == 1 else ids
    early, refs = refs[: len(early_rows)], refs[len(early_rows) :]
    late, refs = refs[: len(late_rows)], refs[len(late_rows) :]
    pieces, refs = refs[:mod_count], refs[mod_count:]
    ctx_ref, wq_ref, wkr_ref, cos_ref, sin_ref = refs[:5]
    cq_ref, kv_ref, kr_ref, ha_ref, hb_ref, mod_ref, both_ref = refs[5:]
    step = 16
    gather_rows(mod_ref, ids, pieces)

    def modulate(source, target, base, rows, is_ctx, is_normed):
        shift_by = mod_ref[is_ctx : is_ctx + 1, :]
        scale_by = 1.0 + mod_ref[2 + is_ctx : 3 + is_ctx, :]
        for row in range(0, rows, step):
            values = source[row : row + step, :]
            if not is_normed:
                values = normalize(values.astype(jnp.float32))
            target[base + row : base + row + step, :] = (values * scale_by + shift_by).astype(
                jnp.bfloat16
            )

    def multiply(source, rows_of, first, with_ctx):
        cq = f32_dot(source[...], wq_ref[...])
        both = f32_dot(source[...], wkr_ref[...])
        base = 0
        for number, rows in enumerate(rows_of):
            start = aligned(offsets[first + number] * rows, 16)
            cq_ref[pl.ds(start, rows), :] = cq[base : base + rows].astype(jnp.bfloat16)
            both_ref[pl.ds(start, rows), :] = both[base : base + rows]
            base += rows
        if with_ctx:
            both_ref[tok_count:, :] = both[base:]

    base = 0
    for source, rows in zip(early, early_rows):
        modulate(source, ha_ref, base, rows, 0, True)
        base += rows
    modulate(ctx_ref, ha_ref, base, ctx_ref.shape[0], 1, True)
    multiply(ha_ref, early_rows, 0, True)
    base = 0
    for source, rows in zip(late, late_rows):
        modulate(source, hb_ref, base, rows, 0, False)
        base += rows
    multiply(hb_ref, late_rows, len(early_rows), False)
    seg = both_ref.shape[0]
    kv_ref[:seg, :] = both_ref[:, LANES:].astype(jnp.bfloat16)
    turned = turn(both_ref[:, :LANES], cos_ref[...], sin_ref[...]).astype(jnp.bfloat16)
    if merged:
        both_ref[:, :LANES] = turned.astype(jnp.float32)
        quarter = seg // mod_count
        sub = quarter // (LANES // ROTARY_DIM)
        lane = lax.broadcasted_iota(jnp.int32, (sub, LANES), 1)
        packed = None
        for part in range(LANES // ROTARY_DIM):
            start = aligned(ids[0] * quarter + part * sub, 8)
            rows = both_ref[pl.ds(start, sub), :LANES]
            rows = jnp.where(lane // ROTARY_DIM == part, rows, 0.0)
            packed = rows if packed is None else packed + rows
        kv_ref[seg:, :] = packed.astype(jnp.bfloat16)
        kr_ref[...] = jnp.zeros_like(kr_ref)
    else:
        kr_ref[...] = turned


def normed_into(scratch, ids, pieces, gain_ref):
    width = pieces[0].shape[1]
    rows = scratch.shape[0]
    total = width * len(pieces)
    squares = None
    for piece in pieces:
        values = piece[:rows, :].astype(jnp.float32)
        part = jnp.sum(values * values, axis=-1, keepdims=True)
        squares = part if squares is None else squares + part
    factor = lax.rsqrt(squares / total + EPSILON)
    for number, piece in enumerate(pieces):
        if len(pieces) == 1:
            where = slice(None)
        else:
            where = pl.ds(aligned(ids[number] * width, LANES), width)
        gained = piece[:rows, :].astype(jnp.float32) * factor * gain_ref[:, where]
        scratch[:, where] = gained.astype(jnp.bfloat16)


def query_kernel(count, info, *refs):
    ids = member_ids(info, count)
    pieces = refs[:count]
    gain_ref, w_ref, table_ref, q_ref, scratch = refs[count:]
    normed_into(scratch, ids, pieces, gain_ref)
    rows = scratch.shape[0]
    raw = lax.dot_general(
        w_ref[...], scratch[...], (((1,), (1,)), ((), ())), preferred_element_type=jnp.float32
    )
    freq_count = ROTARY_DIM // 4
    tables = [table_ref[i * freq_count : (i + 1) * freq_count, :] for i in range(4)]
    span = PLAIN_QK_DIM + ROTARY_DIM
    q_ref[...] = jnp.zeros_like(q_ref)
    for head in range(2 * q_ref.shape[0]):
        half = head % 2
        lanes = slice(half * rows, (half + 1) * rows)
        start = head * span
        q_ref[head // 2, half * PLAIN_QK_DIM : (half + 1) * PLAIN_QK_DIM, lanes] = raw[
            start : start + PLAIN_QK_DIM
        ].astype(jnp.bfloat16)
        start += PLAIN_QK_DIM
        parts = [raw[start + i * freq_count : start + (i + 1) * freq_count] for i in range(4)]
        turned = []
        for axis in range(2):
            low, high = parts[2 * axis : 2 * axis + 2]
            cosine, sine_of = tables[2 * axis : 2 * axis + 2]
            turned += [low * cosine - high * sine_of, low * sine_of + high * cosine]
        q_ref[head // 2, LANES : LANES + ROTARY_DIM, lanes] = jnp.concatenate(
            turned, axis=0
        ).astype(jnp.bfloat16)


def fold_rows(values):
    return jnp.sum(values.reshape(-1, 8, values.shape[1]), axis=0)


def attend_kernel(counts, tok_keys, seg, merged, first, last, chosen, reuse, info, *refs):
    ids = member_ids(info, counts[0])
    bias_ref, q_ref, gain_ref, wk_ref, wv_ref = refs[:5]
    refs = refs[5:]
    blocks = []
    for count in [] if reuse else counts:
        blocks.append(refs[: count + (0 if merged else 1)])
        refs = refs[len(blocks[-1]) :]
    if not first:
        state_in, refs = refs[:3], refs[3:]
    if reuse:
        scratch, r_ref, refs = refs[0], refs[1], refs[2:]
    if last:
        out_ref, refs = refs[0], refs[1:]
    else:
        state_out, refs = refs[:3], refs[3:]
    if reuse:
        k_ref, v_ref = refs
    else:
        scratch, r_ref, k_ref, v_ref = refs
    lanes = q_ref.shape[2]
    rows = lanes // 2
    heads_of = slice(chosen[0] * LANES, (chosen[-1] + 1) * LANES)
    for number in range(len(counts)):
        block = () if reuse else blocks[number]
        pieces = block if merged else block[:-1]
        base = number * seg
        rows_ref = scratch.at[number]
        if not reuse:
            normed_into(rows_ref, ids, pieces, gain_ref)
        k_ref[base : base + seg, :] = f32_dot(rows_ref[...], wk_ref[:, heads_of]).astype(jnp.bfloat16)
        v_ref[number] = lax.dot_general(
            wv_ref[heads_of, :], rows_ref[...], (((1,), (1,)), ((), ())), preferred_element_type=jnp.float32
        ).astype(jnp.bfloat16)
        if reuse:
            continue
        if merged:
            quarter = seg // len(pieces)
            sub = quarter // (LANES // ROTARY_DIM)
            for member, piece in enumerate(pieces):
                packed = piece[seg:, :].astype(jnp.float32)
                for part in range(LANES // ROTARY_DIM):
                    moved = pltpu.roll(packed, (-part * ROTARY_DIM) % LANES, 1) if part else packed
                    start = aligned(base + ids[member] * quarter + part * sub, 16)
                    r_ref[pl.ds(start, sub), :] = moved.astype(jnp.bfloat16)
        else:
            r_ref[base : base + seg, :] = block[-1][...]
    score_scale = (PLAIN_QK_DIM + ROTARY_DIM) ** (-0.5) * LOG2E
    lane = lax.broadcasted_iota(jnp.int32, (1, lanes), 1)

    def score(pair, number):
        base = number * seg
        local = pair - chosen[0]
        span = slice(local * LANES, (local + 1) * LANES)
        key = jnp.concatenate([k_ref[base : base + seg, span], r_ref[base : base + seg, :]], axis=1)
        return f32_dot(key, q_ref[pair])

    steps = [(pair, number) for pair in chosen for number in range(len(counts))]
    ahead = score(*steps[0])
    for local, pair in enumerate(chosen):
        span = slice(local * LANES, (local + 1) * LANES)
        bias = jnp.where(lane < rows, bias_ref[2 * pair], bias_ref[2 * pair + 1]) * LOG2E
        top = total = acc = None
        if not first:
            top = state_in[0][pair, :1, :]
            total, acc = state_in[1][pair], state_in[2][pair]
        for number in range(len(counts)):
            scores = ahead
            after = local * len(counts) + number + 1
            if after < len(steps):
                ahead = score(*steps[after])
            lat, ctx = scores[:tok_keys], scores[tok_keys:]
            peak = jnp.maximum(
                jnp.max(lat, axis=0, keepdims=True) * score_scale,
                jnp.max(ctx, axis=0, keepdims=True) * score_scale + bias,
            )
            new_top = peak if top is None else jnp.maximum(top, peak)
            e_lat = jnp.exp2(lat * score_scale - new_top)
            e_ctx = jnp.exp2(ctx * score_scale - (new_top - bias))
            part = fold_rows(e_lat) + fold_rows(e_ctx)
            weights = jnp.concatenate([e_lat, e_ctx], axis=0).astype(jnp.bfloat16)
            both = f32_dot(v_ref[number, span, :], weights)
            gathered = jnp.concatenate([both[:VALUE_DIM, :rows], both[VALUE_DIM:, rows:]], axis=0)
            if top is None:
                total, acc = part, gathered
            else:
                rescale = jnp.exp2(top - new_top)
                total = total * rescale + part
                acc = gathered + jnp.concatenate(
                    [acc[:VALUE_DIM] * rescale[:, :rows], acc[VALUE_DIM:] * rescale[:, rows:]],
                    axis=0,
                )
            top = new_top
        if last:
            total = jnp.sum(total, axis=0, keepdims=True)
            done = jnp.concatenate(
                [acc[:VALUE_DIM] / total[:, :rows], acc[VALUE_DIM:] / total[:, rows:]], axis=0
            )
            out_ref[:, span] = done.T.astype(jnp.bfloat16)
        else:
            state_out[0][pair] = jnp.broadcast_to(top, (8, lanes))
            state_out[1][pair] = total
            state_out[2][pair] = acc


def out_kernel(count, splits, parts, wanted, info, *refs):
    ids = member_ids(info, count)
    pieces = refs[: count * splits]
    w_ref = refs[count * splits]
    outs = refs[1 + count * splits :]
    rows = outs[0].shape[0]
    for place_of in range(0, len(wanted), 2):
        group = wanted[place_of : place_of + 2]
        total = None
        for member in range(count):
            sides = pieces[member::count]
            if parts == 1:
                strips = [[side[...]] for side in sides]
            else:
                strips = [
                    [side[pl.ds(aligned(ids[owner] * rows, 16), rows), :] for owner in group]
                    for side in sides
                ]
            left = jnp.concatenate([jnp.concatenate(strip, axis=0) for strip in strips], axis=1)
            start = aligned(ids[member] * left.shape[1], LANES)
            part = f32_dot(left, w_ref[pl.ds(start, left.shape[1]), :])
            total = part if total is None else total + part
        for number in range(len(group)):
            outs[place_of + number][...] = total[number * rows : (number + 1) * rows].astype(
                jnp.bfloat16
            )


def final_kernel(count, mod_count, info, *refs):
    ids = member_ids(info, count)
    pieces = refs[:count]
    gates = refs[count : count + mod_count]
    lat_ref, out_ref = refs[count + mod_count :]
    width = pieces[0].shape[1]
    for number, (piece, gate) in enumerate(zip(pieces, gates)):
        span = pl.ds(aligned(ids[number] * width, LANES), width)
        out_ref[:, span] = (
            lat_ref[:, span].astype(jnp.float32)
            + gate[gate.shape[0] - 1 :, :] * piece[...].astype(jnp.float32)
        ).astype(jnp.bfloat16)


def call(kernel, outs, operands, smem=(), hbm=(), scratch=(), mib=16):
    specs = []
    for place_of in range(len(operands)):
        if place_of in hbm:
            specs.append(pl.BlockSpec(memory_space=pl.ANY))
        else:
            specs.append(in_smem() if place_of in smem else in_vmem())
    many = isinstance(outs, (list, tuple))
    return pl.pallas_call(
        kernel,
        out_shape=outs,
        in_specs=specs,
        out_specs=[in_vmem() for _ in outs] if many else in_vmem(),
        scratch_shapes=list(scratch),
        compiler_params=pltpu.CompilerParams(vmem_limit_bytes=mib * 1024 * 1024),
    )(*operands)


def on_device(
    latents,
    conditions,
    context,
    w_shift,
    w_scale,
    w_gate,
    w_qdown,
    w_kvdown,
    w_rope,
    q_gain,
    latent_norm_gain,
    query_up_weight,
    key_up_weight,
    value_up_weight,
    context_bias,
    w_out,
):
    tp_count = lax.axis_size("tp")
    sp_count = lax.axis_size("sp")
    own_rows, width = latents.shape
    tok_count = own_rows * tp_count
    ctx_rows = context.shape[0]
    seg_rows = tok_count + ctx_rows
    small = is_small(tp_count)
    members = jnp.arange(-1, tp_count, dtype=jnp.int32)
    info = jnp.where(
        members < 0, lax.axis_index("sp"), jnp.bitwise_xor(lax.axis_index("tp"), members)
    )
    info, conditions = lax.optimization_barrier((info, conditions))
    ids = member_ids(info, tp_count)
    bf16 = jnp.bfloat16

    shape_of = jax.ShapeDtypeStruct

    lat_blocks = spread(latents)
    cond_act = jax.nn.silu(conditions).astype(bf16)
    partial_mod = jnp.concatenate(
        [f32_dot(cond_act, w_shift), f32_dot(cond_act, w_scale), f32_dot(cond_act[0:1], w_gate)],
        axis=0,
    )
    mod_pieces = spread(add_up(partial_mod, "sp"))

    head_count = query_up_weight.shape[1] // (PLAIN_QK_DIM + ROTARY_DIM)
    pairs = head_count // 2
    k_cosine, k_sine, q_table = call(
        functools.partial(tables_kernel, tok_count),
        [
            shape_of((seg_rows, LANES), jnp.float32),
            shape_of((seg_rows, LANES), jnp.float32),
            shape_of((ROTARY_DIM, tok_count), jnp.float32),
        ],
        [info],
        smem=(0,),
    )
    kv_cols = w_kvdown.shape[1]
    q_cols = w_qdown.shape[1]

    w_q, w_kr = call(
        weights_kernel,
        [shape_of(w_qdown.shape, bf16), shape_of((width, LANES + kv_cols), bf16)],
        [w_qdown, w_kvdown, w_rope.T],
        hbm=(0,),
        scratch=[pltpu.SemaphoreType.DMA],
    )
    if own_rows % 16 or not small:
        lat_blocks = [place(lat_blocks, ids, 0)]
        order = [0]
    else:
        order = [0, 1] + list(range(2, tp_count)) if tp_count > 1 else [0]
    early_of = [lat_blocks[member] for member in order[:2]] if len(order) > 2 else []
    late_of = [lat_blocks[member] for member in order[len(early_of) :]]
    normed = call(
        functools.partial(early_kernel, len(early_of) + 1),
        [shape_of(value.shape, jnp.float32) for value in [*early_of, context]],
        [*early_of, context],
        mib=12,
    )
    w_qt, w_k, w_vt, w_o = call(
        fetch_kernel,
        [
            shape_of(query_up_weight.shape[::-1], bf16),
            shape_of(key_up_weight.shape, bf16),
            shape_of(value_up_weight.shape[::-1], bf16),
            shape_of(w_out.shape, bf16),
        ],
        [query_up_weight, key_up_weight, value_up_weight, w_out],
        hbm=(1, 3),
        scratch=[pltpu.SemaphoreType.DMA((2,))],
    )
    merged = (
        kv_cols % LANES == 0
        and seg_rows % (16 * tp_count * LANES // ROTARY_DIM) == 0
        and small
        and is_small(sp_count)
    )
    extra = seg_rows // tp_count * ROTARY_DIM // LANES if merged else 0
    late_rows = [value.shape[0] for value in late_of]
    early_rows = [value.shape[0] for value in early_of]
    cq_cols, kv_own, kr_own = call(
        functools.partial(down_kernel, early_rows, late_rows, tp_count, tok_count, merged),
        [
            shape_of((tok_count, q_cols), bf16),
            shape_of((seg_rows + extra, kv_cols), bf16),
            shape_of((16 if merged else seg_rows, LANES), bf16),
        ],
        [
            info,
            *normed[:-1],
            *late_of,
            *mod_pieces,
            normed[-1],
            w_q,
            w_kr,
            k_cosine,
            k_sine,
        ],
        smem=(0,),
        scratch=[
            VMEM((sum(early_rows) + ctx_rows, width), bf16),
            VMEM((sum(late_rows), width), bf16),
            VMEM((5, width), jnp.float32),
            VMEM((seg_rows, LANES + kv_cols), jnp.float32),
        ],
        mib=16,
    )

    def columns(value):
        pieces = spread(value)
        if value.shape[1] % LANES:
            return [place(pieces, ids, 1)]
        return pieces

    if is_small(sp_count):
        blocks = []
        for member in range(sp_count):
            moved = swap(kv_own, "sp", member) if member else kv_own
            block = columns(moved)
            if not merged:
                block.append(swap(kr_own, "sp", member) if member else kr_own)
            blocks.append(block)
    else:
        kr_blocks = lax.all_gather(kr_own, "sp")
        whole_rows = lax.all_gather(kv_own, "tp", axis=1, tiled=True)
        kv_blocks = lax.all_gather(whole_rows, "sp")
        blocks = [[kv, kr] for kv, kr in zip(kv_blocks, kr_blocks)]
    cq_pieces = columns(cq_cols)
    queries = call(
        functools.partial(query_kernel, len(cq_pieces)),
        shape_of((pairs, 2 * LANES, 2 * tok_count), bf16),
        [info, *cq_pieces, q_gain[None, :], w_qt, q_table],
        smem=(0,),
        scratch=[VMEM((tok_count, q_gain.shape[0]), bf16)],
    )
    held = [
        shape_of((pairs, 8, 2 * tok_count), jnp.float32),
        shape_of((pairs, 8, 2 * tok_count), jnp.float32),
        shape_of((pairs, LANES, tok_count), jnp.float32),
    ]

    def attend(part, first, last, chosen, state, kept=(), keep=False):
        heads = len(chosen) * LANES
        outs = [shape_of((tok_count, heads), bf16)] if last else held
        carried = [
            ((len(part), seg_rows, latent_norm_gain.shape[0]), bf16),
            ((len(part) * seg_rows, LANES), bf16),
        ]
        scratch = [
            VMEM((len(part) * seg_rows, heads), bf16),
            VMEM((len(part), heads, seg_rows), bf16),
        ]
        if keep:
            outs = outs + [shape_of(*one) for one in carried]
        elif not kept:
            scratch = [VMEM(*one) for one in carried] + scratch
        return call(
            functools.partial(
                attend_kernel,
                [len(block) - (0 if merged else 1) for block in part],
                tok_count,
                seg_rows,
                merged,
                first,
                last,
                chosen,
                bool(kept),
            ),
            outs,
            [
                info,
                context_bias,
                queries,
                latent_norm_gain[None, :],
                w_k,
                w_vt,
                *([] if kept else [piece for block in part for piece in block]),
                *state,
                *kept,
            ],
            smem=(0, 1),
            scratch=scratch,
            mib=16,
        )

    every = list(range(pairs))
    state = []
    begin = 0
    att_pieces = []
    while begin < sp_count:
        part = blocks[begin : begin + (1 if begin < 2 else 2)]
        first, last = begin == 0, begin + len(part) >= sp_count
        if not last:
            state = attend(part, first, False, every, state)
        begin += len(part)
    splits = [every[: pairs // 2], every[pairs // 2 :]] if pairs > 1 else [every]
    kept = ()
    for number, chosen in enumerate(splits):
        keep = number == 0 and len(splits) > 1
        done, *more = attend(part, first, True, chosen, state, kept, keep)
        kept = tuple(more) or kept
        att_pieces.append(spread(done))
    out_cols = w_out.shape[1]
    parts = tp_count if small and own_rows % 16 == 0 else 1
    if parts > 2:
        turns = [list(range(2, parts)), [0, 1]]
    else:
        turns = [list(range(parts))]
    proj = {}
    for wanted in turns:
        emitted = call(
            functools.partial(out_kernel, tp_count, len(att_pieces), parts, wanted),
            [shape_of((tok_count // parts, out_cols), bf16) for _ in wanted],
            [info, *[piece for group in att_pieces for piece in group], w_o],
            smem=(0,),
        )
        proj.update(zip(wanted, emitted))
    if parts > 1:
        proj_pieces = [
            swap(value, "tp", member) if member else value
            for member, value in sorted(proj.items())
        ]
    else:
        by_owner = proj[0].reshape(tp_count, own_rows, out_cols)
        proj_pieces = list(lax.all_to_all(by_owner, "tp", 0, 0))
        if small:
            proj_pieces = [
                lax.dynamic_index_in_dim(jnp.stack(proj_pieces), ids[member], 0, False)
                for member in range(tp_count)
            ]
    return call(
        functools.partial(final_kernel, tp_count, tp_count),
        shape_of((own_rows, width), bf16),
        [info, *proj_pieces, *mod_pieces, latents],
        smem=(0,),
    )


def solution(mesh):
    in_specs = (
        P(("grp", "sp", "tp"), None),
        P("grp", "sp"),
        P(("grp", "sp"), None),
        P("sp", "tp"),
        P("sp", "tp"),
        P("sp", "tp"),
        P(None, "tp"),
        P(None, "tp"),
        P(),
        P(),
        P(),
        P(None, "tp"),
        P(None, "tp"),
        P(None, "tp"),
        P("tp"),
        P(None, "tp"),
    )
    out_specs = P(("grp", "sp", "tp"), None)
    step = jax.shard_map(
        on_device, mesh=mesh, in_specs=in_specs, out_specs=out_specs, check_vma=False
    )
    if not (is_small(mesh.shape["tp"]) and is_small(mesh.shape["sp"])):
        return step
    return step
```
